32 devices in a mesh: sp: 16 (over z, y, x), tp: 2 (over core).
Axes of the slice: x: 2, y: 2, z: 4, core: 2. Of those that a mesh axis runs over, the one named last changes fastest.
Arguments:
- tokens: bfloat16 [4096, 2048], P('sp'), may hold values from -6 to 6
- input_norm_gain: float32 [2048], replicated, may hold values from 0.1 to 1.9
- query_matrix: bfloat16 [2048, 1024], P('sp', 'tp'), may hold values from -0.125 to 0.125
- key_matrix: bfloat16 [2048, 1024], P('sp', 'tp'), may hold values from -0.125 to 0.125
- value_matrix: bfloat16 [2048, 1024], P('sp', 'tp'), may hold values from -0.125 to 0.125
- convolution_value_matrix: bfloat16 [2048, 2048], P('sp', 'tp'), may hold values from -0.125 to 0.125
- convolution_gate_matrix: bfloat16 [2048, 2048], P('sp', 'tp'), may hold values from -0.125 to 0.125
- decay_offset_channel: float32 [1024], P('tp'), may hold values from -16 to -2
- decay_first_matrix: bfloat16 [2048, 128], replicated, may hold values from -0.125 to 0.125
- decay_second_matrix: bfloat16 [128, 1024], P(None, 'tp'), may hold values from -0.59765625 to 0.59765625
- learning_rate_offset: float32 [1024], P('tp'), may hold values from -9 to 1
- learning_rate_first_matrix: bfloat16 [2048, 128], replicated, may hold values from -0.125 to 0.125
- learning_rate_second_matrix: bfloat16 [128, 1024], P(None, 'tp'), may hold values from -0.5 to 0.5
- forgetting_rate_factor: float32 [4096, 16], P('sp', 'tp'), may hold values from 0.39 to 2.53
- state_retention_share: float32 [4096, 16], P('sp', 'tp'), may hold values from 0.12 to 1
- per_head_norm_gain: float32 [1024], P('tp'), may hold values from 0.1 to 1.9
- convolution_filter_taps: float32 [31, 2048], P(None, 'tp'), may hold values from -81 to 81
- convolution_channel_gain: float32 [2048], P('tp'), may hold values from 0.1 to 1.9
- attention_output_matrix: bfloat16 [2048, 1024], P('sp', 'tp'), may hold values from -0.109375 to 0.109375
- convolution_output_matrix: bfloat16 [2048, 2048], P('sp', 'tp'), may hold values from -0.109375 to 0.109375
Outputs:
- mixed: bfloat16 [4096, 2048], P('sp')
The draws below stay inside these ranges and needn't reach their ends.
All inputs are finite; a program needn't handle non-finite values.
Results may differ from the reference program's by a relative error of at most 0.014.
Values may be sent and summed in bfloat16 or wider, within the bound.
A program may use at most 128 MiB of HBM per device.

```python
import jax
import jax.numpy as jnp
from jax import lax

D = 2048
RHEADS = 16
HEAD = 64
RW = 1024
CONV_CH = 2048
CONV_SPAN = 31
LOWRANK = 128
TOK_DEV = 256
TOKENS = 4096
N_TP = 2


def rate_levels(key):
    order = jax.random.permutation(jax.random.fold_in(key, 11), RHEADS)
    fast_count = RHEADS // 2
    fast = jnp.repeat(order < fast_count, HEAD)
    spread = jax.random.uniform(jax.random.fold_in(key, 12), (RW,), jnp.float32)
    other = jax.random.uniform(jax.random.fold_in(key, 13), (RW,), jnp.float32)
    fast_log = jnp.log(1.0 / 60.0) + spread * jnp.log(3.0)
    slow_log = jnp.log(0.01 / TOKENS) + spread * jnp.log(5.0)
    decay_level = jnp.where(fast, fast_log, slow_log) + 0.5
    rate_level = jnp.where(fast, 2.0 * other - 1.0, jnp.log(10.0 / TOKENS) + other - 0.5)
    return (decay_level, rate_level)


def draw_decay_offset_channel(key, part):
    return rate_levels(key)[0]


def draw_learning_rate_offset(key, part):
    return rate_levels(key)[1]


def draw_forgetting_rate_factor(key, part):
    spans = TOKENS // TOK_DEV
    level = jnp.exp(jax.random.uniform(jax.random.fold_in(key, 21), (spans, RHEADS), jnp.float32, -0.7, 0.7))
    rough = jax.random.uniform(jax.random.fold_in(key, 22), (TOKENS, RHEADS), jnp.float32, 0.8, 1.25)
    return jnp.repeat(level, TOK_DEV, axis=0) * rough


def draw_state_retention_share(key, part):
    places = jax.random.randint(jax.random.fold_in(key, 31), (3, RHEADS), 0, TOKENS)
    depth = jax.random.uniform(jax.random.fold_in(key, 32), (3, RHEADS), jnp.float32, 0.6, 0.8)
    struck = jnp.arange(TOKENS, dtype=jnp.int32)[:, None, None] == places[None]
    return jnp.prod(jnp.where(struck, depth[None], 1.0), axis=1)


def draw_convolution_filter_taps(key, part):
    taps = jnp.exp(jax.random.uniform(jax.random.fold_in(key, 41), (CONV_SPAN, 1), jnp.float32, 0.0, jnp.log(10.0)))
    place = jnp.arange(CONV_CH, dtype=jnp.float32)[None, :] / CONV_CH
    rising = jnp.exp(place * jnp.log(10.0))
    rough = jax.random.uniform(jax.random.fold_in(key, 42), (1, CONV_CH), jnp.float32, 0.5, 1.5)
    base = jax.random.truncated_normal(jax.random.fold_in(key, 43), -4.0, 4.0, (CONV_SPAN, CONV_CH), jnp.float32)
    return base * taps * rising * rough / (4.0 * CONV_SPAN ** 0.5)


def block_scale(key, dims, shards, smallest, largest):
    def one(dim, blocks):
        draws = jax.random.uniform(jax.random.fold_in(jax.random.fold_in(key, 6), dim), (blocks,), jnp.float32, smallest / len(shards), largest / len(shards))
        return jnp.repeat(jnp.exp(draws), dims[dim] // blocks).reshape((-1,) + (1,) * (len(dims) - dim - 1))

    loudness = one(*shards[0])
    for cut in shards[1:]:
        loudness = loudness * one(*cut)
    return loudness


def bell_draw(stream_key, extent, width, bound, split=(), kind=jnp.bfloat16):
    entries = jax.random.normal(stream_key, extent, jnp.float32) * width
    if len(split) > 0:
        entries = block_scale(stream_key, extent, split, -0.22, 0.18) * entries
    return jnp.clip(entries, min=-bound, max=bound).astype(kind)


def setup_inputs(seed: int = 0) -> dict:
    arg_keys = jax.random.split(jax.random.key(seed), 21)
    return {
        "tokens": bell_draw(arg_keys[0], (TOKENS, D), 1.0, 6.0, ((0, 16),)),
        "input_norm_gain": jnp.clip(1.0 + 0.18 * jax.random.normal(arg_keys[1], (D,), jnp.float32), 0.1, 1.9),
        "query_matrix": bell_draw(arg_keys[2], (D, RW), D ** -0.5, 0.125, ((0, 16), (1, 2))),
        "key_matrix": bell_draw(arg_keys[3], (D, RW), D ** -0.5, 0.125, ((0, 16), (1, 2))),
        "value_matrix": bell_draw(arg_keys[4], (D, RW), D ** -0.5, 0.125, ((0, 16), (1, 2))),
        "convolution_value_matrix": bell_draw(arg_keys[5], (D, CONV_CH), D ** -0.5, 0.125, ((0, 16), (1, 2))),
        "convolution_gate_matrix": bell_draw(arg_keys[6], (D, CONV_CH), D ** -0.5, 0.125, ((0, 16), (1, 2))),
        "decay_offset_channel": draw_decay_offset_channel(jax.random.fold_in(arg_keys[20], 71), 0),
        "decay_first_matrix": bell_draw(arg_keys[8], (D, LOWRANK), D ** -0.5, 0.125),
        "decay_second_matrix": bell_draw(arg_keys[9], (LOWRANK, RW), 0.1, 0.59765625, ((1, 2),)),
        "learning_rate_offset": draw_learning_rate_offset(jax.random.fold_in(arg_keys[20], 71), 0),
        "learning_rate_first_matrix": bell_draw(arg_keys[11], (D, LOWRANK), D ** -0.5, 0.125),
        "learning_rate_second_matrix": bell_draw(arg_keys[12], (LOWRANK, RW), LOWRANK ** -0.5, 0.5, ((1, 2),)),
        "forgetting_rate_factor": draw_forgetting_rate_factor(jax.random.fold_in(arg_keys[20], 71), 0),
        "state_retention_share": draw_state_retention_share(jax.random.fold_in(arg_keys[20], 71), 0),
        "per_head_norm_gain": jnp.clip(1.0 + 0.18 * jax.random.normal(arg_keys[15], (RW,), jnp.float32), 0.1, 1.9),
        "convolution_filter_taps": draw_convolution_filter_taps(jax.random.fold_in(arg_keys[20], 71), 0),
        "convolution_channel_gain": jnp.clip(1.0 + 0.18 * jax.random.normal(arg_keys[17], (CONV_CH,), jnp.float32), 0.1, 1.9),
        "attention_output_matrix": bell_draw(arg_keys[18], (D, RW), (RW + CONV_CH) ** -0.5, 0.109375, ((0, 16), (1, 2))),
        "convolution_output_matrix": bell_draw(arg_keys[19], (D, CONV_CH), (RW + CONV_CH) ** -0.5, 0.109375, ((0, 16), (1, 2))),
    }


HIGHEST = lax.Precision.HIGHEST

def reference(tokens, input_norm_gain, query_matrix, key_matrix, value_matrix, convolution_value_matrix, convolution_gate_matrix, decay_offset_channel, decay_first_matrix, decay_second_matrix, learning_rate_offset, learning_rate_first_matrix, learning_rate_second_matrix, forgetting_rate_factor, state_retention_share, per_head_norm_gain, convolution_filter_taps, convolution_channel_gain, attention_output_matrix, convolution_output_matrix):
    widened = tokens.astype(jnp.float32)
    normed = (widened * lax.rsqrt(lax.optimization_barrier(jnp.mean(widened * widened, axis=-1, keepdims=True)) + 1e-06) * input_norm_gain).astype(jnp.bfloat16)
    query_proj = jnp.dot(normed, query_matrix, preferred_element_type=jnp.float32)
    key_proj = jnp.dot(normed, key_matrix, preferred_element_type=jnp.float32)
    value_proj = jnp.dot(normed, value_matrix, preferred_element_type=jnp.float32)
    conv_value = jnp.dot(normed, convolution_value_matrix, preferred_element_type=jnp.float32)
    conv_gate = jnp.dot(normed, convolution_gate_matrix, preferred_element_type=jnp.float32)
    decay_mid = jnp.tanh(jnp.dot(normed, decay_first_matrix, preferred_element_type=jnp.float32)).astype(jnp.bfloat16)
    rate_mid = jnp.dot(normed, learning_rate_first_matrix, preferred_element_type=jnp.float32).astype(jnp.bfloat16)
    logarithm_learning_rate = -jax.nn.softplus(-(decay_offset_channel + jnp.dot(decay_mid, decay_second_matrix, preferred_element_type=jnp.float32))) - 0.5
    learn_rate = jax.nn.sigmoid(learning_rate_offset + jnp.dot(rate_mid, learning_rate_second_matrix, preferred_element_type=jnp.float32))
    reshaped_tensor = (TOKENS, RHEADS, HEAD)
    position_decay_factor = jnp.exp(-jnp.exp(logarithm_learning_rate).reshape(reshaped_tensor) * forgetting_rate_factor[:, :, None]) * state_retention_share[:, :, None]
    key_heads = key_proj.reshape(reshaped_tensor)
    unit_key = key_heads * lax.rsqrt(lax.optimization_barrier(jnp.sum(key_heads * key_heads, axis=-1, keepdims=True)) + 1e-06)
    erase = -unit_key
    write = unit_key * learn_rate.reshape(reshaped_tensor)

    def advance(state, inputs):
        query_t, decay_t, key_t, value_t, erase_t, write_t = inputs
        pulled = jnp.einsum('hvk,hk->hv', state, erase_t, precision=HIGHEST)
        state = state * decay_t[:, None, :] + pulled[:, :, None] * write_t[:, None, :] + value_t[:, :, None] * key_t[:, None, :]
        return (state, jnp.einsum('hvk,hk->hv', state, query_t, precision=HIGHEST))
    final_state, state_rows = lax.scan(advance, jnp.zeros((RHEADS, HEAD, HEAD), jnp.float32), (query_proj.reshape(reshaped_tensor), position_decay_factor, key_heads, value_proj.reshape(reshaped_tensor), erase, write))
    centred = state_rows - lax.optimization_barrier(jnp.mean(state_rows, axis=-1, keepdims=True))
    normal_state = centred * lax.rsqrt(lax.optimization_barrier(jnp.mean(centred * centred, axis=-1, keepdims=True)) + 0.00064)
    state_mixed = (normal_state * per_head_norm_gain.reshape(RHEADS, HEAD)).reshape(TOKENS, RW).astype(jnp.bfloat16)
    gated = (conv_value * jax.nn.sigmoid(conv_gate)).astype(jnp.bfloat16)
    padded = jnp.concatenate([jnp.zeros((CONV_SPAN - 1, CONV_CH), jnp.bfloat16), gated], axis=0)
    filtered = jnp.zeros((TOKENS, CONV_CH), jnp.float32)
    for offset in range(CONV_SPAN):
        filtered = filtered + convolution_filter_taps[offset] * padded[offset:offset + TOKENS].astype(jnp.float32)
    row_mean = lax.optimization_barrier(jnp.mean(filtered, axis=-1, keepdims=True))
    deviation = filtered - row_mean
    variance = lax.optimization_barrier(jnp.mean(deviation * deviation, axis=-1, keepdims=True))
    conv_mixed = jax.nn.silu(deviation * lax.rsqrt(variance + 1e-05) * convolution_channel_gain).astype(jnp.bfloat16)
    state_part = RW // N_TP
    conv_part = CONV_CH // N_TP
    total = jnp.zeros((TOKENS, D), jnp.float32)
    for member in range(N_TP):
        state_lo = member * state_part
        conv_lo = member * conv_part
        partial_value = jnp.dot(state_mixed[:, state_lo:state_lo + state_part], attention_output_matrix[:, state_lo:state_lo + state_part].T, preferred_element_type=jnp.float32)
        partial_value = partial_value + jnp.dot(conv_mixed[:, conv_lo:conv_lo + conv_part], convolution_output_matrix[:, conv_lo:conv_lo + conv_part].T, preferred_element_type=jnp.float32)
        total = total + lax.optimization_barrier(partial_value.astype(jnp.bfloat16)).astype(jnp.float32)
    return total.astype(jnp.bfloat16)
```

```python
import functools
import math

import jax
import jax.numpy as jnp
from jax import lax
from jax.experimental import pallas as pl
from jax.experimental.pallas import tpu as pltpu
from jax.sharding import PartitionSpec as P


MESH = pl.DeviceIdType.MESH
HIGHEST = lax.Precision.HIGHEST
RMS_EPSILON = 1e-06
GROUP_EPSILON = 0.00064
LAYER_EPSILON = 1e-05
UNIT_EPSILON = 1e-06
EXP_HALF = math.exp(-0.5)


def split(x):
    top = x.astype(jnp.bfloat16)
    return top, (x - top.astype(jnp.float32)).astype(jnp.bfloat16)


def dot3(left, right, dims=((1,), (0,))):
    (lh, ll), (rh, rl) = split(left), split(right)

    def one(p, q):
        return lax.dot_general(p, q, (dims, ((), ())), preferred_element_type=jnp.float32)

    return one(lh, rh) + (one(lh, rl) + one(ll, rh))


def dot3t(left, right):
    return dot3(left, right, ((1,), (1,)))


def exact(left, right):
    return jnp.dot(left, right, precision=HIGHEST, preferred_element_type=jnp.float32)


def column(values, index):
    lanes = lax.broadcasted_iota(jnp.int32, values.shape, 1)
    return jnp.sum(jnp.where(lanes == index, values, 0.0), axis=1, keepdims=True)


def delta_kernel(
    head_size, chunk, block,
    query_ref, key_ref, value_ref, decay_ref, rate_ref, factor_ref, share_ref,
    local_ref, carried_ref, pair_ref,
):
    rows, width = query_ref.shape
    per = width // head_size
    pair = 0 if factor_ref.shape[1] == per else pl.program_id(0)
    lane = lax.broadcasted_iota(jnp.int32, (1, width), 1)
    lane_head = lane // head_size
    row_w = lax.broadcasted_iota(jnp.int32, (width, width), 0)
    col_w = lax.broadcasted_iota(jnp.int32, (width, width), 1)
    same_head = (row_w // head_size) == (col_w // head_size)
    ones_head = jnp.where(same_head, 1.0, 0.0)
    row_b = lax.broadcasted_iota(jnp.int32, (block, block), 0)
    col_b = lax.broadcasted_iota(jnp.int32, (block, block), 1)
    same_chunk = (row_b // chunk) == (col_b // chunk)
    strict = same_chunk & (row_b > col_b)
    incl = same_chunk & (row_b >= col_b)
    sums = jnp.concatenate([jnp.where(incl, 1.0, 0.0), jnp.where(same_chunk, 1.0, 0.0)], axis=0)
    eye_b = jnp.where(row_b == col_b, 1.0, 0.0)

    factor, share = factor_ref[...], jnp.log(share_ref[...])
    factor_w = jnp.zeros((rows, width), jnp.float32)
    share_w = jnp.zeros((rows, width), jnp.float32)
    for h in range(per):
        factor_w = jnp.where(lane_head == h, column(factor, pair * per + h), factor_w)
        share_w = jnp.where(lane_head == h, column(share, pair * per + h), share_w)
    logdec = share_w - (EXP_HALF * jax.nn.sigmoid(decay_ref[...])) * factor_w
    learn = jax.nn.sigmoid(rate_ref[...])
    key = key_ref[...]
    unit = key * lax.rsqrt(exact(key * key, ones_head) + UNIT_EPSILON)

    blocks = []
    for start in range(0, rows, block):
        cut = slice(start, start + block)
        q, k, v, ld = query_ref[cut], key[cut], value_ref[cut], logdec[cut]
        er, wr = -unit[cut], unit[cut] * learn[cut]
        both = exact(sums, ld)
        gain, total = both[:block], both[block:]
        mid = 0.5 * total
        up, down, bup = jnp.exp(gain - mid), jnp.exp(mid - gain), jnp.exp(gain - ld - mid)
        ehat, qhat, what, khat = er * bup, q * up, wr * down, k * down
        right = jnp.concatenate([what, khat], axis=0)
        eh_full, q_full = er * jnp.exp(gain - ld), q * jnp.exp(gain)
        to_end = jnp.exp(total - gain)
        pulled = solved = local = query = None
        heads = []
        for h in range(per):
            left = jnp.where(lane_head == h, jnp.concatenate([ehat, qhat], axis=0), 0.0)
            grid = dot3t(left, right)
            ew = jnp.where(strict, grid[:block, :block], 0.0)
            ek = jnp.where(strict, grid[:block, block:], 0.0)
            rw = jnp.where(incl, grid[block:, :block], 0.0)
            rk = jnp.where(incl, grid[block:, block:], 0.0)
            size = 2
            off = (row_b // size == col_b // size) & (row_b > col_b)
            inv = eye_b + jnp.where(off, ew, 0.0)
            while size < chunk:
                off = (row_b // (2 * size) == col_b // (2 * size)) & (row_b // size > col_b // size)
                inv = inv + dot3(dot3(inv, jnp.where(off, ew, 0.0)), inv)
                size *= 2
            seen = dot3(jnp.concatenate([ek, rk], axis=0), v)
            both = dot3(inv, jnp.concatenate([seen[:block], eh_full], axis=1))
            read = dot3(rw, both)
            heads.append((both[:, :width], both[:, width:], read[:, :width] + seen[block:], read[:, width:]))
        merged = list(heads[0])
        for h in range(1, per):
            merged = [jnp.where(lane_head == h, new, old) for new, old in zip(heads[h], merged)]
        pulled, solved, local, query = merged
        blocks.append((pulled, solved, local, q_full + query, v, wr * to_end, k * to_end, jnp.exp(total)))

    state = jnp.concatenate([jnp.where(row_w == col_w, 1.0, 0.0), jnp.zeros((width, width), jnp.float32)], axis=0)
    across = ((0,), (0,))
    for number, (pulled, solved, local, query, v, wend, kend, gain) in enumerate(blocks):
        for first in range(0, block, chunk):
            cut = slice(first, first + chunk)
            place = slice(number * block + first, number * block + first + chunk)
            got = dot3t(query[cut], state)
            carried_ref[place] = got[:, :width]
            local_ref[place] = local[cut] + got[:, width:]
            step = jnp.where(same_head, dot3(solved[cut], wend[cut], across), 0.0)
            added = dot3(
                jnp.concatenate([pulled[cut], v[cut]], axis=0),
                jnp.concatenate([wend[cut], kend[cut]], axis=0),
                across,
            )
            added = jnp.where(same_head, added, 0.0)
            moved = state * gain[first : first + 1] + dot3(state, step)
            state = jnp.concatenate([moved[:width], moved[width:] + added], axis=0)
    pair_ref[0] = state


def finish_kernel(head_size, local_ref, carried_ref, state_ref, gain_ref, out_ref):
    width = local_ref.shape[1]
    row_w = lax.broadcasted_iota(jnp.int32, (width, width), 0)
    col_w = lax.broadcasted_iota(jnp.int32, (width, width), 1)
    same_head = (row_w // head_size) == (col_w // head_size)
    average = jnp.where(same_head, 1.0 / head_size, 0.0)
    y = local_ref[...] + dot3t(carried_ref[...], state_ref[0])
    centred = y - exact(y, average)
    variance = exact(centred * centred, average)
    out_ref[...] = (centred * lax.rsqrt(variance + GROUP_EPSILON) * gain_ref[...]).astype(jnp.bfloat16)


def from_behind(value, axis, steps):
    count = lax.axis_size(axis)
    initial, last = (max(0, -steps), min(count, count - steps))
    return lax.ppermute(value, axis, [(source, source + steps) for source in range(initial, last)])


def head_blocks(pairs, head_size):
    width = pairs.shape[-1]
    return jnp.stack(
        [pairs[:, a : a + head_size, a : a + head_size] for a in range(0, width, head_size)], axis=1
    )


def delta_rule(query, key, value, decay_pre, rate_pre, factor, share, gain):
    rows, channels = query.shape
    heads = factor.shape[1]
    head_size = channels // heads
    per = math.gcd(heads, max(1, 128 // head_size))
    width, pairs = per * head_size, heads // per
    block = math.gcd(rows, 128)
    chunk = math.gcd(block, 16)
    wide = pl.BlockSpec((rows, width), lambda i: (0, i))
    whole = pl.BlockSpec((rows, heads), lambda i: (0, 0))
    local, carried, pair = pl.pallas_call(
        functools.partial(delta_kernel, head_size, chunk, block),
        grid=(pairs,),
        in_specs=[wide] * 5 + [whole] * 2,
        out_specs=[wide, wide, pl.BlockSpec((1, 2 * width, width), lambda i: (i, 0, 0))],
        out_shape=[
            jax.ShapeDtypeStruct((rows, channels), jnp.float32),
            jax.ShapeDtypeStruct((rows, channels), jnp.float32),
            jax.ShapeDtypeStruct((pairs, 2 * width, width), jnp.float32),
        ],
        cost_estimate=pl.CostEstimate(
            flops=pairs * rows * width * width * 60, bytes_accessed=rows * channels * 32, transcendentals=rows * channels * 10
        ),
        name="delta_chunks",
    )(query, key, value, decay_pre, rate_pre, factor, share)

    phi, psi = head_blocks(pair[:, :width], head_size), head_blocks(pair[:, width:], head_size)
    both = jnp.concatenate([phi, psi], axis=-2).reshape(heads, 2 * head_size, head_size)
    count, place = lax.axis_size("sp"), lax.axis_index("sp")
    steps = 1
    while steps < count - 1:
        earlier = from_behind(both, "sp", steps)
        new = exact_mul("hcd,hde->hce", earlier, both[:, :head_size])
        new = new + jnp.concatenate([jnp.zeros_like(both[:, :head_size]), both[:, head_size:]], axis=1)
        both = jnp.where(place >= steps, new, both)
        steps *= 2
    state = from_behind(both[:, head_size:], "sp", 1).reshape(pairs, per, head_size, head_size)
    same = jnp.eye(per, dtype=jnp.float32)
    state = (state[:, :, :, None, :] * same[None, :, None, :, None]).reshape(pairs, width, width)
    return pl.pallas_call(
        functools.partial(finish_kernel, head_size),
        grid=(pairs,),
        in_specs=[wide, wide, pl.BlockSpec((1, width, width), lambda i: (i, 0, 0)), pl.BlockSpec((1, width), lambda i: (0, i))],
        out_specs=wide,
        out_shape=jax.ShapeDtypeStruct((rows, channels), jnp.bfloat16),
        name="delta_finish",
    )(local, carried, state, gain[None])


def exact_mul(form, left, right):
    return jnp.einsum(form, left, right, precision=HIGHEST)


def gather_kernel(axis, radices, number, *refs):
    ins, outs = refs[:number], refs[number : 2 * number]
    own_sem, far_send, far_recv, near_send, near_recv = refs[2 * number :]
    outer, middle, inner = radices
    me = lax.axis_index(axis)
    x, y, z = me % inner, (me // inner) % middle, me // (inner * middle)

    def index(z_at, y_at, x_at):
        return (z_at * middle + y_at) * inner + x_at

    far = [index((z + step) % outer, y, x) for step in range(1, outer)]
    near = {}
    if inner == 2:
        near["x"] = index(z, y, 1 - x)
    if middle == 2:
        near["y"] = index(z, 1 - y, x)
    barrier = pltpu.get_barrier_semaphore()
    peers = far + list(near.values())
    for peer in peers:
        pl.semaphore_signal(barrier, inc=1, device_id={axis: peer}, device_id_type=MESH)
    pl.semaphore_wait(barrier, len(peers))

    def far_copy(w, step, to, z_from):
        return pltpu.make_async_remote_copy(
            src_ref=ins[w],
            dst_ref=outs[w].at[z_from, y, x],
            send_sem=far_send.at[w, step],
            recv_sem=far_recv.at[w, step],
            device_id={axis: to},
            device_id_type=MESH,
        )

    own = [pltpu.make_async_copy(ins[w], outs[w].at[z, y, x], own_sem.at[w]) for w in range(number)]
    for w in range(number):
        own[w].start()
        for step in range(outer - 1):
            far_copy(w, step, far[step], z).start()

    def region(w, order, stage, from_y, from_x):
        if stage == 0:
            return outs[w].at[:, from_y, from_x]
        return outs[w].at[:, from_y] if order[0] == "x" else outs[w].at[:, :, from_x]

    def near_copy(w, order, stage, from_y, from_x):
        part = region(w, order, stage, from_y, from_x)
        return pltpu.make_async_remote_copy(
            src_ref=part,
            dst_ref=part,
            send_sem=near_send.at[w, stage],
            recv_sem=near_recv.at[w, stage],
            device_id={axis: near[order[stage]]},
            device_id_type=MESH,
        )

    def theirs(w, order, stage):
        from_y, from_x = (y, 1 - x) if order[stage] == "x" else (1 - y, x)
        return near_copy(w, order, stage, from_y, from_x)

    names = list(near)
    orders = [names if w % 2 == 0 else names[::-1] for w in range(number)]

    def advance(w, stage):
        if stage == 0:
            own[w].wait()
            for step in range(outer - 1):
                far_copy(w, step, far[step], (z + outer - step - 1) % outer).wait_recv()
        else:
            theirs(w, orders[w], stage - 1).wait_recv()
        if stage < len(names):
            near_copy(w, orders[w], stage, y, x).start()

    last = len(names)
    for tick in range(number + last):
        for stage in range(last, -1, -1):
            w = tick - stage
            if 0 <= w < number:
                advance(w, stage)
    for w in range(number):
        for step in range(outer - 1):
            far_copy(w, step, far[step], z).wait_send()
        for stage in range(last):
            near_copy(w, orders[w], stage, y, x).wait_send()


def gather_rows(arrays, axis, number_id=0):
    count, number = lax.axis_size(axis), len(arrays)
    inner = math.gcd(count, 2)
    middle = math.gcd(count // inner, 2)
    radices = (count // inner // middle, middle, inner)
    outs = pl.pallas_call(
        functools.partial(gather_kernel, axis, radices, number),
        in_specs=[pl.BlockSpec(memory_space=pltpu.VMEM)] * number,
        out_specs=[pl.BlockSpec(memory_space=pl.ANY)] * number,
        out_shape=[jax.ShapeDtypeStruct(radices + item.shape, item.dtype) for item in arrays],
        scratch_shapes=[
            pltpu.SemaphoreType.DMA((number,)),
            pltpu.SemaphoreType.DMA((number, max(1, radices[0] - 1))),
            pltpu.SemaphoreType.DMA((number, max(1, radices[0] - 1))),
            pltpu.SemaphoreType.DMA((number, 2)),
            pltpu.SemaphoreType.DMA((number, 2)),
        ],
        compiler_params=pltpu.CompilerParams(collective_id=number_id, has_side_effects=True),
        cost_estimate=pl.CostEstimate(
            flops=10**9, bytes_accessed=sum(item.size for item in arrays) * 2 * count, transcendentals=0
        ),
        name="gather_rows",
    )(*arrays)
    return [out.reshape((-1,) + item.shape[1:]) for out, item in zip(outs, arrays)]


def plain_body(
    tokens,
    input_norm_gain,
    query_matrix,
    key_matrix,
    value_matrix,
    convolution_value_matrix,
    convolution_gate_matrix,
    decay_offset_channel,
    decay_first_matrix,
    decay_second_matrix,
    learning_rate_offset,
    learning_rate_first_matrix,
    learning_rate_second_matrix,
    forgetting_rate_factor,
    state_retention_share,
    per_head_norm_gain,
    convolution_filter_taps,
    convolution_channel_gain,
    attention_output_matrix,
    convolution_output_matrix,
):
    tok_rows = tokens.shape[0]
    widened = tokens.astype(jnp.float32)
    normed = (
        widened
        * lax.rsqrt(jnp.mean(widened * widened, axis=-1, keepdims=True) + RMS_EPSILON)
        * input_norm_gain
    ).astype(jnp.bfloat16)
    pieces = (
        *gather_rows((query_matrix, key_matrix, value_matrix), "sp"),
        lax.all_gather(convolution_value_matrix, "sp", axis=0, tiled=True),
        lax.all_gather(convolution_gate_matrix, "sp", axis=0, tiled=True),
    )
    query_proj, key_proj, value_proj, conv_value, conv_gate = tuple(
        (jnp.dot(normed, piece, preferred_element_type=jnp.float32) for piece in pieces)
    )
    decay_mid = jnp.tanh(
        jnp.dot(normed, decay_first_matrix, preferred_element_type=jnp.float32)
    ).astype(jnp.bfloat16)
    rate_mid = jnp.dot(
        normed, learning_rate_first_matrix, preferred_element_type=jnp.float32
    ).astype(jnp.bfloat16)
    decay_pre = decay_offset_channel + jnp.dot(
        decay_mid, decay_second_matrix, preferred_element_type=jnp.float32
    )
    rate_pre = learning_rate_offset + jnp.dot(
        rate_mid, learning_rate_second_matrix, preferred_element_type=jnp.float32
    )
    state_mixed = delta_rule(
        query_proj, key_proj, value_proj, decay_pre, rate_pre,
        forgetting_rate_factor, state_retention_share, per_head_norm_gain,
    )
    gated = (conv_value * jax.nn.sigmoid(conv_gate)).astype(jnp.bfloat16)
    span = convolution_filter_taps.shape[0]
    rim = from_behind(gated[tok_rows - (span - 1) :], "sp", 1)
    padded = jnp.concatenate([rim, gated], axis=0)
    filtered = jnp.zeros(gated.shape, jnp.float32)
    for offset in range(span):
        filtered = filtered + convolution_filter_taps[offset] * padded[offset : offset + tok_rows]
    total_sum, total_square = lax.psum(
        (jnp.sum(filtered, axis=-1), jnp.sum(filtered * filtered, axis=-1)), "tp"
    )
    conv_channels = filtered.shape[1] * lax.axis_size("tp")
    row_mean = total_sum / conv_channels
    deviation = filtered - row_mean[:, None]
    variance = total_square / conv_channels - row_mean * row_mean
    conv_mixed = jax.nn.silu(
        deviation * lax.rsqrt(variance + LAYER_EPSILON)[:, None] * convolution_channel_gain
    ).astype(jnp.bfloat16)
    contract_dims = (((1,), (1,)), ((), ()))
    pieces = lax.all_gather(
        (attention_output_matrix, convolution_output_matrix), "sp", axis=0, tiled=True
    )
    partial_out = lax.dot_general(
        state_mixed, pieces[0], contract_dims, preferred_element_type=jnp.float32
    ) + lax.dot_general(conv_mixed, pieces[1], contract_dims, preferred_element_type=jnp.float32)
    partial_out = partial_out.astype(jnp.bfloat16)
    if lax.axis_size("tp") != 2:
        return lax.psum(partial_out, "tp")
    other = lax.ppermute(partial_out, "tp", [(0, 1), (1, 0)])
    return (partial_out.astype(jnp.float32) + other.astype(jnp.float32)).astype(jnp.bfloat16)


def radices_of(axis):
    count = lax.axis_size(axis)
    inner = math.gcd(count, 2)
    middle = math.gcd(count // inner, 2)
    return count // inner // middle, middle, inner


def place_of(axis, radices):
    outer, middle, inner = radices
    me = lax.axis_index(axis)
    return me // (inner * middle), (me // inner) % middle, me % inner


def greet(devices):
    barrier = pltpu.get_barrier_semaphore()
    for device in devices:
        pl.semaphore_signal(barrier, inc=1, device_id=device, device_id_type=MESH)
    pl.semaphore_wait(barrier, len(devices))


def spread_kernel(axis, pair_axis, radices, widths, placed, *refs):
    number = len(widths)
    tokens_ref, side_ref, ins = refs[0], refs[1], refs[2 : 2 + number]
    kinds = 1 + max(out for out, _ in placed)
    tokens_out, side_out, outs = refs[2 + number], refs[3 + number], refs[4 + number : 4 + number + kinds]
    (own_sem, far_send, far_recv, near_send, near_recv, side_send, side_recv,
     tok_send, tok_recv, sib_send, sib_recv) = refs[4 + number + kinds :]
    outer, middle, inner = radices
    z, y, x = place_of(axis, radices)
    core = lax.axis_index(pair_axis)
    half = tokens_ref.shape[0] // 2
    mine, other = pl.ds(pl.multiple_of(core * half, half), half), pl.ds(pl.multiple_of((1 - core) * half, half), half)

    def index(z_at, y_at, x_at):
        return (z_at * middle + y_at) * inner + x_at

    far = [(z + step) % outer for step in range(1, outer)]
    near = {"x": index(z, y, 1 - x), "y": index(z, 1 - y, x)}
    greet(
        [{axis: index(at, y, x)} for at in far]
        + [{axis: peer} for peer in near.values()]
        + [{pair_axis: 1 - core}]
    )

    def part(w, at):
        return ins[w].at[:, pl.ds(pl.multiple_of(at * widths[w], widths[w]), widths[w])]

    def slot(w, *where):
        out, offset = placed[w]
        return outs[out].at[(*where, slice(None), pl.ds(offset, widths[w]))]

    def far_copy(w, step, to, z_from):
        return pltpu.make_async_remote_copy(
            src_ref=part(w, to), dst_ref=slot(w, z_from, y, x),
            send_sem=far_send.at[w, step], recv_sem=far_recv.at[w, step],
            device_id={axis: index(to, y, x)}, device_id_type=MESH,
        )

    def side_copy(step, to, z_from):
        return pltpu.make_async_remote_copy(
            src_ref=side_ref, dst_ref=side_out.at[z_from],
            send_sem=side_send.at[step], recv_sem=side_recv.at[step],
            device_id={axis: index(to, y, x)}, device_id_type=MESH,
        )

    def near_copy(w, order, stage, y_at, x_at):
        if stage == 0:
            region = slot(w, slice(None), y_at, x_at)
        elif order[0] == "x":
            region = slot(w, slice(None), y_at, slice(None))
        else:
            region = slot(w, slice(None), slice(None), x_at)
        return pltpu.make_async_remote_copy(
            src_ref=region, dst_ref=region,
            send_sem=near_send.at[w, stage], recv_sem=near_recv.at[w, stage],
            device_id={axis: near[order[stage]]}, device_id_type=MESH,
        )

    def theirs(w, order, stage):
        y_at, x_at = (y, 1 - x) if order[stage] == "x" else (1 - y, x)
        return near_copy(w, order, stage, y_at, x_at)

    def inside(at):
        return (at >= 0) & (at < outer)

    ways = (1, -1)

    def token_copy(way, step, block, source):
        return pltpu.make_async_remote_copy(
            src_ref=source, dst_ref=tokens_out.at[block, mine],
            send_sem=tok_send.at[way, step], recv_sem=tok_recv.at[way, step],
            device_id={axis: index((z + ways[way] + outer) % outer, y, x)}, device_id_type=MESH,
        )

    def sibling_copy(way, step, block, rows):
        return pltpu.make_async_remote_copy(
            src_ref=tokens_out.at[block, rows], dst_ref=tokens_out.at[block, rows],
            send_sem=sib_send.at[way, step], recv_sem=sib_recv.at[way, step],
            device_id={pair_axis: 1 - core}, device_id_type=MESH,
        )

    def arrived(way, step):
        return z - ways[way] * (step + 1)

    def sends(way, step):
        return inside(z + ways[way]) & inside(z - ways[way] * step)

    own = [pltpu.make_async_copy(part(w, z), slot(w, z, y, x), own_sem.at[w]) for w in range(number)]
    own.append(pltpu.make_async_copy(tokens_ref, tokens_out.at[z], own_sem.at[number]))
    own.append(pltpu.make_async_copy(side_ref, side_out.at[z], own_sem.at[number + 1]))
    for step in range(outer - 1):
        side_copy(step, far[step], z).start()
    for w in range(number):
        own[w].start()
        for step in range(outer - 1):
            far_copy(w, step, far[step], z).start()
    for way in range(2):
        @pl.when(sends(way, 0))
        def _():
            token_copy(way, 0, z, tokens_ref.at[mine]).start()
    own[number].start()
    own[number + 1].start()

    names = list(near)
    orders = [names if w % 2 == 0 else names[::-1] for w in range(number)]

    def advance(w, stage):
        if stage == 0:
            own[w].wait()
            for step in range(outer - 1):
                far_copy(w, step, far[step], (z + outer - step - 1) % outer).wait_recv()
        else:
            theirs(w, orders[w], stage - 1).wait_recv()
        if stage < len(names):
            near_copy(w, orders[w], stage, y, x).start()

    def token_step(step):
        for way in range(2):
            block = arrived(way, step)
            @pl.when(inside(block))
            def _():
                token_copy(way, step, block, tokens_out.at[block, mine]).wait_recv()
                if step + 1 < outer - 1:
                    @pl.when(sends(way, step + 1))
                    def _():
                        token_copy(way, step + 1, block, tokens_out.at[block, mine]).start()
                sibling_copy(way, step, block, mine).start()

    last = len(names)
    steps = 0
    for tick in range(number + last):
        for stage in range(last, -1, -1):
            w = tick - stage
            if 0 <= w < number:
                advance(w, stage)
        if tick >= number - 1 and steps < outer - 1:
            token_step(steps)
            steps += 1
    while steps < outer - 1:
        token_step(steps)
        steps += 1
    own[number].wait()
    own[number + 1].wait()
    for step in range(outer - 1):
        side_copy(step, far[step], (z + outer - step - 1) % outer).wait_recv()
        side_copy(step, far[step], z).wait_send()
    for step in range(outer - 1):
        for way in range(2):
            block = arrived(way, step)
            @pl.when(inside(block))
            def _():
                sibling_copy(way, step, block, other).wait_recv()
                sibling_copy(way, step, block, mine).wait_send()
            @pl.when(sends(way, step))
            def _():
                token_copy(way, step, z - ways[way] * step, tokens_ref.at[mine]).wait_send()
    for w in range(number):
        for step in range(outer - 1):
            far_copy(w, step, far[step], z).wait_send()
        for stage in range(last):
            near_copy(w, orders[w], stage, y, x).wait_send()


def spread(normed, side, weights, groups, axis, pair_axis):
    radices = radices_of(axis)
    outer, number = radices[0], len(weights)
    widths = [item.shape[1] // outer for item in weights]
    placed, totals = [None] * number, []
    for out, members in enumerate(groups):
        offset = 0
        for w in members:
            placed[w] = (out, offset)
            offset += widths[w]
        totals.append(offset)
    depth = weights[0].shape[0]
    outs = pl.pallas_call(
        functools.partial(spread_kernel, axis, pair_axis, radices, widths, placed),
        in_specs=[pl.BlockSpec(memory_space=pltpu.VMEM)] * (2 + number),
        out_specs=[pl.BlockSpec(memory_space=pl.ANY)] * (2 + len(groups)),
        out_shape=[
            jax.ShapeDtypeStruct((outer,) + normed.shape, normed.dtype),
            jax.ShapeDtypeStruct((outer,) + side.shape, side.dtype),
        ]
        + [jax.ShapeDtypeStruct(radices + (depth, total), weights[0].dtype) for total in totals],
        scratch_shapes=[
            pltpu.SemaphoreType.DMA((number + 2,)),
            pltpu.SemaphoreType.DMA((number, outer - 1)),
            pltpu.SemaphoreType.DMA((number, outer - 1)),
            pltpu.SemaphoreType.DMA((number, 2)),
            pltpu.SemaphoreType.DMA((number, 2)),
            pltpu.SemaphoreType.DMA((outer - 1,)),
            pltpu.SemaphoreType.DMA((outer - 1,)),
            pltpu.SemaphoreType.DMA((2, outer - 1)),
            pltpu.SemaphoreType.DMA((2, outer - 1)),
            pltpu.SemaphoreType.DMA((2, outer - 1)),
            pltpu.SemaphoreType.DMA((2, outer - 1)),
        ],
        compiler_params=pltpu.CompilerParams(collective_id=0, has_side_effects=True),
        cost_estimate=pl.CostEstimate(flops=10**9, bytes_accessed=2 * normed.size * 2 * outer, transcendentals=0),
        name="spread_weights",
    )(normed, side, *weights)
    return outs[0], outs[1], [out.reshape(-1, total) for out, total in zip(outs[2:], totals)]


def states_kernel(
    axis, pair_axis, radices, head_size,
    pair_ref, sums_ref, local_ref, carried_ref, gain_ref,
    mixed_ref, totals_ref,
    held, stats, own_sem, pair_send, pair_recv, stat_send, stat_recv,
):
    outer, middle, inner = radices
    planes = middle * inner
    z, y, x = place_of(axis, radices)
    place = y * inner + x
    core = lax.axis_index(pair_axis)
    width = pair_ref.shape[-1]
    rows = local_ref.shape[0] // outer
    plane_peers = [(place + step) % planes for step in range(1, planes)]
    cores = lax.axis_size(pair_axis)
    lines = [(dz, dc) for dz in range(outer) for dc in range(cores) if dz or dc]

    def line_device(dz, dc):
        return {axis: ((z + dz) % outer) * planes + place, pair_axis: (core + dc) % cores}

    greet([{axis: z * planes + peer} for peer in plane_peers] + [line_device(*line) for line in lines])

    def pair_copy(step, p_from):
        return pltpu.make_async_remote_copy(
            src_ref=pair_ref, dst_ref=held.at[p_from],
            send_sem=pair_send.at[step], recv_sem=pair_recv.at[step],
            device_id={axis: z * planes + plane_peers[step]}, device_id_type=MESH,
        )

    def stat_copy(number, slot):
        return pltpu.make_async_remote_copy(
            src_ref=sums_ref, dst_ref=stats.at[slot],
            send_sem=stat_send.at[number], recv_sem=stat_recv.at[number],
            device_id=line_device(*lines[number]), device_id_type=MESH,
        )

    for step in range(planes - 1):
        pair_copy(step, place).start()
    for number in range(len(lines)):
        stat_copy(number, number).start()
    own = pltpu.make_async_copy(pair_ref, held.at[place], own_sem.at[0])
    own.start()

    for number in range(len(lines)):
        stat_copy(number, number).wait_recv()
    totals = sums_ref[...]
    for number in range(len(lines)):
        totals = totals + stats[number]
    totals_ref[...] = totals

    own.wait()
    for step in range(planes - 1):
        pair_copy(step, (place + planes - step - 1) % planes).wait_recv()

    lane_head = lax.broadcasted_iota(jnp.int32, (1, width), 1) // head_size
    row_w = lax.broadcasted_iota(jnp.int32, (width, width), 0)
    col_w = lax.broadcasted_iota(jnp.int32, (width, width), 1)
    average = jnp.where((row_w // head_size) == (col_w // head_size), 1.0 / head_size, 0.0)

    def widen(compact):
        return jnp.concatenate([jnp.where(lane_head == h, compact, 0.0) for h in range(width // head_size)], axis=0)

    state = jnp.zeros((head_size, width), jnp.float32)
    for block in range(outer):
        keep = state
        for p in range(planes):
            if p:
                keep = jnp.where(place == p, state, keep)
            state = dot3(state, widen(held[p, block, :head_size])) + held[p, block, head_size:]
        cut = slice(block * rows, (block + 1) * rows)
        full = local_ref[cut] + dot3t(carried_ref[cut], widen(keep))
        centred = full - exact(full, average)
        variance = exact(centred * centred, average)
        mixed_ref[cut] = (centred * lax.rsqrt(variance + GROUP_EPSILON) * gain_ref[...]).astype(jnp.bfloat16)

    for step in range(planes - 1):
        pair_copy(step, place).wait_send()
    for number in range(len(lines)):
        stat_copy(number, number).wait_send()


def states(pair, sums, local, carried, gain, head_size, axis, pair_axis):
    radices = radices_of(axis)
    planes, cores = radices[1] * radices[2], lax.axis_size(pair_axis)
    lines = radices[0] * cores - 1
    vmem = pl.BlockSpec(memory_space=pltpu.VMEM)
    return pl.pallas_call(
        functools.partial(states_kernel, axis, pair_axis, radices, head_size),
        in_specs=[vmem] * 5,
        out_specs=[vmem] * 2,
        out_shape=[jax.ShapeDtypeStruct(local.shape, jnp.bfloat16), jax.ShapeDtypeStruct(sums.shape, jnp.float32)],
        scratch_shapes=[
            pltpu.VMEM((planes,) + pair.shape, jnp.float32),
            pltpu.VMEM((lines,) + sums.shape, jnp.float32),
            pltpu.SemaphoreType.DMA((1,)),
            pltpu.SemaphoreType.DMA((planes - 1,)),
            pltpu.SemaphoreType.DMA((planes - 1,)),
            pltpu.SemaphoreType.DMA((lines,)),
            pltpu.SemaphoreType.DMA((lines,)),
        ],
        compiler_params=pltpu.CompilerParams(collective_id=1, has_side_effects=True),
        cost_estimate=pl.CostEstimate(flops=10**9, bytes_accessed=pair.size * 16, transcendentals=0),
        name="carry_states",
    )(pair, sums, local, carried, gain)


def reduce_kernel(
    axis, pair_axis, radices,
    state_ref, conv_ref, matrix_ref, out_ref,
    keep, twin_out, twin_in, chain_out, chain_in,
    twin_send, twin_recv, chain_send, chain_recv, last_send, last_recv,
):
    outer, middle, inner = radices
    z, y, x = place_of(axis, radices)
    core = lax.axis_index(pair_axis)
    rows, half = keep.shape[1:]
    split_at = state_ref.shape[1]
    ways = (1, -1)

    def index(z_at):
        return (z_at * middle + y) * inner + x

    def inside(at):
        return (at >= 0) & (at < outer)

    greet([{axis: index((z + step) % outer)} for step in range(1, outer)] + [{pair_axis: 1 - core}])

    def twin_copy(block):
        return pltpu.make_async_remote_copy(
            src_ref=twin_out.at[block], dst_ref=twin_in.at[block],
            send_sem=twin_send.at[block], recv_sem=twin_recv.at[block],
            device_id={pair_axis: 1 - core}, device_id_type=MESH,
        )

    def chain_copy(way, steps):
        return pltpu.make_async_remote_copy(
            src_ref=chain_out.at[way, steps - 1], dst_ref=chain_in.at[way, steps - 1],
            send_sem=chain_send.at[way, steps - 1], recv_sem=chain_recv.at[way, steps - 1],
            device_id={axis: index((z + ways[way] + outer) % outer)}, device_id_type=MESH,
        )

    def product(block, side):
        cut = pl.ds(pl.multiple_of(block * rows, rows), rows)
        these = pl.ds(pl.multiple_of(side * half, half), half)
        dims = (((1,), (1,)), ((), ()))
        return lax.dot_general(
            state_ref[cut, :], matrix_ref[these, :split_at], dims, preferred_element_type=jnp.float32
        ) + lax.dot_general(
            conv_ref[cut, :], matrix_ref[these, split_at:], dims, preferred_element_type=jnp.float32
        )

    def one_block(number, carry):
        block = jnp.where(z < outer // 2, outer - 1 - number, number)
        twin_out[block] = product(block, 1 - core).astype(jnp.bfloat16)
        twin_copy(block).start()
        keep[block] = product(block, core)
        return carry

    lax.fori_loop(0, outer, one_block, 0)

    for steps in range(outer - 1, 0, -1):
        for way in range(2):
            block = z + ways[way] * steps

            @pl.when(inside(block))
            def _():
                twin_copy(block).wait_recv()
                keep[block] += twin_in[block].astype(jnp.float32)
                if steps + 1 < outer:
                    @pl.when(inside(z - ways[way]))
                    def _():
                        chain_copy(way, steps + 1).wait_recv()
                        keep[block] += chain_in[way, steps].astype(jnp.float32)
                chain_out[way, steps - 1] = keep[block].astype(jnp.bfloat16)
                chain_copy(way, steps).start()

    twin_copy(z).wait_recv()
    keep[z] += twin_in[z].astype(jnp.float32)
    for way in range(2):
        @pl.when(inside(z - ways[way]))
        def _():
            chain_copy(way, 1).wait_recv()
            keep[z] += chain_in[way, 0].astype(jnp.float32)

    ours = pl.ds(pl.multiple_of(core * half, half), half)
    out_ref[:, ours] = keep[z].astype(jnp.bfloat16)

    def last_copy(side):
        place = out_ref.at[:, pl.ds(pl.multiple_of(side * half, half), half)]
        return pltpu.make_async_remote_copy(
            src_ref=place, dst_ref=place, send_sem=last_send.at[0], recv_sem=last_recv.at[0],
            device_id={pair_axis: 1 - core}, device_id_type=MESH,
        )

    last_copy(core).start()
    for block in range(outer):
        twin_copy(block).wait_send()
    for steps in range(outer - 1, 0, -1):
        for way in range(2):
            @pl.when(inside(z + ways[way] * steps))
            def _():
                chain_copy(way, steps).wait_send()
    last_copy(1 - core).wait_recv()
    last_copy(core).wait_send()


def reduce_rows(state_mixed, conv_mixed, matrix, outer, axis, pair_axis):
    radices = radices_of(axis)
    rows, half = state_mixed.shape[0] // outer, matrix.shape[0] // 2
    vmem = pl.BlockSpec(memory_space=pltpu.VMEM)
    slots = (2, outer - 1)
    return pl.pallas_call(
        functools.partial(reduce_kernel, axis, pair_axis, radices),
        in_specs=[vmem] * 3,
        out_specs=vmem,
        out_shape=jax.ShapeDtypeStruct((rows, 2 * half), jnp.bfloat16),
        scratch_shapes=[
            pltpu.VMEM((outer, rows, half), jnp.float32),
            pltpu.VMEM((outer, rows, half), jnp.bfloat16),
            pltpu.VMEM((outer, rows, half), jnp.bfloat16),
            pltpu.VMEM(slots + (rows, half), jnp.bfloat16),
            pltpu.VMEM(slots + (rows, half), jnp.bfloat16),
            pltpu.SemaphoreType.DMA((outer,)),
            pltpu.SemaphoreType.DMA((outer,)),
            pltpu.SemaphoreType.DMA(slots),
            pltpu.SemaphoreType.DMA(slots),
            pltpu.SemaphoreType.DMA((1,)),
            pltpu.SemaphoreType.DMA((1,)),
        ],
        compiler_params=pltpu.CompilerParams(collective_id=2, has_side_effects=True, vmem_limit_bytes=60 * 2**20),
        cost_estimate=pl.CostEstimate(flops=10**9, bytes_accessed=matrix.size * 8, transcendentals=0),
        name="reduce_rows",
    )(state_mixed, conv_mixed, matrix)


def delta_blocks_kernel(head_size, chunk, block, *refs):
    ins, (local_ref, carried_ref, pair_ref), scratch = refs[:7], refs[7:10], refs[10]
    delta_kernel(head_size, chunk, block, *ins, local_ref, carried_ref, scratch)
    width = scratch.shape[-1]
    for first in range(2):
        total = jnp.zeros((head_size, width), jnp.float32)
        for h in range(width // head_size):
            at = first * width + h * head_size
            total = total + scratch[0, at : at + head_size]
        pair_ref[0, first * head_size : (first + 1) * head_size] = total


def delta_blocks(query, key, value, decay_pre, rate_pre, factor, share, blocks, head_size):
    total, width = query.shape
    rows, heads = total // blocks, factor.shape[1]
    block = math.gcd(rows, 128)
    chunk = math.gcd(block, 16)
    wide = pl.BlockSpec((rows, width), lambda i: (i, 0))
    thin = pl.BlockSpec((rows, heads), lambda i: (i, 0))
    return pl.pallas_call(
        functools.partial(delta_blocks_kernel, head_size, chunk, block),
        grid=(blocks,),
        in_specs=[wide] * 5 + [thin] * 2,
        out_specs=[wide, wide, pl.BlockSpec((1, 2 * head_size, width), lambda i: (i, 0, 0))],
        out_shape=[
            jax.ShapeDtypeStruct((total, width), jnp.float32),
            jax.ShapeDtypeStruct((total, width), jnp.float32),
            jax.ShapeDtypeStruct((blocks, 2 * head_size, width), jnp.float32),
        ],
        scratch_shapes=[pltpu.VMEM((1, 2 * width, width), jnp.float32)],
        cost_estimate=pl.CostEstimate(
            flops=total * width * width * 60, bytes_accessed=total * width * 32, transcendentals=total * width * 10
        ),
        name="delta_chunks",
    )(query, key, value, decay_pre, rate_pre, factor, share)


def body(*args):
    outer, middle, inner = radices_of("sp")
    heads, channels = args[13].shape[1], args[2].shape[1]
    width = channels // outer
    fits = (
        lax.axis_size("tp") == 2 and outer > 1 and middle == 2 and inner == 2
        and heads % outer == 0 and width == 128 and args[5].shape[1] % (128 * outer) == 0
    )
    return fast_body(*args) if fits else plain_body(*args)


def fast_body(
    tokens,
    input_norm_gain,
    query_matrix,
    key_matrix,
    value_matrix,
    convolution_value_matrix,
    convolution_gate_matrix,
    decay_offset_channel,
    decay_first_matrix,
    decay_second_matrix,
    learning_rate_offset,
    learning_rate_first_matrix,
    learning_rate_second_matrix,
    forgetting_rate_factor,
    state_retention_share,
    per_head_norm_gain,
    convolution_filter_taps,
    convolution_channel_gain,
    attention_output_matrix,
    convolution_output_matrix,
):
    outer, middle, inner = radices_of("sp")
    planes = middle * inner
    rows = tokens.shape[0]
    heads, channels = forgetting_rate_factor.shape[1], query_matrix.shape[1]
    head_size = channels // heads
    z = lax.axis_index("sp") // planes

    def quarter(value, axis=-1):
        size = value.shape[axis] // outer
        return lax.dynamic_slice_in_dim(value, z * size, size, axis)

    widened = tokens.astype(jnp.float32)
    normed = (
        widened
        * lax.rsqrt(jnp.mean(widened * widened, axis=-1, keepdims=True) + RMS_EPSILON)
        * input_norm_gain
    ).astype(jnp.bfloat16)
    side = jnp.concatenate([forgetting_rate_factor.T, state_retention_share.T], axis=0)
    weights = (
        query_matrix, key_matrix, value_matrix, convolution_value_matrix, convolution_gate_matrix,
        attention_output_matrix, convolution_output_matrix,
    )
    normed, side, (heads_in, conv_in, both_out) = spread(normed, side, weights, ((0, 1, 2), (3, 4), (5, 6)), "sp", "tp")
    normed = normed.reshape(-1, normed.shape[-1])

    width = channels // outer
    projected = [
        jnp.dot(normed, heads_in[:, i * width : (i + 1) * width], preferred_element_type=jnp.float32) for i in range(3)
    ]
    conv_width = conv_in.shape[1] // 2
    conv_value = jnp.dot(normed, conv_in[:, :conv_width], preferred_element_type=jnp.float32)
    conv_gate = jnp.dot(normed, conv_in[:, conv_width:], preferred_element_type=jnp.float32)
    decay_mid = jnp.tanh(jnp.dot(normed, decay_first_matrix, preferred_element_type=jnp.float32)).astype(jnp.bfloat16)
    rate_mid = jnp.dot(normed, learning_rate_first_matrix, preferred_element_type=jnp.float32).astype(jnp.bfloat16)
    decay_pre = quarter(decay_offset_channel) + jnp.dot(
        decay_mid, quarter(decay_second_matrix), preferred_element_type=jnp.float32
    )
    rate_pre = quarter(learning_rate_offset) + jnp.dot(
        rate_mid, quarter(learning_rate_second_matrix), preferred_element_type=jnp.float32
    )
    few = quarter(side.reshape(outer, 2, heads, rows), 2).transpose(1, 0, 3, 2).reshape(2, outer * rows, heads // outer)

    gated = (conv_value * jax.nn.sigmoid(conv_gate)).astype(jnp.bfloat16).reshape(outer, rows, conv_width)
    span = convolution_filter_taps.shape[0]
    ring = [
        (at * planes + p, at * planes + (p + 1) % planes) for at in range(outer) for p in range(planes)
    ]
    rim = lax.ppermute(gated[:, rows - (span - 1) :], "sp", ring)
    shifted = jnp.concatenate([jnp.zeros_like(rim[:1]), rim[:-1]], axis=0)
    rim = jnp.where(lax.axis_index("sp") % planes == 0, shifted, rim)
    padded = jnp.concatenate([rim, gated], axis=1)
    taps = quarter(convolution_filter_taps)
    filtered = jnp.zeros(gated.shape, jnp.float32)
    for offset in range(span):
        filtered = filtered + taps[offset] * padded[:, offset : offset + rows]
    filtered = filtered.reshape(outer * rows, conv_width)
    sums = jnp.stack([jnp.sum(filtered, axis=-1), jnp.sum(filtered * filtered, axis=-1)])

    local, carried, pair = delta_blocks(*projected, decay_pre, rate_pre, few[0], few[1], outer, head_size)
    state_mixed, totals = states(
        pair, sums, local, carried, quarter(per_head_norm_gain)[None], head_size, "sp", "tp"
    )
    conv_channels = conv_width * outer * lax.axis_size("tp")
    row_mean = totals[0] / conv_channels
    deviation = filtered - row_mean[:, None]
    variance = totals[1] / conv_channels - row_mean * row_mean
    conv_mixed = jax.nn.silu(
        deviation * lax.rsqrt(variance + LAYER_EPSILON)[:, None] * quarter(convolution_channel_gain)
    ).astype(jnp.bfloat16)
    return reduce_rows(state_mixed, conv_mixed, both_out, outer, "sp", "tp")


def solution(mesh):
    return jax.shard_map(
        body,
        mesh=mesh,
        in_specs=(
            P("sp", None),
            P(),
            P("sp", "tp"),
            P("sp", "tp"),
            P("sp", "tp"),
            P("sp", "tp"),
            P("sp", "tp"),
            P("tp"),
            P(),
            P(None, "tp"),
            P("tp"),
            P(),
            P(None, "tp"),
            P("sp", "tp"),
            P("sp", "tp"),
            P("tp"),
            P(None, "tp"),
            P("tp"),
            P("sp", "tp"),
            P("sp", "tp"),
        ),
        out_specs=P("sp", None),
        check_vma=False,
    )
```

```python
import functools
import math

import jax
import jax.numpy as jnp
from jax import lax
from jax.experimental import pallas as pl
from jax.experimental.pallas import tpu as pltpu
from jax.sharding import PartitionSpec as P


MESH = pl.DeviceIdType.MESH
HIGHEST = lax.Precision.HIGHEST
RMS_EPSILON = 1e-06
GROUP_EPSILON = 0.00064
LAYER_EPSILON = 1e-05
UNIT_EPSILON = 1e-06
EXP_HALF = math.exp(-0.5)


def split(x):
    top = x.astype(jnp.bfloat16)
    return top, (x - top.astype(jnp.float32)).astype(jnp.bfloat16)


def dot3(left, right, dims=((1,), (0,))):
    (lh, ll), (rh, rl) = split(left), split(right)

    def one(p, q):
        return lax.dot_general(p, q, (dims, ((), ())), preferred_element_type=jnp.float32)

    return one(lh, rh) + (one(lh, rl) + one(ll, rh))


def dot3t(left, right):
    return dot3(left, right, ((1,), (1,)))


def exact(left, right):
    return jnp.dot(left, right, precision=HIGHEST, preferred_element_type=jnp.float32)


def column(values, index):
    lanes = lax.broadcasted_iota(jnp.int32, values.shape, 1)
    return jnp.sum(jnp.where(lanes == index, values, 0.0), axis=1, keepdims=True)


def delta_kernel(
    head_size, chunk, block,
    query_ref, key_ref, value_ref, decay_ref, rate_ref, factor_ref, share_ref,
    local_ref, carried_ref, pair_ref,
):
    rows, width = query_ref.shape
    per = width // head_size
    pair = 0 if factor_ref.shape[1] == per else pl.program_id(0)
    lane = lax.broadcasted_iota(jnp.int32, (1, width), 1)
    lane_head = lane // head_size
    row_w = lax.broadcasted_iota(jnp.int32, (width, width), 0)
    col_w = lax.broadcasted_iota(jnp.int32, (width, width), 1)
    same_head = (row_w // head_size) == (col_w // head_size)
    ones_head = jnp.where(same_head, 1.0, 0.0)
    row_b = lax.broadcasted_iota(jnp.int32, (block, block), 0)
    col_b = lax.broadcasted_iota(jnp.int32, (block, block), 1)
    same_chunk = (row_b // chunk) == (col_b // chunk)
    strict = same_chunk & (row_b > col_b)
    incl = same_chunk & (row_b >= col_b)
    sums = jnp.concatenate([jnp.where(incl, 1.0, 0.0), jnp.where(same_chunk, 1.0, 0.0)], axis=0)
    eye_b = jnp.where(row_b == col_b, 1.0, 0.0)

    factor, share = factor_ref[...], jnp.log(share_ref[...])
    factor_w = jnp.zeros((rows, width), jnp.float32)
    share_w = jnp.zeros((rows, width), jnp.float32)
    for h in range(per):
        factor_w = jnp.where(lane_head == h, column(factor, pair * per + h), factor_w)
        share_w = jnp.where(lane_head == h, column(share, pair * per + h), share_w)
    logdec = share_w - (EXP_HALF * jax.nn.sigmoid(decay_ref[...])) * factor_w
    learn = jax.nn.sigmoid(rate_ref[...])
    key = key_ref[...]
    unit = key * lax.rsqrt(exact(key * key, ones_head) + UNIT_EPSILON)

    blocks = []
    for start in range(0, rows, block):
        cut = slice(start, start + block)
        q, k, v, ld = query_ref[cut], key[cut], value_ref[cut], logdec[cut]
        er, wr = -unit[cut], unit[cut] * learn[cut]
        both = exact(sums, ld)
        gain, total = both[:block], both[block:]
        mid = 0.5 * total
        up, down, bup = jnp.exp(gain - mid), jnp.exp(mid - gain), jnp.exp(gain - ld - mid)
        ehat, qhat, what, khat = er * bup, q * up, wr * down, k * down
        right = jnp.concatenate([what, khat], axis=0)
        eh_full, q_full = er * jnp.exp(gain - ld), q * jnp.exp(gain)
        to_end = jnp.exp(total - gain)
        pulled = solved = local = query = None
        heads = []
        for h in range(per):
            left = jnp.where(lane_head == h, jnp.concatenate([ehat, qhat], axis=0), 0.0)
            grid = dot3t(left, right)
            ew = jnp.where(strict, grid[:block, :block], 0.0)
            ek = jnp.where(strict, grid[:block, block:], 0.0)
            rw = jnp.where(incl, grid[block:, :block], 0.0)
            rk = jnp.where(incl, grid[block:, block:], 0.0)
            size = 2
            off = (row_b // size == col_b // size) & (row_b > col_b)
            inv = eye_b + jnp.where(off, ew, 0.0)
            while size < chunk:
                off = (row_b // (2 * size) == col_b // (2 * size)) & (row_b // size > col_b // size)
                inv = inv + dot3(dot3(inv, jnp.where(off, ew, 0.0)), inv)
                size *= 2
            seen = dot3(jnp.concatenate([ek, rk], axis=0), v)
            both = dot3(inv, jnp.concatenate([seen[:block], eh_full], axis=1))
            read = dot3(rw, both)
            heads.append((both[:, :width], both[:, width:], read[:, :width] + seen[block:], read[:, width:]))
        merged = list(heads[0])
        for h in range(1, per):
            merged = [jnp.where(lane_head == h, new, old) for new, old in zip(heads[h], merged)]
        pulled, solved, local, query = merged
        blocks.append((pulled, solved, local, q_full + query, v, wr * to_end, k * to_end, jnp.exp(total)))

    state = jnp.concatenate([jnp.where(row_w == col_w, 1.0, 0.0), jnp.zeros((width, width), jnp.float32)], axis=0)
    across = ((0,), (0,))
    for number, (pulled, solved, local, query, v, wend, kend, gain) in enumerate(blocks):
        for first in range(0, block, chunk):
            cut = slice(first, first + chunk)
            place = slice(number * block + first, number * block + first + chunk)
            got = dot3t(query[cut], state)
            carried_ref[place] = got[:, :width]
            local_ref[place] = local[cut] + got[:, width:]
            step = jnp.where(same_head, dot3(solved[cut], wend[cut], across), 0.0)
            added = dot3(
                jnp.concatenate([pulled[cut], v[cut]], axis=0),
                jnp.concatenate([wend[cut], kend[cut]], axis=0),
                across,
            )
            added = jnp.where(same_head, added, 0.0)
            moved = state * gain[first : first + 1] + dot3(state, step)
            state = jnp.concatenate([moved[:width], moved[width:] + added], axis=0)
    pair_ref[0] = state


def finish_kernel(head_size, local_ref, carried_ref, state_ref, gain_ref, out_ref):
    width = local_ref.shape[1]
    row_w = lax.broadcasted_iota(jnp.int32, (width, width), 0)
    col_w = lax.broadcasted_iota(jnp.int32, (width, width), 1)
    same_head = (row_w // head_size) == (col_w // head_size)
    average = jnp.where(same_head, 1.0 / head_size, 0.0)
    y = local_ref[...] + dot3t(carried_ref[...], state_ref[0])
    centred = y - exact(y, average)
    variance = exact(centred * centred, average)
    out_ref[...] = (centred * lax.rsqrt(variance + GROUP_EPSILON) * gain_ref[...]).astype(jnp.bfloat16)


def from_behind(value, axis, steps):
    count = lax.axis_size(axis)
    initial, last = (max(0, -steps), min(count, count - steps))
    return lax.ppermute(value, axis, [(source, source + steps) for source in range(initial, last)])


def head_blocks(pairs, head_size):
    width = pairs.shape[-1]
    return jnp.stack(
        [pairs[:, a : a + head_size, a : a + head_size] for a in range(0, width, head_size)], axis=1
    )


def delta_rule(query, key, value, decay_pre, rate_pre, factor, share, gain):
    rows, channels = query.shape
    heads = factor.shape[1]
    head_size = channels // heads
    per = math.gcd(heads, max(1, 128 // head_size))
    width, pairs = per * head_size, heads // per
    block = math.gcd(rows, 128)
    chunk = math.gcd(block, 16)
    wide = pl.BlockSpec((rows, width), lambda i: (0, i))
    whole = pl.BlockSpec((rows, heads), lambda i: (0, 0))
    local, carried, pair = pl.pallas_call(
        functools.partial(delta_kernel, head_size, chunk, block),
        grid=(pairs,),
        in_specs=[wide] * 5 + [whole] * 2,
        out_specs=[wide, wide, pl.BlockSpec((1, 2 * width, width), lambda i: (i, 0, 0))],
        out_shape=[
            jax.ShapeDtypeStruct((rows, channels), jnp.float32),
            jax.ShapeDtypeStruct((rows, channels), jnp.float32),
            jax.ShapeDtypeStruct((pairs, 2 * width, width), jnp.float32),
        ],
        cost_estimate=pl.CostEstimate(
            flops=pairs * rows * width * width * 60, bytes_accessed=rows * channels * 32, transcendentals=rows * channels * 10
        ),
        name="delta_chunks",
    )(query, key, value, decay_pre, rate_pre, factor, share)

    phi, psi = head_blocks(pair[:, :width], head_size), head_blocks(pair[:, width:], head_size)
    both = jnp.concatenate([phi, psi], axis=-2).reshape(heads, 2 * head_size, head_size)
    count, place = lax.axis_size("sp"), lax.axis_index("sp")
    steps = 1
    while steps < count - 1:
        earlier = from_behind(both, "sp", steps)
        new = exact_mul("hcd,hde->hce", earlier, both[:, :head_size])
        new = new + jnp.concatenate([jnp.zeros_like(both[:, :head_size]), both[:, head_size:]], axis=1)
        both = jnp.where(place >= steps, new, both)
        steps *= 2
    state = from_behind(both[:, head_size:], "sp", 1).reshape(pairs, per, head_size, head_size)
    same = jnp.eye(per, dtype=jnp.float32)
    state = (state[:, :, :, None, :] * same[None, :, None, :, None]).reshape(pairs, width, width)
    return pl.pallas_call(
        functools.partial(finish_kernel, head_size),
        grid=(pairs,),
        in_specs=[wide, wide, pl.BlockSpec((1, width, width), lambda i: (i, 0, 0)), pl.BlockSpec((1, width), lambda i: (0, i))],
        out_specs=wide,
        out_shape=jax.ShapeDtypeStruct((rows, channels), jnp.bfloat16),
        name="delta_finish",
    )(local, carried, state, gain[None])


def exact_mul(form, left, right):
    return jnp.einsum(form, left, right, precision=HIGHEST)


def gather_kernel(axis, radices, number, *refs):
    ins, outs = refs[:number], refs[number : 2 * number]
    own_sem, far_send, far_recv, near_send, near_recv = refs[2 * number :]
    outer, middle, inner = radices
    me = lax.axis_index(axis)
    x, y, z = me % inner, (me // inner) % middle, me // (inner * middle)

    def index(z_at, y_at, x_at):
        return (z_at * middle + y_at) * inner + x_at

    far = [index((z + step) % outer, y, x) for step in range(1, outer)]
    near = {}
    if inner == 2:
        near["x"] = index(z, y, 1 - x)
    if middle == 2:
        near["y"] = index(z, 1 - y, x)
    barrier = pltpu.get_barrier_semaphore()
    peers = far + list(near.values())
    for peer in peers:
        pl.semaphore_signal(barrier, inc=1, device_id={axis: peer}, device_id_type=MESH)
    pl.semaphore_wait(barrier, len(peers))

    def far_copy(w, step, to, z_from):
        return pltpu.make_async_remote_copy(
            src_ref=ins[w],
            dst_ref=outs[w].at[z_from, y, x],
            send_sem=far_send.at[w, step],
            recv_sem=far_recv.at[w, step],
            device_id={axis: to},
            device_id_type=MESH,
        )

    own = [pltpu.make_async_copy(ins[w], outs[w].at[z, y, x], own_sem.at[w]) for w in range(number)]
    for w in range(number):
        own[w].start()
        for step in range(outer - 1):
            far_copy(w, step, far[step], z).start()

    def region(w, order, stage, from_y, from_x):
        if stage == 0:
            return outs[w].at[:, from_y, from_x]
        return outs[w].at[:, from_y] if order[0] == "x" else outs[w].at[:, :, from_x]

    def near_copy(w, order, stage, from_y, from_x):
        part = region(w, order, stage, from_y, from_x)
        return pltpu.make_async_remote_copy(
            src_ref=part,
            dst_ref=part,
            send_sem=near_send.at[w, stage],
            recv_sem=near_recv.at[w, stage],
            device_id={axis: near[order[stage]]},
            device_id_type=MESH,
        )

    def theirs(w, order, stage):
        from_y, from_x = (y, 1 - x) if order[stage] == "x" else (1 - y, x)
        return near_copy(w, order, stage, from_y, from_x)

    names = list(near)
    orders = [names if w % 2 == 0 else names[::-1] for w in range(number)]

    def advance(w, stage):
        if stage == 0:
            own[w].wait()
            for step in range(outer - 1):
                far_copy(w, step, far[step], (z + outer - step - 1) % outer).wait_recv()
        else:
            theirs(w, orders[w], stage - 1).wait_recv()
        if stage < len(names):
            near_copy(w, orders[w], stage, y, x).start()

    last = len(names)
    for tick in range(number + last):
        for stage in range(last, -1, -1):
            w = tick - stage
            if 0 <= w < number:
                advance(w, stage)
    for w in range(number):
        for step in range(outer - 1):
            far_copy(w, step, far[step], z).wait_send()
        for stage in range(last):
            near_copy(w, orders[w], stage, y, x).wait_send()


def gather_rows(arrays, axis, number_id=0):
    count, number = lax.axis_size(axis), len(arrays)
    inner = math.gcd(count, 2)
    middle = math.gcd(count // inner, 2)
    radices = (count // inner // middle, middle, inner)
    outs = pl.pallas_call(
        functools.partial(gather_kernel, axis, radices, number),
        in_specs=[pl.BlockSpec(memory_space=pltpu.VMEM)] * number,
        out_specs=[pl.BlockSpec(memory_space=pl.ANY)] * number,
        out_shape=[jax.ShapeDtypeStruct(radices + item.shape, item.dtype) for item in arrays],
        scratch_shapes=[
            pltpu.SemaphoreType.DMA((number,)),
            pltpu.SemaphoreType.DMA((number, max(1, radices[0] - 1))),
            pltpu.SemaphoreType.DMA((number, max(1, radices[0] - 1))),
            pltpu.SemaphoreType.DMA((number, 2)),
            pltpu.SemaphoreType.DMA((number, 2)),
        ],
        compiler_params=pltpu.CompilerParams(collective_id=number_id, has_side_effects=True),
        cost_estimate=pl.CostEstimate(
            flops=10**9, bytes_accessed=sum(item.size for item in arrays) * 2 * count, transcendentals=0
        ),
        name="gather_rows",
    )(*arrays)
    return [out.reshape((-1,) + item.shape[1:]) for out, item in zip(outs, arrays)]


def plain_body(
    tokens,
    input_norm_gain,
    query_matrix,
    key_matrix,
    value_matrix,
    convolution_value_matrix,
    convolution_gate_matrix,
    decay_offset_channel,
    decay_first_matrix,
    decay_second_matrix,
    learning_rate_offset,
    learning_rate_first_matrix,
    learning_rate_second_matrix,
    forgetting_rate_factor,
    state_retention_share,
    per_head_norm_gain,
    convolution_filter_taps,
    convolution_channel_gain,
    attention_output_matrix,
    convolution_output_matrix,
):
    tok_rows = tokens.shape[0]
    widened = tokens.astype(jnp.float32)
    normed = (
        widened
        * lax.rsqrt(jnp.mean(widened * widened, axis=-1, keepdims=True) + RMS_EPSILON)
        * input_norm_gain
    ).astype(jnp.bfloat16)
    pieces = (
        *gather_rows((query_matrix, key_matrix, value_matrix), "sp"),
        lax.all_gather(convolution_value_matrix, "sp", axis=0, tiled=True),
        lax.all_gather(convolution_gate_matrix, "sp", axis=0, tiled=True),
    )
    query_proj, key_proj, value_proj, conv_value, conv_gate = tuple(
        (jnp.dot(normed, piece, preferred_element_type=jnp.float32) for piece in pieces)
    )
    decay_mid = jnp.tanh(
        jnp.dot(normed, decay_first_matrix, preferred_element_type=jnp.float32)
    ).astype(jnp.bfloat16)
    rate_mid = jnp.dot(
        normed, learning_rate_first_matrix, preferred_element_type=jnp.float32
    ).astype(jnp.bfloat16)
    decay_pre = decay_offset_channel + jnp.dot(
        decay_mid, decay_second_matrix, preferred_element_type=jnp.float32
    )
    rate_pre = learning_rate_offset + jnp.dot(
        rate_mid, learning_rate_second_matrix, preferred_element_type=jnp.float32
    )
    state_mixed = delta_rule(
        query_proj, key_proj, value_proj, decay_pre, rate_pre,
        forgetting_rate_factor, state_retention_share, per_head_norm_gain,
    )
    gated = (conv_value * jax.nn.sigmoid(conv_gate)).astype(jnp.bfloat16)
    span = convolution_filter_taps.shape[0]
    rim = from_behind(gated[tok_rows - (span - 1) :], "sp", 1)
    padded = jnp.concatenate([rim, gated], axis=0)
    filtered = jnp.zeros(gated.shape, jnp.float32)
    for offset in range(span):
        filtered = filtered + convolution_filter_taps[offset] * padded[offset : offset + tok_rows]
    total_sum, total_square = lax.psum(
        (jnp.sum(filtered, axis=-1), jnp.sum(filtered * filtered, axis=-1)), "tp"
    )
    conv_channels = filtered.shape[1] * lax.axis_size("tp")
    row_mean = total_sum / conv_channels
    deviation = filtered - row_mean[:, None]
    variance = total_square / conv_channels - row_mean * row_mean
    conv_mixed = jax.nn.silu(
        deviation * lax.rsqrt(variance + LAYER_EPSILON)[:, None] * convolution_channel_gain
    ).astype(jnp.bfloat16)
    contract_dims = (((1,), (1,)), ((), ()))
    pieces = lax.all_gather(
        (attention_output_matrix, convolution_output_matrix), "sp", axis=0, tiled=True
    )
    partial_out = lax.dot_general(
        state_mixed, pieces[0], contract_dims, preferred_element_type=jnp.float32
    ) + lax.dot_general(conv_mixed, pieces[1], contract_dims, preferred_element_type=jnp.float32)
    partial_out = partial_out.astype(jnp.bfloat16)
    if lax.axis_size("tp") != 2:
        return lax.psum(partial_out, "tp")
    other = lax.ppermute(partial_out, "tp", [(0, 1), (1, 0)])
    return (partial_out.astype(jnp.float32) + other.astype(jnp.float32)).astype(jnp.bfloat16)


def radices_of(axis):
    count = lax.axis_size(axis)
    inner = math.gcd(count, 2)
    middle = math.gcd(count // inner, 2)
    return count // inner // middle, middle, inner


def place_of(axis, radices):
    outer, middle, inner = radices
    me = lax.axis_index(axis)
    return me // (inner * middle), (me // inner) % middle, me % inner


def greet(devices):
    barrier = pltpu.get_barrier_semaphore()
    for device in devices:
        pl.semaphore_signal(barrier, inc=1, device_id=device, device_id_type=MESH)
    pl.semaphore_wait(barrier, len(devices))


def spread_kernel(axis, pair_axis, radices, widths, placed, firsts, early, head_size, chunk, block, *refs):
    number = len(widths)
    raw_ref, gain_ref, side_ref, ins = refs[0], refs[1], refs[2], refs[3 : 3 + number]
    refs = refs[3 + number :]
    extra, (decay_ref, rate_ref, decay_offset_ref, rate_offset_ref) = refs[: len(firsts)], refs[len(firsts) : len(firsts) + 4]
    refs = refs[len(firsts) + 4 :]
    kinds = 1 + max(out for out, _ in placed)
    tokens_all, local_ref, carried_ref, pair_ref = refs[:4]
    later, refs = refs[4 : 3 + kinds], refs[3 + kinds :]
    (first_out, tokens_out, side_out, tokens_ref, proj, mats, adds, hist, queries,
     first_sem, own_sem, far_send, far_recv, near_send, near_recv, side_send, side_recv,
     tok_send, tok_recv, sib_send, sib_recv) = refs
    outs = [first_out, *later]
    outer, middle, inner = radices
    z, y, x = place_of(axis, radices)
    core = lax.axis_index(pair_axis)
    widened = raw_ref[...].astype(jnp.float32)
    scale = lax.rsqrt(jnp.mean(widened * widened, axis=-1, keepdims=True) + RMS_EPSILON)
    tokens_ref[...] = (widened * scale * gain_ref[...]).astype(jnp.bfloat16)
    half = tokens_ref.shape[0] // 2
    mine, other = pl.ds(pl.multiple_of(core * half, half), half), pl.ds(pl.multiple_of((1 - core) * half, half), half)

    def index(z_at, y_at, x_at):
        return (z_at * middle + y_at) * inner + x_at

    far = [(z + step) % outer for step in range(1, outer)]
    near = {"x": index(z, y, 1 - x), "y": index(z, 1 - y, x)}
    greet(
        [{axis: index(at, y, x)} for at in far]
        + [{axis: peer} for peer in near.values()]
        + [{pair_axis: 1 - core}]
    )

    def part(w, at):
        return ins[w].at[:, pl.ds(pl.multiple_of(at * widths[w], widths[w]), widths[w])]

    def slot(w, *where, cut=slice(None)):
        out, offset = placed[w]
        return outs[out].at[(*where, cut, pl.ds(offset, widths[w]))]

    def far_copy(w, step, to, z_from):
        return pltpu.make_async_remote_copy(
            src_ref=part(w, to), dst_ref=slot(w, z_from, y, x),
            send_sem=far_send.at[w, step], recv_sem=far_recv.at[w, step],
            device_id={axis: index(to, y, x)}, device_id_type=MESH,
        )

    def side_copy(step, to, z_from):
        return pltpu.make_async_remote_copy(
            src_ref=side_ref, dst_ref=side_out.at[z_from],
            send_sem=side_send.at[step], recv_sem=side_recv.at[step],
            device_id={axis: index(to, y, x)}, device_id_type=MESH,
        )

    names = list(near)
    depth = ins[0].shape[0]
    orders = [names, names[::-1]]

    def near_copy(w, part_at, stage, y_at, x_at):
        order = orders[part_at]
        cut = pl.ds(part_at * (depth // 2), depth // 2)
        if stage == 0:
            region = slot(w, slice(None), y_at, x_at, cut=cut)
        elif order[0] == "x":
            region = slot(w, slice(None), y_at, slice(None), cut=cut)
        else:
            region = slot(w, slice(None), slice(None), x_at, cut=cut)
        return pltpu.make_async_remote_copy(
            src_ref=region, dst_ref=region,
            send_sem=near_send.at[w, part_at, stage], recv_sem=near_recv.at[w, part_at, stage],
            device_id={axis: near[order[stage]]}, device_id_type=MESH,
        )

    def theirs(w, part_at, stage):
        y_at, x_at = (y, 1 - x) if orders[part_at][stage] == "x" else (1 - y, x)
        return near_copy(w, part_at, stage, y_at, x_at)

    def inside(at):
        return (at >= 0) & (at < outer)

    ways = (1, -1)

    def token_copy(way, step, block, source):
        return pltpu.make_async_remote_copy(
            src_ref=source, dst_ref=tokens_out.at[block, mine],
            send_sem=tok_send.at[way, step], recv_sem=tok_recv.at[way, step],
            device_id={axis: index((z + ways[way] + outer) % outer, y, x)}, device_id_type=MESH,
        )

    def sibling_copy(way, step, block, rows):
        return pltpu.make_async_remote_copy(
            src_ref=tokens_out.at[block, rows], dst_ref=tokens_out.at[block, rows],
            send_sem=sib_send.at[way, step], recv_sem=sib_recv.at[way, step],
            device_id={pair_axis: 1 - core}, device_id_type=MESH,
        )

    def arrived(way, step):
        return z - ways[way] * (step + 1)

    def sends(way, step):
        return inside(z + ways[way]) & inside(z - ways[way] * step)

    own = [pltpu.make_async_copy(part(w, z), slot(w, z, y, x), own_sem.at[w]) for w in range(number)]
    own.append(pltpu.make_async_copy(tokens_ref, tokens_out.at[z], own_sem.at[number]))
    own.append(pltpu.make_async_copy(side_ref, side_out.at[z], own_sem.at[number + 1]))
    for step in range(outer - 1):
        side_copy(step, far[step], z).start()
    def send_far(some):
        for w in some:
            own[w].start()
            for step in range(outer - 1):
                far_copy(w, step, far[step], z).start()

    send_far(early)
    for way in range(2):
        @pl.when(sends(way, 0))
        def _():
            token_copy(way, 0, z, tokens_ref.at[mine]).start()
    own[number].start()
    own[number + 1].start()
    kept = []
    for item, (out, offset) in enumerate(firsts):
        for at in range(outer * middle * inner):
            where = (at // (middle * inner), (at // inner) % middle, at % inner)
            kept.append(pltpu.make_async_copy(
                extra[item].at[at * depth : (at + 1) * depth],
                outs[out].at[(*where, slice(None), pl.ds(offset, extra[item].shape[1]))],
                first_sem.at[item, at],
            ))
            kept[-1].start()

    def advance(w, stage):
        if stage == 0:
            own[w].wait()
            for step in range(outer - 1):
                far_copy(w, step, far[step], (z + outer - step - 1) % outer).wait_recv()
        for part_at in range(2):
            if stage:
                theirs(w, part_at, stage - 1).wait_recv()
            if stage < len(names):
                near_copy(w, part_at, stage, y, x).start()

    def token_step(step):
        for way in range(2):
            block = arrived(way, step)
            @pl.when(inside(block))
            def _():
                token_copy(way, step, block, tokens_out.at[block, mine]).wait_recv()
                @pl.when(sends(way, step + 1) & (step + 1 < outer - 1))
                def _():
                    token_copy(way, step + 1, block, tokens_out.at[block, mine]).start()
                sibling_copy(way, step, block, mine).start()

    last = len(names)

    def sibling_step(step):
        for way in range(2):
            block = arrived(way, step)
            @pl.when(inside(block))
            def _():
                sibling_copy(way, step, block, other).wait_recv()

    def run(some):
        for tick in range(len(some) + last):
            for stage in range(last + 1):
                if 0 <= tick - stage < len(some):
                    advance(some[tick - stage], stage)

    run(early)
    own[number].wait()
    own[number + 1].wait()
    for item in kept:
        item.wait()
    for step in range(outer - 1):
        side_copy(step, far[step], (z + outer - step - 1) % outer).wait_recv()
    token_step(0)
    rest = [[w for w in range(number) if placed[w][0] == out] for out in range(1, kinds)]
    one_block, chain, read = delta_phases(
        z, head_size, chunk, block, proj, side_out, decay_ref, rate_ref, decay_offset_ref, rate_offset_ref,
        local_ref, carried_ref, pair_ref, mats, adds, hist, queries,
    )
    pieces = tokens_ref.shape[0] // block
    edge = jnp.minimum(z, outer - 1 - z)
    toward = jnp.where(z < outer // 2, -1, 1)
    piece_depth = middle * inner * depth

    def project(group):
        total = None
        for part_at in range(outer):
            matrix = first_out[part_at].reshape(piece_depth, first_out.shape[-1])
            term = jnp.dot(
                tokens_out[group, :, part_at * piece_depth : (part_at + 1) * piece_depth], matrix,
                preferred_element_type=jnp.float32,
            )
            total = term if total is None else total + term
        proj[...] = total

    def one_round(k, carry):
        twosided = k <= 2 * edge
        distance = jnp.where(twosided, (k + 1) // 2, k - edge)
        side = jnp.where(twosided & (k % 2 == 1), toward, -toward)
        group = z + side * distance

        @pl.when(k > 0)
        def _():
            sibling_step(k - 1)

        project(group)
        for piece in range(pieces):
            one_block(group, piece)
            if piece == 0:
                @pl.when((k > 0) & (k < outer - 1))
                def _():
                    token_step(k)

                for at, some in enumerate(rest):
                    @pl.when(k == at)
                    def _():
                        send_far(some)

                    for stage in range(last):
                        @pl.when(k == at + 2 + stage)
                        def _():
                            for w in some:
                                advance(w, stage)
        return carry

    lax.fori_loop(0, outer, one_round, 0)
    keep_tokens = pltpu.make_async_copy(tokens_out, tokens_all, own_sem.at[number + 2])
    keep_tokens.start()
    chain()
    for at, some in enumerate(rest):
        for stage in range(last + 1):
            if at + 2 + stage >= outer and stage < last:
                for w in some:
                    advance(w, stage)
    read()
    for some in rest:
        for w in some:
            advance(w, last)
    keep_tokens.wait()
    for step in range(outer - 1):
        side_copy(step, far[step], z).wait_send()
    for step in range(outer - 1):
        for way in range(2):
            block = arrived(way, step)
            @pl.when(inside(block))
            def _():
                sibling_copy(way, step, block, mine).wait_send()
            @pl.when(sends(way, step))
            def _():
                token_copy(way, step, z - ways[way] * step, tokens_ref.at[mine]).wait_send()
    for w in range(number):
        for step in range(outer - 1):
            far_copy(w, step, far[step], z).wait_send()
        for stage in range(last):
            for part_at in range(2):
                near_copy(w, part_at, stage, y, x).wait_send()


def spread(tokens, gain, side, weights, groups, firsts, maps, head_size, axis, pair_axis):
    radices = radices_of(axis)
    outer, number = radices[0], len(weights)
    widths = [item.shape[1] // outer for item in weights]
    placed, totals = [None] * number, []
    for out, members in enumerate(groups):
        offset = 0
        for w in members:
            placed[w] = (out, offset)
            offset += widths[w]
        totals.append(offset)
    extras, width = [], widths[0]
    for item in firsts:
        extras.append((0, totals[0]))
        totals[0] += item.shape[1]
    depth, rows = weights[0].shape[0], tokens.shape[0]
    block = math.gcd(rows, 128)
    chunk = math.gcd(block, 32)
    total = outer * rows
    vmem, hbm = pl.BlockSpec(memory_space=pltpu.VMEM), pl.BlockSpec(memory_space=pl.ANY)
    outs = pl.pallas_call(
        functools.partial(
            spread_kernel, axis, pair_axis, radices, widths, placed, extras, groups[0], head_size, chunk, block
        ),
        in_specs=[vmem] * (3 + number + len(firsts) + len(maps)),
        out_specs=[hbm] + [vmem] * 3 + [hbm] * (len(groups) - 1),
        out_shape=[
            jax.ShapeDtypeStruct((outer,) + tokens.shape, tokens.dtype),
            jax.ShapeDtypeStruct((total, width), jnp.float32),
            jax.ShapeDtypeStruct((total, width), jnp.float32),
            jax.ShapeDtypeStruct((outer, width, width), jnp.float32),
        ]
        + [jax.ShapeDtypeStruct(radices + (depth, size), weights[0].dtype) for size in totals[1:]],
        scratch_shapes=[
            pltpu.VMEM(radices + (depth, totals[0]), weights[0].dtype),
            pltpu.VMEM((outer,) + tokens.shape, tokens.dtype),
            pltpu.VMEM((outer,) + side.shape, side.dtype),
            pltpu.VMEM(tokens.shape, tokens.dtype),
            pltpu.VMEM((rows, totals[0]), jnp.float32),
        ]
        + [pltpu.VMEM((total // chunk, width, width), jnp.float32)] * 3
        + [
            pltpu.VMEM((total, width), jnp.float32),
            pltpu.SemaphoreType.DMA((len(firsts), math.prod(radices))),
            pltpu.SemaphoreType.DMA((number + 3,)),
            pltpu.SemaphoreType.DMA((number, outer - 1)),
            pltpu.SemaphoreType.DMA((number, outer - 1)),
            pltpu.SemaphoreType.DMA((number, 2, 2)),
            pltpu.SemaphoreType.DMA((number, 2, 2)),
            pltpu.SemaphoreType.DMA((outer - 1,)),
            pltpu.SemaphoreType.DMA((outer - 1,)),
            pltpu.SemaphoreType.DMA((2, outer - 1)),
            pltpu.SemaphoreType.DMA((2, outer - 1)),
            pltpu.SemaphoreType.DMA((2, outer - 1)),
            pltpu.SemaphoreType.DMA((2, outer - 1)),
        ],
        compiler_params=pltpu.CompilerParams(collective_id=0, has_side_effects=True, vmem_limit_bytes=60 * 2**20),
        cost_estimate=pl.CostEstimate(flops=10**10, bytes_accessed=8 * tokens.size * outer, transcendentals=0),
        name="spread_and_delta",
    )(tokens, gain, side, *weights, *firsts, *maps)
    return outs[:4], [out.reshape(-1, size) for out, size in zip(outs[4:], totals[1:])]


def spread_sum(values, matrix):
    top, rest = split(values)
    return jnp.dot(top, matrix, preferred_element_type=jnp.float32) + jnp.dot(
        rest, matrix, preferred_element_type=jnp.float32
    )


def states_kernel(
    axis, pair_axis, radices, head_size,
    pair_ref, sums_ref, local_ref, carried_ref, gain_ref,
    mixed_ref, totals_ref,
    held, stats, own_sem, pair_send, pair_recv, stat_send, stat_recv,
):
    outer, middle, inner = radices
    planes = middle * inner
    z, y, x = place_of(axis, radices)
    place = y * inner + x
    core = lax.axis_index(pair_axis)
    width = pair_ref.shape[-1]
    rows = local_ref.shape[0] // outer
    plane_peers = [(place + step) % planes for step in range(1, planes)]
    cores = lax.axis_size(pair_axis)
    lines = [(dz, dc) for dz in range(outer) for dc in range(cores) if dz or dc]

    def line_device(dz, dc):
        return {axis: ((z + dz) % outer) * planes + place, pair_axis: (core + dc) % cores}

    greet([{axis: z * planes + peer} for peer in plane_peers] + [line_device(*line) for line in lines])

    def pair_copy(step, p_from):
        return pltpu.make_async_remote_copy(
            src_ref=pair_ref, dst_ref=held.at[p_from],
            send_sem=pair_send.at[step], recv_sem=pair_recv.at[step],
            device_id={axis: z * planes + plane_peers[step]}, device_id_type=MESH,
        )

    def stat_copy(number, slot):
        return pltpu.make_async_remote_copy(
            src_ref=sums_ref, dst_ref=stats.at[slot],
            send_sem=stat_send.at[number], recv_sem=stat_recv.at[number],
            device_id=line_device(*lines[number]), device_id_type=MESH,
        )

    for step in range(planes - 1):
        pair_copy(step, place).start()
    for number in range(len(lines)):
        stat_copy(number, number).start()
    own = pltpu.make_async_copy(pair_ref, held.at[place], own_sem.at[0])
    own.start()

    for number in range(len(lines)):
        stat_copy(number, number).wait_recv()
    totals = sums_ref[...]
    for number in range(len(lines)):
        totals = totals + stats[number]
    totals_ref[...] = totals

    own.wait()
    for step in range(planes - 1):
        pair_copy(step, (place + planes - step - 1) % planes).wait_recv()

    row = lax.broadcasted_iota(jnp.int32, (width, width), 0)
    lane = lax.broadcasted_iota(jnp.int32, (width, width), 1)
    average = jnp.where((row // head_size) == (lane // head_size), 1.0 / head_size, 0.0).astype(jnp.bfloat16)
    first_head, moves = row < head_size, lane < head_size

    def step_matrix(item):
        part = jnp.where(moves, item, 0.0)
        return jnp.where(first_head, part, pltpu.roll(part, head_size, 1))

    def state_matrix(item):
        part = jnp.where(moves, 0.0, item)
        return jnp.where(first_head, pltpu.roll(part, head_size, 1), part)

    def compose(earlier, later):
        return dot3(step_matrix(later), earlier) + jnp.where(moves, 0.0, later)

    nothing = jnp.where(moves & (row % head_size == lane), 1.0, 0.0)
    before, whole = [], []
    for block in range(outer):
        total, keep = held[0, block], nothing
        for p in range(1, planes):
            keep = jnp.where(place == p, total, keep)
            total = compose(total, held[p, block])
        before.append(keep)
        whole.append(total)
    state = jnp.zeros((width, width), jnp.float32)
    for block in range(outer):
        cut = slice(block * rows, (block + 1) * rows)
        full = local_ref[cut] + dot3(carried_ref[cut], state_matrix(compose(state, before[block])))
        if block + 1 < outer:
            state = compose(state, whole[block])
        centred = full - spread_sum(full, average)
        variance = spread_sum(centred * centred, average)
        mixed_ref[cut] = (centred * lax.rsqrt(variance + GROUP_EPSILON) * gain_ref[...]).astype(jnp.bfloat16)

    for step in range(planes - 1):
        pair_copy(step, place).wait_send()
    for number in range(len(lines)):
        stat_copy(number, number).wait_send()


def states(pair, sums, local, carried, gain, head_size, axis, pair_axis):
    radices = radices_of(axis)
    planes, cores = radices[1] * radices[2], lax.axis_size(pair_axis)
    lines = radices[0] * cores - 1
    vmem = pl.BlockSpec(memory_space=pltpu.VMEM)
    return pl.pallas_call(
        functools.partial(states_kernel, axis, pair_axis, radices, head_size),
        in_specs=[vmem] * 5,
        out_specs=[vmem] * 2,
        out_shape=[jax.ShapeDtypeStruct(local.shape, jnp.bfloat16), jax.ShapeDtypeStruct(sums.shape, jnp.float32)],
        scratch_shapes=[
            pltpu.VMEM((planes,) + pair.shape, jnp.float32),
            pltpu.VMEM((lines,) + sums.shape, jnp.float32),
            pltpu.SemaphoreType.DMA((1,)),
            pltpu.SemaphoreType.DMA((planes - 1,)),
            pltpu.SemaphoreType.DMA((planes - 1,)),
            pltpu.SemaphoreType.DMA((lines,)),
            pltpu.SemaphoreType.DMA((lines,)),
        ],
        compiler_params=pltpu.CompilerParams(collective_id=1, has_side_effects=True),
        cost_estimate=pl.CostEstimate(flops=10**9, bytes_accessed=pair.size * 16, transcendentals=0),
        name="carry_states",
    )(pair, sums, local, carried, gain)


def reduce_kernel(
    axis, pair_axis, radices,
    state_ref, conv_ref, matrix_ref, out_ref,
    keep, twin_out, twin_in, chain_out, chain_in,
    twin_send, twin_recv, chain_send, chain_recv, last_send, last_recv,
):
    outer, middle, inner = radices
    z, y, x = place_of(axis, radices)
    core = lax.axis_index(pair_axis)
    rows, half = keep.shape[1:]
    split_at = state_ref.shape[1]
    ways = (1, -1)

    def index(z_at):
        return (z_at * middle + y) * inner + x

    def inside(at):
        return (at >= 0) & (at < outer)

    greet([{axis: index((z + step) % outer)} for step in range(1, outer)] + [{pair_axis: 1 - core}])

    def twin_copy(block):
        return pltpu.make_async_remote_copy(
            src_ref=twin_out.at[block], dst_ref=twin_in.at[block],
            send_sem=twin_send.at[block], recv_sem=twin_recv.at[block],
            device_id={pair_axis: 1 - core}, device_id_type=MESH,
        )

    def chain_copy(way, steps):
        return pltpu.make_async_remote_copy(
            src_ref=chain_out.at[way, steps - 1], dst_ref=chain_in.at[way, steps - 1],
            send_sem=chain_send.at[way, steps - 1], recv_sem=chain_recv.at[way, steps - 1],
            device_id={axis: index((z + ways[way] + outer) % outer)}, device_id_type=MESH,
        )

    def product(block, side):
        cut = pl.ds(pl.multiple_of(block * rows, rows), rows)
        these = pl.ds(pl.multiple_of(side * half, half), half)
        dims = (((1,), (1,)), ((), ()))
        return lax.dot_general(
            state_ref[cut, :], matrix_ref[these, :split_at], dims, preferred_element_type=jnp.float32
        ) + lax.dot_general(
            conv_ref[cut, :], matrix_ref[these, split_at:], dims, preferred_element_type=jnp.float32
        )

    def one_block(number, carry):
        block = jnp.where(z < outer // 2, outer - 1 - number, number)
        twin_out[block] = product(block, 1 - core).astype(jnp.bfloat16)
        twin_copy(block).start()
        keep[block] = product(block, core)
        return carry

    lax.fori_loop(0, outer, one_block, 0)

    for steps in range(outer - 1, 0, -1):
        for way in range(2):
            block = z + ways[way] * steps

            @pl.when(inside(block))
            def _():
                twin_copy(block).wait_recv()
                keep[block] += twin_in[block].astype(jnp.float32)
                if steps + 1 < outer:
                    @pl.when(inside(z - ways[way]))
                    def _():
                        chain_copy(way, steps + 1).wait_recv()
                        keep[block] += chain_in[way, steps].astype(jnp.float32)
                chain_out[way, steps - 1] = keep[block].astype(jnp.bfloat16)
                chain_copy(way, steps).start()

    twin_copy(z).wait_recv()
    keep[z] += twin_in[z].astype(jnp.float32)
    for way in range(2):
        @pl.when(inside(z - ways[way]))
        def _():
            chain_copy(way, 1).wait_recv()
            keep[z] += chain_in[way, 0].astype(jnp.float32)

    ours = pl.ds(pl.multiple_of(core * half, half), half)
    out_ref[:, ours] = keep[z].astype(jnp.bfloat16)

    def last_copy(side):
        place = out_ref.at[:, pl.ds(pl.multiple_of(side * half, half), half)]
        return pltpu.make_async_remote_copy(
            src_ref=place, dst_ref=place, send_sem=last_send.at[0], recv_sem=last_recv.at[0],
            device_id={pair_axis: 1 - core}, device_id_type=MESH,
        )

    last_copy(core).start()
    for block in range(outer):
        twin_copy(block).wait_send()
    for steps in range(outer - 1, 0, -1):
        for way in range(2):
            @pl.when(inside(z + ways[way] * steps))
            def _():
                chain_copy(way, steps).wait_send()
    last_copy(1 - core).wait_recv()
    last_copy(core).wait_send()


def reduce_rows(state_mixed, conv_mixed, matrix, outer, axis, pair_axis):
    radices = radices_of(axis)
    rows, half = state_mixed.shape[0] // outer, matrix.shape[0] // 2
    vmem = pl.BlockSpec(memory_space=pltpu.VMEM)
    slots = (2, outer - 1)
    return pl.pallas_call(
        functools.partial(reduce_kernel, axis, pair_axis, radices),
        in_specs=[vmem] * 3,
        out_specs=vmem,
        out_shape=jax.ShapeDtypeStruct((rows, 2 * half), jnp.bfloat16),
        scratch_shapes=[
            pltpu.VMEM((outer, rows, half), jnp.float32),
            pltpu.VMEM((outer, rows, half), jnp.bfloat16),
            pltpu.VMEM((outer, rows, half), jnp.bfloat16),
            pltpu.VMEM(slots + (rows, half), jnp.bfloat16),
            pltpu.VMEM(slots + (rows, half), jnp.bfloat16),
            pltpu.SemaphoreType.DMA((outer,)),
            pltpu.SemaphoreType.DMA((outer,)),
            pltpu.SemaphoreType.DMA(slots),
            pltpu.SemaphoreType.DMA(slots),
            pltpu.SemaphoreType.DMA((1,)),
            pltpu.SemaphoreType.DMA((1,)),
        ],
        compiler_params=pltpu.CompilerParams(collective_id=2, has_side_effects=True, vmem_limit_bytes=60 * 2**20),
        cost_estimate=pl.CostEstimate(flops=10**9, bytes_accessed=matrix.size * 8, transcendentals=0),
        name="reduce_rows",
    )(state_mixed, conv_mixed, matrix)


def dotp(left, right, passes, dims=((1,), (0,))):
    def one(p, q):
        return lax.dot_general(p, q, (dims, ((), ())), preferred_element_type=jnp.float32)

    if passes == 1:
        return one(left.astype(jnp.bfloat16), right.astype(jnp.bfloat16))
    (lh, ll), (rh, rl) = split(left), split(right)
    return one(lh, rh) + (one(lh, rl) + one(ll, rh))


GRID_PASSES, SOLVE_PASSES, SEEN_PASSES, STEP_PASSES, CHAIN_PASSES, READ_PASSES = 3, 3, 3, 3, 3, 3


def delta_phases(
    z, head_size, chunk, block,
    proj_ref, side_ref, decay_ref, rate_ref, decay_offset_ref, rate_offset_ref,
    local_ref, carried_ref, pair_ref,
    mats, adds, hist, queries,
):
    groups, _, rows = side_ref.shape
    width = local_ref.shape[1]
    heads = side_ref.shape[1] // 2
    per, pieces = width // head_size, rows // block
    chunks, steps = block // chunk, rows // chunk
    wide = per * block

    def iota(shape, dim):
        return lax.broadcasted_iota(jnp.int32, shape, dim)

    lane_head = iota((1, width), 1) // head_size
    lane_head2 = (iota((1, 2 * width), 1) % width) // head_size
    row_w, col_w = iota((width, width), 0), iota((width, width), 1)
    same_head = (row_w // head_size) == (col_w // head_size)
    ones_head = jnp.where(same_head, 1.0, 0.0).astype(jnp.bfloat16)
    row_b, col_b = iota((block, block), 0), iota((block, block), 1)
    same_chunk = (row_b // chunk) == (col_b // chunk)
    strict = same_chunk & (row_b > col_b)
    incl = same_chunk & (row_b >= col_b)
    sums = jnp.concatenate([jnp.where(incl, 1.0, 0.0), jnp.where(same_chunk, 1.0, 0.0)], axis=0).astype(jnp.bfloat16)
    row_c, col_c = iota((chunk, wide), 0), iota((chunk, wide), 1) % chunk
    eye_c = jnp.where(row_c == col_c, 1.0, 0.0)
    diagonal = (iota((wide, wide), 0) // chunk) == (iota((wide, wide), 1) // chunk)
    spread_rows = (iota((block, wide), 0) // chunk) == ((iota((block, wide), 1) % block) // chunk)
    place = iota((2 * heads, 2 * width), 0)
    chosen = z * per + lane_head2 + jnp.where(iota((1, 2 * width), 1) < width, 0, heads)
    expand = jnp.where(place == chosen, 1.0, 0.0)
    ours = pl.ds(pl.multiple_of(z * width, width), width)
    decay_matrix, rate_matrix = decay_ref[:, ours], rate_ref[:, ours]
    decay_offset, rate_offset = decay_offset_ref[:, ours], rate_offset_ref[:, ours]
    side_row = iota((2 * heads, block), 0)

    def by_head(values, mark):
        return jnp.concatenate([jnp.where(mark == h, values, 0.0) for h in range(per)], axis=0)

    def widen(compact):
        return jnp.where(diagonal, jnp.concatenate([compact] * (wide // chunk), axis=0), 0.0)

    def one_block(group, piece):
        start = pl.multiple_of(group * rows + piece * block, block)
        cut = pl.ds(start, block)
        here = slice(piece * block, (piece + 1) * block)
        q, key, v = proj_ref[here, 0:width], proj_ref[here, width : 2 * width], proj_ref[here, 2 * width : 3 * width]
        inner_width = decay_ref.shape[0]
        mid_at = 3 * width
        decay_mid = jnp.tanh(proj_ref[here, mid_at : mid_at + inner_width]).astype(jnp.bfloat16)
        rate_mid = proj_ref[here, mid_at + inner_width : mid_at + 2 * inner_width].astype(jnp.bfloat16)
        decay_pre = decay_offset + jnp.dot(decay_mid, decay_matrix, preferred_element_type=jnp.float32)
        rate_pre = rate_offset + jnp.dot(rate_mid, rate_matrix, preferred_element_type=jnp.float32)
        thin = side_ref[group, :, piece * block : (piece + 1) * block]
        thin = jnp.where(side_row < heads, thin, jnp.log(thin))
        both = lax.dot_general(
            thin, expand, (((0,), (0,)), ((), ())), precision=HIGHEST, preferred_element_type=jnp.float32
        )
        ld = both[:, width:] - (EXP_HALF * jax.nn.sigmoid(decay_pre)) * both[:, :width]
        learn = jax.nn.sigmoid(rate_pre)
        unit = key * lax.rsqrt(spread_sum(key * key, ones_head) + UNIT_EPSILON)
        er, wr = -unit, unit * learn
        top, rest = split(ld)
        third = (ld - top.astype(jnp.float32) - rest.astype(jnp.float32)).astype(jnp.bfloat16)
        both = jnp.dot(sums, top, preferred_element_type=jnp.float32) + (
            jnp.dot(sums, rest, preferred_element_type=jnp.float32)
            + jnp.dot(sums, third, preferred_element_type=jnp.float32)
        )
        gain, total = both[:block], both[block:]
        mid = 0.5 * total
        up, down, bup = jnp.exp(gain - mid), jnp.exp(mid - gain), jnp.exp(gain - ld - mid)
        left = jnp.concatenate([er * bup, q * up], axis=0)
        what, khat = wr * down, key * down
        right = jnp.concatenate(
            [jnp.where(lane_head == h, item, 0.0) for h in range(per) for item in (what, khat)], axis=0
        )
        grid = dotp(left, right, GRID_PASSES, ((1,), (1,)))

        def piece_of(upper, kind, mask):
            cut_rows = slice(0, block) if upper else slice(block, 2 * block)
            return jnp.concatenate(
                [jnp.where(mask, grid[cut_rows, (2 * h + kind) * block : (2 * h + kind + 1) * block], 0.0) for h in range(per)],
                axis=1,
            )

        ew, ek = piece_of(True, 0, strict), piece_of(True, 1, strict)
        rw, rk = piece_of(False, 0, incl), piece_of(False, 1, incl)
        compact = ew[:chunk]
        for c in range(1, chunks):
            compact = compact + ew[c * chunk : (c + 1) * chunk]
        size = 2
        inv = eye_c + jnp.where((row_c // size == col_c // size) & (row_c > col_c), compact, 0.0)
        while size < chunk:
            off = (row_c // (2 * size) == col_c // (2 * size)) & (row_c // size > col_c // size)
            part = dotp(inv, widen(jnp.where(off, compact, 0.0)), SOLVE_PASSES)
            inv = inv + dotp(part, widen(inv), SOLVE_PASSES)
            size *= 2
        inverse = jnp.where(spread_rows, jnp.concatenate([inv] * chunks, axis=0), 0.0)
        seen = dotp(jnp.concatenate([ek, rk], axis=0), by_head(v, lane_head), SEEN_PASSES)
        eh_full = er * jnp.exp(gain - ld)
        both = jnp.concatenate([seen[:block], eh_full], axis=1)
        both = dotp(inverse, by_head(both, lane_head2), SEEN_PASSES)
        read = dotp(rw, by_head(both, lane_head2), SEEN_PASSES)
        local_ref[cut] = read[:, :width] + seen[block:]
        queries[cut] = q * jnp.exp(gain) + read[:, width:]
        to_end, ends = jnp.exp(total - gain), jnp.exp(total)
        wend, kend = wr * to_end, key * to_end
        zero = jnp.zeros((chunk, width), jnp.float32)
        for c in range(chunks):
            now = slice(c * chunk, (c + 1) * chunk)
            lhs = jnp.concatenate([wend[now], kend[now]], axis=0)
            rhs = jnp.concatenate(
                [
                    jnp.concatenate([both[now, width:], both[now, :width]], axis=1),
                    jnp.concatenate([zero, v[now]], axis=1),
                ],
                axis=0,
            )
            made = dotp(lhs, rhs, STEP_PASSES, ((0,), (0,)))
            number = group * steps + piece * chunks + c
            step = jnp.where(same_head, made[:, :width], 0.0)
            mats[number] = step + jnp.where(row_w == col_w, ends[c * chunk : c * chunk + 1], 0.0)
            added = made[:, width:]
            added = jnp.where(row_w < head_size, pltpu.roll(added, head_size, 1), added)
            adds[number] = jnp.where(col_w < head_size, 0.0, added)

    begin = jnp.where(row_w % head_size == col_w, 1.0, 0.0)

    def one_step(step, carry):
        for group in range(groups):
            number = group * steps + step
            state = pair_ref[group]
            hist[number] = state
            pair_ref[group] = dotp(mats[number], state, CHAIN_PASSES) + adds[number]
        return carry

    def chain():
        for group in range(groups):
            pair_ref[group] = begin
        lax.fori_loop(0, steps, one_step, 0)

    def one_read(group, carry):
        for step in range(steps):
            place_rows = pl.ds(pl.multiple_of(group * rows + step * chunk, chunk), chunk)
            got = dotp(by_head(queries[place_rows], lane_head), hist[group * steps + step], READ_PASSES)
            upper, lower = got[:chunk], got[chunk:]
            carried_ref[place_rows] = jnp.where(lane_head == 0, upper, pltpu.roll(lower, head_size, 1))
            local_ref[place_rows] += jnp.where(lane_head == 0, pltpu.roll(upper, head_size, 1), lower)
        return carry

    return one_block, chain, lambda: lax.fori_loop(0, groups, one_read, 0)


def body(*args):
    outer, middle, inner = radices_of("sp")
    heads, channels = args[13].shape[1], args[2].shape[1]
    width = channels // outer
    fits = (
        lax.axis_size("tp") == 2 and outer > 3 and middle == 2 and inner == 2
        and heads % outer == 0 and width == 128 and args[5].shape[1] % (128 * outer) == 0
    )
    return fast_body(*args) if fits else plain_body(*args)


def fast_body(
    tokens,
    input_norm_gain,
    query_matrix,
    key_matrix,
    value_matrix,
    convolution_value_matrix,
    convolution_gate_matrix,
    decay_offset_channel,
    decay_first_matrix,
    decay_second_matrix,
    learning_rate_offset,
    learning_rate_first_matrix,
    learning_rate_second_matrix,
    forgetting_rate_factor,
    state_retention_share,
    per_head_norm_gain,
    convolution_filter_taps,
    convolution_channel_gain,
    attention_output_matrix,
    convolution_output_matrix,
):
    outer, middle, inner = radices_of("sp")
    planes = middle * inner
    rows = tokens.shape[0]
    heads, channels = forgetting_rate_factor.shape[1], query_matrix.shape[1]
    head_size = channels // heads
    z = lax.axis_index("sp") // planes

    def quarter(value, axis=-1):
        size = value.shape[axis] // outer
        return lax.dynamic_slice_in_dim(value, z * size, size, axis)

    side = jnp.concatenate([forgetting_rate_factor.T, state_retention_share.T], axis=0)
    weights = (
        query_matrix, key_matrix, value_matrix, convolution_value_matrix, convolution_gate_matrix,
        attention_output_matrix, convolution_output_matrix,
    )
    (normed, local, carried, pair), (conv_in, both_out) = spread(
        tokens, input_norm_gain[None], side, weights, ((0, 1, 2), (3, 4), (5, 6)),
        (decay_first_matrix, learning_rate_first_matrix),
        (decay_second_matrix, learning_rate_second_matrix, decay_offset_channel[None], learning_rate_offset[None]),
        head_size, "sp", "tp",
    )
    normed = normed.reshape(-1, normed.shape[-1])

    conv_width = conv_in.shape[1] // 2
    conv_value = jnp.dot(normed, conv_in[:, :conv_width], preferred_element_type=jnp.float32)
    conv_gate = jnp.dot(normed, conv_in[:, conv_width:], preferred_element_type=jnp.float32)
    gated = (conv_value * jax.nn.sigmoid(conv_gate)).astype(jnp.bfloat16).reshape(outer, rows, conv_width)
    span = convolution_filter_taps.shape[0]
    ring = [
        (at * planes + p, at * planes + (p + 1) % planes) for at in range(outer) for p in range(planes)
    ]
    rim = lax.ppermute(gated[:, rows - (span - 1) :], "sp", ring)
    shifted = jnp.concatenate([jnp.zeros_like(rim[:1]), rim[:-1]], axis=0)
    rim = jnp.where(lax.axis_index("sp") % planes == 0, shifted, rim)
    padded = jnp.concatenate([rim, gated], axis=1)
    taps = quarter(convolution_filter_taps)
    filtered = jnp.zeros(gated.shape, jnp.float32)
    for offset in range(span):
        filtered = filtered + taps[offset] * padded[:, offset : offset + rows]
    filtered = filtered.reshape(outer * rows, conv_width)
    sums = jnp.stack([jnp.sum(filtered, axis=-1), jnp.sum(filtered * filtered, axis=-1)])

    state_mixed, totals = states(
        pair, sums, local, carried, quarter(per_head_norm_gain)[None], head_size, "sp", "tp"
    )
    conv_channels = conv_width * outer * lax.axis_size("tp")
    row_mean = totals[0] / conv_channels
    deviation = filtered - row_mean[:, None]
    variance = totals[1] / conv_channels - row_mean * row_mean
    conv_mixed = jax.nn.silu(
        deviation * lax.rsqrt(variance + LAYER_EPSILON)[:, None] * quarter(convolution_channel_gain)
    ).astype(jnp.bfloat16)
    return reduce_rows(state_mixed, conv_mixed, both_out, outer, "sp", "tp")


def solution(mesh):
    return jax.shard_map(
        body,
        mesh=mesh,
        in_specs=(
            P("sp", None),
            P(),
            P("sp", "tp"),
            P("sp", "tp"),
            P("sp", "tp"),
            P("sp", "tp"),
            P("sp", "tp"),
            P("tp"),
            P(),
            P(None, "tp"),
            P("tp"),
            P(),
            P(None, "tp"),
            P("sp", "tp"),
            P("sp", "tp"),
            P("tp"),
            P(None, "tp"),
            P("tp"),
            P("sp", "tp"),
            P("sp", "tp"),
        ),
        out_specs=P("sp", None),
        check_vma=False,
    )
```

```python
import functools
import math

import jax
import jax.numpy as jnp
from jax import lax
from jax.experimental import pallas as pl
from jax.experimental.pallas import tpu as pltpu
from jax.sharding import PartitionSpec as P


MESH = pl.DeviceIdType.MESH
HIGHEST = lax.Precision.HIGHEST
RMS_EPSILON = 1e-06
GROUP_EPSILON = 0.00064
LAYER_EPSILON = 1e-05
UNIT_EPSILON = 1e-06
EXP_HALF = math.exp(-0.5)


def split(x):
    top = x.astype(jnp.bfloat16)
    return top, (x - top.astype(jnp.float32)).astype(jnp.bfloat16)


def dot3(left, right, dims=((1,), (0,))):
    (lh, ll), (rh, rl) = split(left), split(right)

    def one(p, q):
        return lax.dot_general(p, q, (dims, ((), ())), preferred_element_type=jnp.float32)

    return one(lh, rh) + (one(lh, rl) + one(ll, rh))


def dot3t(left, right):
    return dot3(left, right, ((1,), (1,)))


def exact(left, right):
    return jnp.dot(left, right, precision=HIGHEST, preferred_element_type=jnp.float32)


def column(values, index):
    lanes = lax.broadcasted_iota(jnp.int32, values.shape, 1)
    return jnp.sum(jnp.where(lanes == index, values, 0.0), axis=1, keepdims=True)


def delta_kernel(
    head_size, chunk, block,
    query_ref, key_ref, value_ref, decay_ref, rate_ref, factor_ref, share_ref,
    local_ref, carried_ref, pair_ref,
):
    rows, width = query_ref.shape
    per = width // head_size
    pair = 0 if factor_ref.shape[1] == per else pl.program_id(0)
    lane = lax.broadcasted_iota(jnp.int32, (1, width), 1)
    lane_head = lane // head_size
    row_w = lax.broadcasted_iota(jnp.int32, (width, width), 0)
    col_w = lax.broadcasted_iota(jnp.int32, (width, width), 1)
    same_head = (row_w // head_size) == (col_w // head_size)
    ones_head = jnp.where(same_head, 1.0, 0.0)
    row_b = lax.broadcasted_iota(jnp.int32, (block, block), 0)
    col_b = lax.broadcasted_iota(jnp.int32, (block, block), 1)
    same_chunk = (row_b // chunk) == (col_b // chunk)
    strict = same_chunk & (row_b > col_b)
    incl = same_chunk & (row_b >= col_b)
    sums = jnp.concatenate([jnp.where(incl, 1.0, 0.0), jnp.where(same_chunk, 1.0, 0.0)], axis=0)
    eye_b = jnp.where(row_b == col_b, 1.0, 0.0)

    factor, share = factor_ref[...], jnp.log(share_ref[...])
    factor_w = jnp.zeros((rows, width), jnp.float32)
    share_w = jnp.zeros((rows, width), jnp.float32)
    for h in range(per):
        factor_w = jnp.where(lane_head == h, column(factor, pair * per + h), factor_w)
        share_w = jnp.where(lane_head == h, column(share, pair * per + h), share_w)
    logdec = share_w - (EXP_HALF * jax.nn.sigmoid(decay_ref[...])) * factor_w
    learn = jax.nn.sigmoid(rate_ref[...])
    key = key_ref[...]
    unit = key * lax.rsqrt(exact(key * key, ones_head) + UNIT_EPSILON)

    blocks = []
    for start in range(0, rows, block):
        cut = slice(start, start + block)
        q, k, v, ld = query_ref[cut], key[cut], value_ref[cut], logdec[cut]
        er, wr = -unit[cut], unit[cut] * learn[cut]
        both = exact(sums, ld)
        gain, total = both[:block], both[block:]
        mid = 0.5 * total
        up, down, bup = jnp.exp(gain - mid), jnp.exp(mid - gain), jnp.exp(gain - ld - mid)
        ehat, qhat, what, khat = er * bup, q * up, wr * down, k * down
        right = jnp.concatenate([what, khat], axis=0)
        eh_full, q_full = er * jnp.exp(gain - ld), q * jnp.exp(gain)
        to_end = jnp.exp(total - gain)
        pulled = solved = local = query = None
        heads = []
        for h in range(per):
            left = jnp.where(lane_head == h, jnp.concatenate([ehat, qhat], axis=0), 0.0)
            grid = dot3t(left, right)
            ew = jnp.where(strict, grid[:block, :block], 0.0)
            ek = jnp.where(strict, grid[:block, block:], 0.0)
            rw = jnp.where(incl, grid[block:, :block], 0.0)
            rk = jnp.where(incl, grid[block:, block:], 0.0)
            size = 2
            off = (row_b // size == col_b // size) & (row_b > col_b)
            inv = eye_b + jnp.where(off, ew, 0.0)
            while size < chunk:
                off = (row_b // (2 * size) == col_b // (2 * size)) & (row_b // size > col_b // size)
                inv = inv + dot3(dot3(inv, jnp.where(off, ew, 0.0)), inv)
                size *= 2
            seen = dot3(jnp.concatenate([ek, rk], axis=0), v)
            both = dot3(inv, jnp.concatenate([seen[:block], eh_full], axis=1))
            read = dot3(rw, both)
            heads.append((both[:, :width], both[:, width:], read[:, :width] + seen[block:], read[:, width:]))
        merged = list(heads[0])
        for h in range(1, per):
            merged = [jnp.where(lane_head == h, new, old) for new, old in zip(heads[h], merged)]
        pulled, solved, local, query = merged
        blocks.append((pulled, solved, local, q_full + query, v, wr * to_end, k * to_end, jnp.exp(total)))

    state = jnp.concatenate([jnp.where(row_w == col_w, 1.0, 0.0), jnp.zeros((width, width), jnp.float32)], axis=0)
    across = ((0,), (0,))
    for number, (pulled, solved, local, query, v, wend, kend, gain) in enumerate(blocks):
        for first in range(0, block, chunk):
            cut = slice(first, first + chunk)
            place = slice(number * block + first, number * block + first + chunk)
            got = dot3t(query[cut], state)
            carried_ref[place] = got[:, :width]
            local_ref[place] = local[cut] + got[:, width:]
            step = jnp.where(same_head, dot3(solved[cut], wend[cut], across), 0.0)
            added = dot3(
                jnp.concatenate([pulled[cut], v[cut]], axis=0),
                jnp.concatenate([wend[cut], kend[cut]], axis=0),
                across,
            )
            added = jnp.where(same_head, added, 0.0)
            moved = state * gain[first : first + 1] + dot3(state, step)
            state = jnp.concatenate([moved[:width], moved[width:] + added], axis=0)
    pair_ref[0] = state


def finish_kernel(head_size, local_ref, carried_ref, state_ref, gain_ref, out_ref):
    width = local_ref.shape[1]
    row_w = lax.broadcasted_iota(jnp.int32, (width, width), 0)
    col_w = lax.broadcasted_iota(jnp.int32, (width, width), 1)
    same_head = (row_w // head_size) == (col_w // head_size)
    average = jnp.where(same_head, 1.0 / head_size, 0.0)
    y = local_ref[...] + dot3t(carried_ref[...], state_ref[0])
    centred = y - exact(y, average)
    variance = exact(centred * centred, average)
    out_ref[...] = (centred * lax.rsqrt(variance + GROUP_EPSILON) * gain_ref[...]).astype(jnp.bfloat16)


def from_behind(value, axis, steps):
    count = lax.axis_size(axis)
    initial, last = (max(0, -steps), min(count, count - steps))
    return lax.ppermute(value, axis, [(source, source + steps) for source in range(initial, last)])


def head_blocks(pairs, head_size):
    width = pairs.shape[-1]
    return jnp.stack(
        [pairs[:, a : a + head_size, a : a + head_size] for a in range(0, width, head_size)], axis=1
    )


def delta_rule(query, key, value, decay_pre, rate_pre, factor, share, gain):
    rows, channels = query.shape
    heads = factor.shape[1]
    head_size = channels // heads
    per = math.gcd(heads, max(1, 128 // head_size))
    width, pairs = per * head_size, heads // per
    block = math.gcd(rows, 128)
    chunk = math.gcd(block, 16)
    wide = pl.BlockSpec((rows, width), lambda i: (0, i))
    whole = pl.BlockSpec((rows, heads), lambda i: (0, 0))
    local, carried, pair = pl.pallas_call(
        functools.partial(delta_kernel, head_size, chunk, block),
        grid=(pairs,),
        in_specs=[wide] * 5 + [whole] * 2,
        out_specs=[wide, wide, pl.BlockSpec((1, 2 * width, width), lambda i: (i, 0, 0))],
        out_shape=[
            jax.ShapeDtypeStruct((rows, channels), jnp.float32),
            jax.ShapeDtypeStruct((rows, channels), jnp.float32),
            jax.ShapeDtypeStruct((pairs, 2 * width, width), jnp.float32),
        ],
        cost_estimate=pl.CostEstimate(
            flops=pairs * rows * width * width * 60, bytes_accessed=rows * channels * 32, transcendentals=rows * channels * 10
        ),
        name="delta_chunks",
    )(query, key, value, decay_pre, rate_pre, factor, share)

    phi, psi = head_blocks(pair[:, :width], head_size), head_blocks(pair[:, width:], head_size)
    both = jnp.concatenate([phi, psi], axis=-2).reshape(heads, 2 * head_size, head_size)
    count, place = lax.axis_size("sp"), lax.axis_index("sp")
    steps = 1
    while steps < count - 1:
        earlier = from_behind(both, "sp", steps)
        new = exact_mul("hcd,hde->hce", earlier, both[:, :head_size])
        new = new + jnp.concatenate([jnp.zeros_like(both[:, :head_size]), both[:, head_size:]], axis=1)
        both = jnp.where(place >= steps, new, both)
        steps *= 2
    state = from_behind(both[:, head_size:], "sp", 1).reshape(pairs, per, head_size, head_size)
    same = jnp.eye(per, dtype=jnp.float32)
    state = (state[:, :, :, None, :] * same[None, :, None, :, None]).reshape(pairs, width, width)
    return pl.pallas_call(
        functools.partial(finish_kernel, head_size),
        grid=(pairs,),
        in_specs=[wide, wide, pl.BlockSpec((1, width, width), lambda i: (i, 0, 0)), pl.BlockSpec((1, width), lambda i: (0, i))],
        out_specs=wide,
        out_shape=jax.ShapeDtypeStruct((rows, channels), jnp.bfloat16),
        name="delta_finish",
    )(local, carried, state, gain[None])


def exact_mul(form, left, right):
    return jnp.einsum(form, left, right, precision=HIGHEST)


def gather_kernel(axis, radices, number, *refs):
    ins, outs = refs[:number], refs[number : 2 * number]
    own_sem, far_send, far_recv, near_send, near_recv = refs[2 * number :]
    outer, middle, inner = radices
    me = lax.axis_index(axis)
    x, y, z = me % inner, (me // inner) % middle, me // (inner * middle)

    def index(z_at, y_at, x_at):
        return (z_at * middle + y_at) * inner + x_at

    far = [index((z + step) % outer, y, x) for step in range(1, outer)]
    near = {}
    if inner == 2:
        near["x"] = index(z, y, 1 - x)
    if middle == 2:
        near["y"] = index(z, 1 - y, x)
    barrier = pltpu.get_barrier_semaphore()
    peers = far + list(near.values())
    for peer in peers:
        pl.semaphore_signal(barrier, inc=1, device_id={axis: peer}, device_id_type=MESH)
    pl.semaphore_wait(barrier, len(peers))

    def far_copy(w, step, to, z_from):
        return pltpu.make_async_remote_copy(
            src_ref=ins[w],
            dst_ref=outs[w].at[z_from, y, x],
            send_sem=far_send.at[w, step],
            recv_sem=far_recv.at[w, step],
            device_id={axis: to},
            device_id_type=MESH,
        )

    own = [pltpu.make_async_copy(ins[w], outs[w].at[z, y, x], own_sem.at[w]) for w in range(number)]
    for w in range(number):
        own[w].start()
        for step in range(outer - 1):
            far_copy(w, step, far[step], z).start()

    def region(w, order, stage, from_y, from_x):
        if stage == 0:
            return outs[w].at[:, from_y, from_x]
        return outs[w].at[:, from_y] if order[0] == "x" else outs[w].at[:, :, from_x]

    def near_copy(w, order, stage, from_y, from_x):
        part = region(w, order, stage, from_y, from_x)
        return pltpu.make_async_remote_copy(
            src_ref=part,
            dst_ref=part,
            send_sem=near_send.at[w, stage],
            recv_sem=near_recv.at[w, stage],
            device_id={axis: near[order[stage]]},
            device_id_type=MESH,
        )

    def theirs(w, order, stage):
        from_y, from_x = (y, 1 - x) if order[stage] == "x" else (1 - y, x)
        return near_copy(w, order, stage, from_y, from_x)

    names = list(near)
    orders = [names if w % 2 == 0 else names[::-1] for w in range(number)]

    def advance(w, stage):
        if stage == 0:
            own[w].wait()
            for step in range(outer - 1):
                far_copy(w, step, far[step], (z + outer - step - 1) % outer).wait_recv()
        else:
            theirs(w, orders[w], stage - 1).wait_recv()
        if stage < len(names):
            near_copy(w, orders[w], stage, y, x).start()

    last = len(names)
    for tick in range(number + last):
        for stage in range(last, -1, -1):
            w = tick - stage
            if 0 <= w < number:
                advance(w, stage)
    for w in range(number):
        for step in range(outer - 1):
            far_copy(w, step, far[step], z).wait_send()
        for stage in range(last):
            near_copy(w, orders[w], stage, y, x).wait_send()


def gather_rows(arrays, axis, number_id=0):
    count, number = lax.axis_size(axis), len(arrays)
    inner = math.gcd(count, 2)
    middle = math.gcd(count // inner, 2)
    radices = (count // inner // middle, middle, inner)
    outs = pl.pallas_call(
        functools.partial(gather_kernel, axis, radices, number),
        in_specs=[pl.BlockSpec(memory_space=pltpu.VMEM)] * number,
        out_specs=[pl.BlockSpec(memory_space=pl.ANY)] * number,
        out_shape=[jax.ShapeDtypeStruct(radices + item.shape, item.dtype) for item in arrays],
        scratch_shapes=[
            pltpu.SemaphoreType.DMA((number,)),
            pltpu.SemaphoreType.DMA((number, max(1, radices[0] - 1))),
            pltpu.SemaphoreType.DMA((number, max(1, radices[0] - 1))),
            pltpu.SemaphoreType.DMA((number, 2)),
            pltpu.SemaphoreType.DMA((number, 2)),
        ],
        compiler_params=pltpu.CompilerParams(collective_id=number_id, has_side_effects=True),
        cost_estimate=pl.CostEstimate(
            flops=10**9, bytes_accessed=sum(item.size for item in arrays) * 2 * count, transcendentals=0
        ),
        name="gather_rows",
    )(*arrays)
    return [out.reshape((-1,) + item.shape[1:]) for out, item in zip(outs, arrays)]


def plain_body(
    tokens,
    input_norm_gain,
    query_matrix,
    key_matrix,
    value_matrix,
    convolution_value_matrix,
    convolution_gate_matrix,
    decay_offset_channel,
    decay_first_matrix,
    decay_second_matrix,
    learning_rate_offset,
    learning_rate_first_matrix,
    learning_rate_second_matrix,
    forgetting_rate_factor,
    state_retention_share,
    per_head_norm_gain,
    convolution_filter_taps,
    convolution_channel_gain,
    attention_output_matrix,
    convolution_output_matrix,
):
    tok_rows = tokens.shape[0]
    widened = tokens.astype(jnp.float32)
    normed = (
        widened
        * lax.rsqrt(jnp.mean(widened * widened, axis=-1, keepdims=True) + RMS_EPSILON)
        * input_norm_gain
    ).astype(jnp.bfloat16)
    pieces = (
        *gather_rows((query_matrix, key_matrix, value_matrix), "sp"),
        lax.all_gather(convolution_value_matrix, "sp", axis=0, tiled=True),
        lax.all_gather(convolution_gate_matrix, "sp", axis=0, tiled=True),
    )
    query_proj, key_proj, value_proj, conv_value, conv_gate = tuple(
        (jnp.dot(normed, piece, preferred_element_type=jnp.float32) for piece in pieces)
    )
    decay_mid = jnp.tanh(
        jnp.dot(normed, decay_first_matrix, preferred_element_type=jnp.float32)
    ).astype(jnp.bfloat16)
    rate_mid = jnp.dot(
        normed, learning_rate_first_matrix, preferred_element_type=jnp.float32
    ).astype(jnp.bfloat16)
    decay_pre = decay_offset_channel + jnp.dot(
        decay_mid, decay_second_matrix, preferred_element_type=jnp.float32
    )
    rate_pre = learning_rate_offset + jnp.dot(
        rate_mid, learning_rate_second_matrix, preferred_element_type=jnp.float32
    )
    state_mixed = delta_rule(
        query_proj, key_proj, value_proj, decay_pre, rate_pre,
        forgetting_rate_factor, state_retention_share, per_head_norm_gain,
    )
    gated = (conv_value * jax.nn.sigmoid(conv_gate)).astype(jnp.bfloat16)
    span = convolution_filter_taps.shape[0]
    rim = from_behind(gated[tok_rows - (span - 1) :], "sp", 1)
    padded = jnp.concatenate([rim, gated], axis=0)
    filtered = jnp.zeros(gated.shape, jnp.float32)
    for offset in range(span):
        filtered = filtered + convolution_filter_taps[offset] * padded[offset : offset + tok_rows]
    total_sum, total_square = lax.psum(
        (jnp.sum(filtered, axis=-1), jnp.sum(filtered * filtered, axis=-1)), "tp"
    )
    conv_channels = filtered.shape[1] * lax.axis_size("tp")
    row_mean = total_sum / conv_channels
    deviation = filtered - row_mean[:, None]
    variance = total_square / conv_channels - row_mean * row_mean
    conv_mixed = jax.nn.silu(
        deviation * lax.rsqrt(variance + LAYER_EPSILON)[:, None] * convolution_channel_gain
    ).astype(jnp.bfloat16)
    contract_dims = (((1,), (1,)), ((), ()))
    pieces = lax.all_gather(
        (attention_output_matrix, convolution_output_matrix), "sp", axis=0, tiled=True
    )
    partial_out = lax.dot_general(
        state_mixed, pieces[0], contract_dims, preferred_element_type=jnp.float32
    ) + lax.dot_general(conv_mixed, pieces[1], contract_dims, preferred_element_type=jnp.float32)
    partial_out = partial_out.astype(jnp.bfloat16)
    if lax.axis_size("tp") != 2:
        return lax.psum(partial_out, "tp")
    other = lax.ppermute(partial_out, "tp", [(0, 1), (1, 0)])
    return (partial_out.astype(jnp.float32) + other.astype(jnp.float32)).astype(jnp.bfloat16)


def radices_of(axis):
    count = lax.axis_size(axis)
    inner = math.gcd(count, 2)
    middle = math.gcd(count // inner, 2)
    return count // inner // middle, middle, inner


def place_of(axis, radices):
    outer, middle, inner = radices
    me = lax.axis_index(axis)
    return me // (inner * middle), (me // inner) % middle, me % inner


def greet(devices):
    barrier = pltpu.get_barrier_semaphore()
    for device in devices:
        pl.semaphore_signal(barrier, inc=1, device_id=device, device_id_type=MESH)
    pl.semaphore_wait(barrier, len(devices))


def spread_kernel(axis, pair_axis, radices, widths, placed, firsts, early, head_size, chunk, block, *refs):
    number = len(widths)
    raw_ref, gain_ref, side_ref, ins = refs[0], refs[1], refs[2], refs[3 : 3 + number]
    refs = refs[3 + number :]
    extra, maps, refs = refs[: len(firsts)], refs[len(firsts) : len(firsts) + 7], refs[len(firsts) + 7 :]
    decay_ref, rate_ref, decay_offset_ref, rate_offset_ref, taps_ref, head_gain_ref, conv_gain_ref = maps
    kinds = 1 + max(out for out, _ in placed)
    out_ref, local_ref, carried_ref, pair_ref, filtered_ref, stats_ref, last_out = refs[:7]
    finish_refs, refs = refs[7:27], refs[27:]
    (first_out, second_out, padded, rim_out, rim_in, rim_send, rim_recv, tokens_out, side_out, tokens_ref, proj, mats, adds, hist, queries,
     first_sem, own_sem, far_send, far_recv, near_send, near_recv, side_send, side_recv,
     tok_send, tok_recv, sib_send, sib_recv) = refs
    outs = [first_out, second_out, last_out]
    outer, middle, inner = radices
    z, y, x = place_of(axis, radices)
    core = lax.axis_index(pair_axis)
    widened = raw_ref[...].astype(jnp.float32)
    scale = lax.rsqrt(jnp.mean(widened * widened, axis=-1, keepdims=True) + RMS_EPSILON)
    tokens_ref[...] = (widened * scale * gain_ref[...]).astype(jnp.bfloat16)
    half = tokens_ref.shape[0] // 2
    mine, other = pl.ds(pl.multiple_of(core * half, half), half), pl.ds(pl.multiple_of((1 - core) * half, half), half)

    def index(z_at, y_at, x_at):
        return (z_at * middle + y_at) * inner + x_at

    far = [(z + step) % outer for step in range(1, outer)]
    near = {"x": index(z, y, 1 - x), "y": index(z, 1 - y, x)}
    planes = middle * inner
    plane = y * inner + x
    peers, send_pairs, send_stats, wait_pairs, make_states, state_rows, wait_stats, reduce_all = finish_phases(
        axis, pair_axis, radices, head_size,
        pair_ref, stats_ref, local_ref, carried_ref, head_gain_ref, filtered_ref, conv_gain_ref, last_out, out_ref,
        *finish_refs,
    )
    greet(peers)

    def part(w, at):
        return ins[w].at[:, pl.ds(pl.multiple_of(at * widths[w], widths[w]), widths[w])]

    def slot(w, *where, cut=slice(None)):
        out, offset = placed[w]
        return outs[out].at[(*where, cut, pl.ds(offset, widths[w]))]

    def far_copy(w, step, to, z_from):
        return pltpu.make_async_remote_copy(
            src_ref=part(w, to), dst_ref=slot(w, z_from, y, x),
            send_sem=far_send.at[w, step], recv_sem=far_recv.at[w, step],
            device_id={axis: index(to, y, x)}, device_id_type=MESH,
        )

    def side_copy(step, to, z_from):
        return pltpu.make_async_remote_copy(
            src_ref=side_ref, dst_ref=side_out.at[z_from],
            send_sem=side_send.at[step], recv_sem=side_recv.at[step],
            device_id={axis: index(to, y, x)}, device_id_type=MESH,
        )

    names = list(near)
    depth = ins[0].shape[0]
    orders = [names, names[::-1]]

    def near_copy(w, part_at, stage, y_at, x_at):
        order = orders[part_at]
        cut = pl.ds(part_at * (depth // 2), depth // 2)
        if stage == 0:
            region = slot(w, slice(None), y_at, x_at, cut=cut)
        elif order[0] == "x":
            region = slot(w, slice(None), y_at, slice(None), cut=cut)
        else:
            region = slot(w, slice(None), slice(None), x_at, cut=cut)
        return pltpu.make_async_remote_copy(
            src_ref=region, dst_ref=region,
            send_sem=near_send.at[w, part_at, stage], recv_sem=near_recv.at[w, part_at, stage],
            device_id={axis: near[order[stage]]}, device_id_type=MESH,
        )

    def theirs(w, part_at, stage):
        y_at, x_at = (y, 1 - x) if orders[part_at][stage] == "x" else (1 - y, x)
        return near_copy(w, part_at, stage, y_at, x_at)

    def inside(at):
        return (at >= 0) & (at < outer)

    ways = (1, -1)

    def token_copy(way, step, block, source):
        return pltpu.make_async_remote_copy(
            src_ref=source, dst_ref=tokens_out.at[block, mine],
            send_sem=tok_send.at[way, step], recv_sem=tok_recv.at[way, step],
            device_id={axis: index((z + ways[way] + outer) % outer, y, x)}, device_id_type=MESH,
        )

    def sibling_copy(way, step, block, rows):
        return pltpu.make_async_remote_copy(
            src_ref=tokens_out.at[block, rows], dst_ref=tokens_out.at[block, rows],
            send_sem=sib_send.at[way, step], recv_sem=sib_recv.at[way, step],
            device_id={pair_axis: 1 - core}, device_id_type=MESH,
        )

    def arrived(way, step):
        return z - ways[way] * (step + 1)

    def sends(way, step):
        return inside(z + ways[way]) & inside(z - ways[way] * step)

    own = [pltpu.make_async_copy(part(w, z), slot(w, z, y, x), own_sem.at[w]) for w in range(number)]
    own.append(pltpu.make_async_copy(tokens_ref, tokens_out.at[z], own_sem.at[number]))
    own.append(pltpu.make_async_copy(side_ref, side_out.at[z], own_sem.at[number + 1]))
    for step in range(outer - 1):
        side_copy(step, far[step], z).start()
    def send_far(some):
        for w in some:
            own[w].start()
            for step in range(outer - 1):
                far_copy(w, step, far[step], z).start()

    send_far(early)
    for way in range(2):
        @pl.when(sends(way, 0))
        def _():
            token_copy(way, 0, z, tokens_ref.at[mine]).start()
    rest = [[w for w in range(number) if placed[w][0] == out] for out in range(1, kinds)]
    send_far(rest[0])
    own[number].start()
    own[number + 1].start()
    kept = []
    for item, (out, offset) in enumerate(firsts):
        for at in range(outer * middle * inner):
            where = (at // (middle * inner), (at // inner) % middle, at % inner)
            kept.append(pltpu.make_async_copy(
                extra[item].at[at * depth : (at + 1) * depth],
                outs[out].at[(*where, slice(None), pl.ds(offset, extra[item].shape[1]))],
                first_sem.at[item, at],
            ))
            kept[-1].start()

    def advance(w, stage):
        if stage == 0:
            own[w].wait()
            for step in range(outer - 1):
                far_copy(w, step, far[step], (z + outer - step - 1) % outer).wait_recv()
        for part_at in range(2):
            if stage:
                theirs(w, part_at, stage - 1).wait_recv()
            if stage < len(names):
                near_copy(w, part_at, stage, y, x).start()

    def token_step(step):
        for way in range(2):
            block = arrived(way, step)
            @pl.when(inside(block))
            def _():
                token_copy(way, step, block, tokens_out.at[block, mine]).wait_recv()
                @pl.when(sends(way, step + 1) & (step + 1 < outer - 1))
                def _():
                    token_copy(way, step + 1, block, tokens_out.at[block, mine]).start()
                sibling_copy(way, step, block, mine).start()

    last = len(names)

    def sibling_step(step):
        for way in range(2):
            block = arrived(way, step)
            @pl.when(inside(block))
            def _():
                sibling_copy(way, step, block, other).wait_recv()

    def run(some):
        for tick in range(len(some) + last):
            for stage in range(last + 1):
                if 0 <= tick - stage < len(some):
                    advance(some[tick - stage], stage)

    run(early)
    own[number].wait()
    own[number + 1].wait()
    for item in kept:
        item.wait()
    for step in range(outer - 1):
        side_copy(step, far[step], (z + outer - step - 1) % outer).wait_recv()
    token_step(0)
    send_far(rest[1])
    for w in rest[0]:
        advance(w, 0)
    one_block, chain, read = delta_phases(
        z, head_size, chunk, block, proj, side_out, decay_ref, rate_ref, decay_offset_ref, rate_offset_ref,
        local_ref, carried_ref, pair_ref, mats, adds, hist, queries,
    )
    pieces = tokens_ref.shape[0] // block
    edge = jnp.minimum(z, outer - 1 - z)
    toward = jnp.where(z < outer // 2, -1, 1)
    piece_depth = middle * inner * depth

    def project(group):
        total = None
        for part_at in range(outer):
            matrix = first_out[part_at].reshape(piece_depth, first_out.shape[-1])
            term = jnp.dot(
                tokens_out[group, :, part_at * piece_depth : (part_at + 1) * piece_depth], matrix,
                preferred_element_type=jnp.float32,
            )
            total = term if total is None else total + term
        proj[...] = total

    def one_round(k, carry):
        twosided = k <= 2 * edge
        distance = jnp.where(twosided, (k + 1) // 2, k - edge)
        side = jnp.where(twosided & (k % 2 == 1), toward, -toward)
        group = z + side * distance

        @pl.when(k > 0)
        def _():
            sibling_step(k - 1)

        project(group)
        for piece in range(pieces):
            one_block(group, piece)
            if piece == 0:
                @pl.when(k == 0)
                def _():
                    for w in rest[0]:
                        advance(w, 1)

                @pl.when(k == 2)
                def _():
                    for w in rest[1]:
                        advance(w, 1)

                @pl.when((k > 0) & (k < outer - 1))
                def _():
                    token_step(k)

                @pl.when(k == 1)
                def _():
                    for w in rest[1]:
                        advance(w, 0)
        return carry

    lax.fori_loop(0, outer, one_round, 0)
    chain()

    rows = tokens_ref.shape[0]
    span, rim_rows = taps_ref.shape[0], rim_out.shape[1]
    conv_width = second_out.shape[-1] // 2
    for w in rest[0]:
        advance(w, last)

    def gate(group, carry):
        total = None
        for part_at in range(outer):
            matrix = second_out[part_at].reshape(piece_depth, 2 * conv_width)
            term = jnp.dot(
                tokens_out[group, :, part_at * piece_depth : (part_at + 1) * piece_depth], matrix,
                preferred_element_type=jnp.float32,
            )
            total = term if total is None else total + term
        gated = (total[:, :conv_width] * jax.nn.sigmoid(total[:, conv_width:])).astype(jnp.bfloat16)
        padded[group, rim_rows:] = gated.astype(jnp.float32)
        rim_out[group] = gated[rows - rim_rows :]
        return carry

    lax.fori_loop(0, outer, gate, 0)
    rim_copy = pltpu.make_async_remote_copy(
        src_ref=rim_out, dst_ref=rim_in, send_sem=rim_send.at[0], recv_sem=rim_recv.at[0],
        device_id={axis: z * planes + (plane + 1) % planes}, device_id_type=MESH,
    )
    rim_copy.start()
    send_pairs()
    read()
    rim_copy.wait_recv()
    for group in range(outer):
        before = jnp.zeros(rim_in.shape[1:], jnp.bfloat16) if group == 0 else rim_in[group - 1]
        padded[group, :rim_rows] = jnp.where(plane == 0, before, rim_in[group]).astype(jnp.float32)
    taps = taps_ref[:, pl.ds(pl.multiple_of(z * conv_width, conv_width), conv_width)]
    part_rows = math.gcd(rows, 64)
    row_8 = lax.broadcasted_iota(jnp.int32, (8, conv_width), 0)
    sum_rows = [jnp.where(row_8 == at, 1.0, 0.0).astype(jnp.bfloat16) for at in range(2)]
    skip = rim_rows - (span - 1)

    def row_sums(values, marks):
        total = None
        for _ in range(3):
            top = values.astype(jnp.bfloat16)
            term = lax.dot_general(marks, top, (((1,), (1,)), ((), ())), preferred_element_type=jnp.float32)
            total = term if total is None else total + term
            values = values - top.astype(jnp.float32)
        return total

    def convolve(number, carry):
        group, start = number // (rows // part_rows), (number % (rows // part_rows)) * part_rows
        window = padded[group, pl.ds(pl.multiple_of(start, part_rows), part_rows + rim_rows)]
        total = jnp.zeros((part_rows, conv_width), jnp.float32)
        for turn in range(8):
            moved = window if turn == 0 else window[turn : turn + part_rows + rim_rows - 8]
            for tap in range(span):
                if (tap + skip) % 8 == turn:
                    first = tap + skip - turn
                    total = total + taps[tap : tap + 1] * moved[first : first + part_rows]
        filtered_ref[pl.ds(pl.multiple_of(number * part_rows, part_rows), part_rows)] = total
        return carry

    lax.fori_loop(0, outer * (rows // part_rows), convolve, 0)
    for group in range(outer):
        values = filtered_ref[group * rows : (group + 1) * rows]
        stats_ref[group] = row_sums(values, sum_rows[0]) + row_sums(values * values, sum_rows[1])
    for w in rest[1]:
        advance(w, last)
    send_stats()
    wait_pairs()
    make_states()
    state_rows()
    wait_stats()
    reduce_all()
    rim_copy.wait_send()
    for step in range(outer - 1):
        side_copy(step, far[step], z).wait_send()
    for step in range(outer - 1):
        for way in range(2):
            block = arrived(way, step)
            @pl.when(inside(block))
            def _():
                sibling_copy(way, step, block, mine).wait_send()
            @pl.when(sends(way, step))
            def _():
                token_copy(way, step, z - ways[way] * step, tokens_ref.at[mine]).wait_send()
    for w in range(number):
        for step in range(outer - 1):
            far_copy(w, step, far[step], z).wait_send()
        for stage in range(last):
            for part_at in range(2):
                near_copy(w, part_at, stage, y, x).wait_send()


def spread(tokens, gain, side, weights, groups, firsts, maps, head_size, axis, pair_axis):
    radices = radices_of(axis)
    outer, number = radices[0], len(weights)
    widths = [item.shape[1] // outer for item in weights]
    placed, totals = [None] * number, []
    for out, members in enumerate(groups):
        offset = 0
        for w in members:
            placed[w] = (out, offset)
            offset += widths[w]
        totals.append(offset)
    extras, width = [], widths[0]
    for item in firsts:
        extras.append((0, totals[0]))
        totals[0] += item.shape[1]
    depth, rows = weights[0].shape[0], tokens.shape[0]
    block = math.gcd(rows, 128)
    chunk = math.gcd(block, 32)
    total = outer * rows
    conv_width, rim_rows = totals[1] // 2, -(-(maps[4].shape[0] - 1) // 16) * 16
    vmem, dma = pl.BlockSpec(memory_space=pltpu.VMEM), pltpu.SemaphoreType.DMA
    planes, lines = radices[1] * radices[2], outer * lax.axis_size(pair_axis) - 1
    half, slots = tokens.shape[1] // 2, (2, outer - 1)
    return pl.pallas_call(
        functools.partial(
            spread_kernel, axis, pair_axis, radices, widths, placed, extras, groups[0], head_size, chunk, block
        ),
        in_specs=[vmem] * (3 + number + len(firsts) + len(maps)),
        out_specs=vmem,
        out_shape=jax.ShapeDtypeStruct(tokens.shape, jnp.bfloat16),
        scratch_shapes=[
            pltpu.VMEM((total, width), jnp.float32),
            pltpu.VMEM((total, width), jnp.float32),
            pltpu.VMEM((outer, width, width), jnp.float32),
            pltpu.VMEM((total, conv_width), jnp.float32),
            pltpu.VMEM((outer, 8, rows), jnp.float32),
            pltpu.VMEM(radices + (depth, totals[2]), weights[0].dtype),
            pltpu.VMEM((planes, outer, width, width), jnp.float32),
            pltpu.VMEM((lines, outer, 8, rows), jnp.float32),
            pltpu.VMEM((outer, width, width), jnp.float32),
            pltpu.VMEM((outer, rows, width + conv_width), jnp.bfloat16),
            pltpu.VMEM((outer, rows, half), jnp.float32),
            pltpu.VMEM((outer, rows, half), jnp.bfloat16),
            pltpu.VMEM((outer, rows, half), jnp.bfloat16),
            pltpu.VMEM(slots + (rows, half), jnp.bfloat16),
            pltpu.VMEM(slots + (rows, half), jnp.bfloat16),
            dma((1,)), dma((planes - 1,)), dma((planes - 1,)), dma((lines,)), dma((lines,)),
            dma((outer,)), dma((outer,)), dma(slots), dma(slots), dma((1,)), dma((1,)),
            pltpu.VMEM(radices + (depth, totals[0]), weights[0].dtype),
            pltpu.VMEM(radices + (depth, totals[1]), weights[0].dtype),
            pltpu.VMEM((outer, rim_rows + rows, conv_width), jnp.float32),
            pltpu.VMEM((outer, rim_rows, conv_width), weights[0].dtype),
            pltpu.VMEM((outer, rim_rows, conv_width), weights[0].dtype),
            pltpu.SemaphoreType.DMA((1,)),
            pltpu.SemaphoreType.DMA((1,)),
            pltpu.VMEM((outer,) + tokens.shape, tokens.dtype),
            pltpu.VMEM((outer,) + side.shape, side.dtype),
            pltpu.VMEM(tokens.shape, tokens.dtype),
            pltpu.VMEM((rows, totals[0]), jnp.float32),
        ]
        + [pltpu.VMEM((total // chunk, width, width), jnp.float32)] * 3
        + [
            pltpu.VMEM((total, width), jnp.float32),
            pltpu.SemaphoreType.DMA((len(firsts), math.prod(radices))),
            pltpu.SemaphoreType.DMA((number + 3,)),
            pltpu.SemaphoreType.DMA((number, outer - 1)),
            pltpu.SemaphoreType.DMA((number, outer - 1)),
            pltpu.SemaphoreType.DMA((number, 2, 2)),
            pltpu.SemaphoreType.DMA((number, 2, 2)),
            pltpu.SemaphoreType.DMA((outer - 1,)),
            pltpu.SemaphoreType.DMA((outer - 1,)),
            pltpu.SemaphoreType.DMA((2, outer - 1)),
            pltpu.SemaphoreType.DMA((2, outer - 1)),
            pltpu.SemaphoreType.DMA((2, outer - 1)),
            pltpu.SemaphoreType.DMA((2, outer - 1)),
        ],
        compiler_params=pltpu.CompilerParams(collective_id=0, has_side_effects=True, vmem_limit_bytes=60 * 2**20),
        cost_estimate=pl.CostEstimate(flops=10**10, bytes_accessed=8 * tokens.size * outer, transcendentals=0),
        name="whole_layer",
    )(tokens, gain, side, *weights, *firsts, *maps)


def spread_sum(values, matrix):
    top, rest = split(values)
    return jnp.dot(top, matrix, preferred_element_type=jnp.float32) + jnp.dot(
        rest, matrix, preferred_element_type=jnp.float32
    )


def finish_phases(
    axis, pair_axis, radices, head_size,
    pair_ref, stats_ref, local_ref, carried_ref, gain_ref, filtered_ref, conv_gain_ref, matrix_ref,
    out_ref,
    held, stats, smat, mixed_all, keep, twin_out, twin_in, chain_out, chain_in,
    own_sem, pair_send, pair_recv, stat_send, stat_recv,
    twin_send, twin_recv, chain_send, chain_recv, last_send, last_recv,
):
    outer, middle, inner = radices
    planes = middle * inner
    z, y, x = place_of(axis, radices)
    place = y * inner + x
    core = lax.axis_index(pair_axis)
    width, conv_width = pair_ref.shape[-1], filtered_ref.shape[-1]
    rows, half = keep.shape[1:]
    ways = (1, -1)
    plane_peers = [(place + step) % planes for step in range(1, planes)]
    cores = lax.axis_size(pair_axis)
    lines = [(dz, dc) for dz in range(outer) for dc in range(cores) if dz or dc]

    def line_device(dz, dc):
        return {axis: ((z + dz) % outer) * planes + place, pair_axis: (core + dc) % cores}

    def inside(at):
        return (at >= 0) & (at < outer)

    peers = [{axis: z * planes + peer} for peer in plane_peers] + [line_device(*line) for line in lines]

    def pair_copy(step, p_from):
        return pltpu.make_async_remote_copy(
            src_ref=pair_ref, dst_ref=held.at[p_from],
            send_sem=pair_send.at[step], recv_sem=pair_recv.at[step],
            device_id={axis: z * planes + plane_peers[step]}, device_id_type=MESH,
        )

    def stat_copy(number):
        return pltpu.make_async_remote_copy(
            src_ref=stats_ref, dst_ref=stats.at[number],
            send_sem=stat_send.at[number], recv_sem=stat_recv.at[number],
            device_id=line_device(*lines[number]), device_id_type=MESH,
        )

    def twin_copy(block):
        return pltpu.make_async_remote_copy(
            src_ref=twin_out.at[block], dst_ref=twin_in.at[block],
            send_sem=twin_send.at[block], recv_sem=twin_recv.at[block],
            device_id={pair_axis: 1 - core}, device_id_type=MESH,
        )

    def chain_copy(way, steps):
        return pltpu.make_async_remote_copy(
            src_ref=chain_out.at[way, steps - 1], dst_ref=chain_in.at[way, steps - 1],
            send_sem=chain_send.at[way, steps - 1], recv_sem=chain_recv.at[way, steps - 1],
            device_id={axis: ((z + 1 - 2 * way + outer) % outer) * planes + place}, device_id_type=MESH,
        )

    own = pltpu.make_async_copy(pair_ref, held.at[place], own_sem.at[0])

    def send_pairs():
        for step in range(planes - 1):
            pair_copy(step, place).start()
        own.start()

    def send_stats():
        for number in range(len(lines)):
            stat_copy(number).start()

    channels = conv_width * outer * cores
    conv_gain = conv_gain_ref[:, pl.ds(pl.multiple_of(z * conv_width, conv_width), conv_width)]
    lane_2 = lax.broadcasted_iota(jnp.int32, (8, 256), 1) // 128
    pick = jnp.where(lax.broadcasted_iota(jnp.int32, (8, 256), 0) == lane_2, 1.0, 0.0)
    dims = (((1,), (1,)), ((), ()))

    def rows_of(block):
        return pl.ds(pl.multiple_of(block * rows, rows), rows)

    def side_rows(side):
        return pl.ds(pl.multiple_of(side * half, half), half)

    def side_matrix(side):
        these = matrix_ref[pl.ds(side * (outer // 2), outer // 2)]
        return these.reshape(half, matrix_ref.shape[-1])

    def conv_part(block):
        totals = stats_ref[block]
        for number in range(len(lines)):
            totals = totals + stats[number, block]
        spread_totals = lax.dot_general(
            totals, pick, (((0,), (0,)), ((), ())), precision=HIGHEST, preferred_element_type=jnp.float32
        )
        mean, square = spread_totals[:, :128] / channels, spread_totals[:, 128:] / channels
        scale = lax.rsqrt(square - mean * mean + LAYER_EPSILON)
        mean = jnp.concatenate([mean] * (conv_width // 128), axis=1)
        scale = jnp.concatenate([scale] * (conv_width // 128), axis=1)
        normal = (filtered_ref[rows_of(block), :] - mean) * scale * conv_gain
        mixed_all[block, :, width:] = jax.nn.silu(normal).astype(jnp.bfloat16)

    row = lax.broadcasted_iota(jnp.int32, (width, width), 0)
    lane = lax.broadcasted_iota(jnp.int32, (width, width), 1)
    average = jnp.where((row // head_size) == (lane // head_size), 1.0 / head_size, 0.0).astype(jnp.bfloat16)
    first_head, moves = row < head_size, lane < head_size

    def step_matrix(item):
        part = jnp.where(moves, item, 0.0)
        return jnp.where(first_head, part, pltpu.roll(part, head_size, 1))

    def state_matrix(item):
        part = jnp.where(moves, 0.0, item)
        return jnp.where(first_head, pltpu.roll(part, head_size, 1), part)

    def compose(earlier, later):
        return dot3(step_matrix(later), earlier) + jnp.where(moves, 0.0, later)

    nothing = jnp.where(moves & (row % head_size == lane), 1.0, 0.0)

    def wait_pairs():
        own.wait()
        for step in range(planes - 1):
            pair_copy(step, (place + planes - step - 1) % planes).wait_recv()

    def make_states():
        before, whole = [], []
        for block in range(outer):
            total, kept = held[0, block], nothing
            for p in range(1, planes):
                kept = jnp.where(place == p, total, kept)
                total = compose(total, held[p, block])
            before.append(kept)
            whole.append(total)
        state = jnp.zeros((width, width), jnp.float32)
        for block in range(outer):
            smat[block] = state_matrix(compose(state, before[block]))
            if block + 1 < outer:
                state = compose(state, whole[block])

    gain = gain_ref[:, pl.ds(pl.multiple_of(z * width, width), width)]

    def state_part(block, carry):
        cut = rows_of(block)
        full = local_ref[cut, :] + dot3(carried_ref[cut, :], smat[block])
        centred = full - spread_sum(full, average)
        variance = spread_sum(centred * centred, average)
        mixed_all[block, :, :width] = (centred * lax.rsqrt(variance + GROUP_EPSILON) * gain).astype(jnp.bfloat16)
        return carry

    def at_end():
        return (z == 0) | (z == outer - 1)

    def order(number):
        return jnp.where(z < outer // 2, outer - 1 - number, number)

    def product(block, side):
        return lax.dot_general(
            mixed_all[block], side_matrix(side), dims, preferred_element_type=jnp.float32
        )

    def one_product(number, carry):
        block = order(number)
        conv_part(block)
        twin_out[block] = product(block, 1 - core).astype(jnp.bfloat16)
        twin_copy(block).start()
        keep[block] = product(block, core)

        @pl.when(at_end() & (number > 0))
        def _():
            earlier = order(number - 1)
            way = jnp.where(z == 0, 0, 1)
            steps = jnp.where(z == 0, earlier, z - earlier)
            twin_copy(earlier).wait_recv()
            chain_out[way, steps - 1] = (keep[earlier] + twin_in[earlier].astype(jnp.float32)).astype(jnp.bfloat16)
            chain_copy(way, steps).start()
        return carry

    def wait_stats():
        for number in range(len(lines)):
            stat_copy(number).wait_recv()

    def reduce_all():
        lax.fori_loop(0, outer, one_product, 0)
        for steps in range(outer - 2, 0, -1):
            for way in range(2):
                block = z + ways[way] * steps

                @pl.when(inside(block) & (z > 0) & (z < outer - 1))
                def _():
                    twin_copy(block).wait_recv()
                    keep[block] += twin_in[block].astype(jnp.float32)
                    chain_copy(way, steps + 1).wait_recv()
                    chain_out[way, steps - 1] = (keep[block] + chain_in[way, steps].astype(jnp.float32)).astype(jnp.bfloat16)
                    chain_copy(way, steps).start()

        twin_copy(z).wait_recv()
        keep[z] += twin_in[z].astype(jnp.float32)
        for way in range(2):
            @pl.when(inside(z - ways[way]))
            def _():
                chain_copy(way, 1).wait_recv()
                keep[z] += chain_in[way, 0].astype(jnp.float32)

        out_ref[:, side_rows(core)] = keep[z].astype(jnp.bfloat16)

        def last_copy(side):
            where = out_ref.at[:, side_rows(side)]
            return pltpu.make_async_remote_copy(
                src_ref=where, dst_ref=where, send_sem=last_send.at[0], recv_sem=last_recv.at[0],
                device_id={pair_axis: 1 - core}, device_id_type=MESH,
            )

        last_copy(core).start()
        for step in range(planes - 1):
            pair_copy(step, place).wait_send()
        for number in range(len(lines)):
            stat_copy(number).wait_send()
        for block in range(outer):
            twin_copy(block).wait_send()
        for steps in range(outer - 1, 0, -1):
            for way in range(2):
                @pl.when(inside(z + ways[way] * steps))
                def _():
                    chain_copy(way, steps).wait_send()
        last_copy(1 - core).wait_recv()
        last_copy(core).wait_send()

    return peers, send_pairs, send_stats, wait_pairs, make_states, lambda: lax.fori_loop(0, outer, state_part, 0), wait_stats, reduce_all


def dotp(left, right, passes, dims=((1,), (0,))):
    def one(p, q):
        return lax.dot_general(p, q, (dims, ((), ())), preferred_element_type=jnp.float32)

    if passes == 1:
        return one(left.astype(jnp.bfloat16), right.astype(jnp.bfloat16))
    (lh, ll), (rh, rl) = split(left), split(right)
    return one(lh, rh) + (one(lh, rl) + one(ll, rh))


GRID_PASSES, SOLVE_PASSES, SEEN_PASSES, STEP_PASSES, CHAIN_PASSES, READ_PASSES = 3, 3, 3, 3, 3, 3


def delta_phases(
    z, head_size, chunk, block,
    proj_ref, side_ref, decay_ref, rate_ref, decay_offset_ref, rate_offset_ref,
    local_ref, carried_ref, pair_ref,
    mats, adds, hist, queries,
):
    groups, _, rows = side_ref.shape
    width = local_ref.shape[1]
    heads = side_ref.shape[1] // 2
    per, pieces = width // head_size, rows // block
    chunks, steps = block // chunk, rows // chunk
    wide = per * block

    def iota(shape, dim):
        return lax.broadcasted_iota(jnp.int32, shape, dim)

    lane_head = iota((1, width), 1) // head_size
    lane_head2 = (iota((1, 2 * width), 1) % width) // head_size
    row_w, col_w = iota((width, width), 0), iota((width, width), 1)
    same_head = (row_w // head_size) == (col_w // head_size)
    ones_head = jnp.where(same_head, 1.0, 0.0).astype(jnp.bfloat16)
    row_b, col_b = iota((block, block), 0), iota((block, block), 1)
    same_chunk = (row_b // chunk) == (col_b // chunk)
    strict = same_chunk & (row_b > col_b)
    incl = same_chunk & (row_b >= col_b)
    sums = jnp.concatenate([jnp.where(incl, 1.0, 0.0), jnp.where(same_chunk, 1.0, 0.0)], axis=0).astype(jnp.bfloat16)
    row_c, col_c = iota((chunk, wide), 0), iota((chunk, wide), 1) % chunk
    eye_c = jnp.where(row_c == col_c, 1.0, 0.0)
    diagonal = (iota((wide, wide), 0) // chunk) == (iota((wide, wide), 1) // chunk)
    spread_rows = (iota((block, wide), 0) // chunk) == ((iota((block, wide), 1) % block) // chunk)
    place = iota((2 * heads, 2 * width), 0)
    chosen = z * per + lane_head2 + jnp.where(iota((1, 2 * width), 1) < width, 0, heads)
    expand = jnp.where(place == chosen, 1.0, 0.0)
    ours = pl.ds(pl.multiple_of(z * width, width), width)
    decay_matrix, rate_matrix = decay_ref[:, ours], rate_ref[:, ours]
    decay_offset, rate_offset = decay_offset_ref[:, ours], rate_offset_ref[:, ours]
    side_row = iota((2 * heads, block), 0)

    def by_head(values, mark):
        return jnp.concatenate([jnp.where(mark == h, values, 0.0) for h in range(per)], axis=0)

    def widen(compact):
        return jnp.where(diagonal, jnp.concatenate([compact] * (wide // chunk), axis=0), 0.0)

    def one_block(group, piece):
        start = pl.multiple_of(group * rows + piece * block, block)
        cut = pl.ds(start, block)
        here = slice(piece * block, (piece + 1) * block)
        q, key, v = proj_ref[here, 0:width], proj_ref[here, width : 2 * width], proj_ref[here, 2 * width : 3 * width]
        inner_width = decay_ref.shape[0]
        mid_at = 3 * width
        decay_mid = jnp.tanh(proj_ref[here, mid_at : mid_at + inner_width]).astype(jnp.bfloat16)
        rate_mid = proj_ref[here, mid_at + inner_width : mid_at + 2 * inner_width].astype(jnp.bfloat16)
        decay_pre = decay_offset + jnp.dot(decay_mid, decay_matrix, preferred_element_type=jnp.float32)
        rate_pre = rate_offset + jnp.dot(rate_mid, rate_matrix, preferred_element_type=jnp.float32)
        thin = side_ref[group, :, piece * block : (piece + 1) * block]
        thin = jnp.where(side_row < heads, thin, jnp.log(thin))
        both = lax.dot_general(
            thin, expand, (((0,), (0,)), ((), ())), precision=HIGHEST, preferred_element_type=jnp.float32
        )
        ld = both[:, width:] - (EXP_HALF * jax.nn.sigmoid(decay_pre)) * both[:, :width]
        learn = jax.nn.sigmoid(rate_pre)
        unit = key * lax.rsqrt(spread_sum(key * key, ones_head) + UNIT_EPSILON)
        er, wr = -unit, unit * learn
        top, rest = split(ld)
        third = (ld - top.astype(jnp.float32) - rest.astype(jnp.float32)).astype(jnp.bfloat16)
        both = jnp.dot(sums, top, preferred_element_type=jnp.float32) + (
            jnp.dot(sums, rest, preferred_element_type=jnp.float32)
            + jnp.dot(sums, third, preferred_element_type=jnp.float32)
        )
        gain, total = both[:block], both[block:]
        mid = 0.5 * total
        up, down, bup = jnp.exp(gain - mid), jnp.exp(mid - gain), jnp.exp(gain - ld - mid)
        left = jnp.concatenate([er * bup, q * up], axis=0)
        what, khat = wr * down, key * down
        right = jnp.concatenate(
            [jnp.where(lane_head == h, item, 0.0) for h in range(per) for item in (what, khat)], axis=0
        )
        grid = dotp(left, right, GRID_PASSES, ((1,), (1,)))

        def piece_of(upper, kind, mask):
            cut_rows = slice(0, block) if upper else slice(block, 2 * block)
            return jnp.concatenate(
                [jnp.where(mask, grid[cut_rows, (2 * h + kind) * block : (2 * h + kind + 1) * block], 0.0) for h in range(per)],
                axis=1,
            )

        ew, ek = piece_of(True, 0, strict), piece_of(True, 1, strict)
        rw, rk = piece_of(False, 0, incl), piece_of(False, 1, incl)
        compact = ew[:chunk]
        for c in range(1, chunks):
            compact = compact + ew[c * chunk : (c + 1) * chunk]
        size = 2
        inv = eye_c + jnp.where((row_c // size == col_c // size) & (row_c > col_c), compact, 0.0)
        while size < chunk:
            off = (row_c // (2 * size) == col_c // (2 * size)) & (row_c // size > col_c // size)
            part = dotp(inv, widen(jnp.where(off, compact, 0.0)), SOLVE_PASSES)
            inv = inv + dotp(part, widen(inv), SOLVE_PASSES)
            size *= 2
        inverse = jnp.where(spread_rows, jnp.concatenate([inv] * chunks, axis=0), 0.0)
        seen = dotp(jnp.concatenate([ek, rk], axis=0), by_head(v, lane_head), SEEN_PASSES)
        eh_full = er * jnp.exp(gain - ld)
        both = jnp.concatenate([seen[:block], eh_full], axis=1)
        both = dotp(inverse, by_head(both, lane_head2), SEEN_PASSES)
        read = dotp(rw, by_head(both, lane_head2), SEEN_PASSES)
        local_ref[cut] = read[:, :width] + seen[block:]
        queries[cut] = q * jnp.exp(gain) + read[:, width:]
        to_end, ends = jnp.exp(total - gain), jnp.exp(total)
        wend, kend = wr * to_end, key * to_end
        zero = jnp.zeros((chunk, width), jnp.float32)
        for c in range(chunks):
            now = slice(c * chunk, (c + 1) * chunk)
            lhs = jnp.concatenate([wend[now], kend[now]], axis=0)
            rhs = jnp.concatenate(
                [
                    jnp.concatenate([both[now, width:], both[now, :width]], axis=1),
                    jnp.concatenate([zero, v[now]], axis=1),
                ],
                axis=0,
            )
            made = dotp(lhs, rhs, STEP_PASSES, ((0,), (0,)))
            number = group * steps + piece * chunks + c
            step = jnp.where(same_head, made[:, :width], 0.0)
            mats[number] = step + jnp.where(row_w == col_w, ends[c * chunk : c * chunk + 1], 0.0)
            added = made[:, width:]
            added = jnp.where(row_w < head_size, pltpu.roll(added, head_size, 1), added)
            adds[number] = jnp.where(col_w < head_size, 0.0, added)

    begin = jnp.where(row_w % head_size == col_w, 1.0, 0.0)

    def one_step(step, carry):
        for group in range(groups):
            number = group * steps + step
            state = pair_ref[group]
            hist[number] = state
            pair_ref[group] = dotp(mats[number], state, CHAIN_PASSES) + adds[number]
        return carry

    def chain():
        for group in range(groups):
            pair_ref[group] = begin
        lax.fori_loop(0, steps, one_step, 0)

    def one_read(group, carry):
        for step in range(steps):
            place_rows = pl.ds(pl.multiple_of(group * rows + step * chunk, chunk), chunk)
            got = dotp(by_head(queries[place_rows], lane_head), hist[group * steps + step], READ_PASSES)
            upper, lower = got[:chunk], got[chunk:]
            carried_ref[place_rows] = jnp.where(lane_head == 0, upper, pltpu.roll(lower, head_size, 1))
            local_ref[place_rows] += jnp.where(lane_head == 0, pltpu.roll(upper, head_size, 1), lower)
        return carry

    return one_block, chain, lambda: lax.fori_loop(0, groups, one_read, 0)


def body(*args):
    outer, middle, inner = radices_of("sp")
    heads, channels = args[13].shape[1], args[2].shape[1]
    width = channels // outer
    fits = (
        lax.axis_size("tp") == 2 and outer > 3 and middle == 2 and inner == 2
        and heads % outer == 0 and width == 128 and args[5].shape[1] % (128 * outer) == 0
    )
    return fast_body(*args) if fits else plain_body(*args)


def fast_body(
    tokens,
    input_norm_gain,
    query_matrix,
    key_matrix,
    value_matrix,
    convolution_value_matrix,
    convolution_gate_matrix,
    decay_offset_channel,
    decay_first_matrix,
    decay_second_matrix,
    learning_rate_offset,
    learning_rate_first_matrix,
    learning_rate_second_matrix,
    forgetting_rate_factor,
    state_retention_share,
    per_head_norm_gain,
    convolution_filter_taps,
    convolution_channel_gain,
    attention_output_matrix,
    convolution_output_matrix,
):
    heads, channels = forgetting_rate_factor.shape[1], query_matrix.shape[1]
    head_size = channels // heads
    side = jnp.concatenate([forgetting_rate_factor.T, state_retention_share.T], axis=0)
    weights = (
        query_matrix, key_matrix, value_matrix, convolution_value_matrix, convolution_gate_matrix,
        attention_output_matrix, convolution_output_matrix,
    )
    return spread(
        tokens, input_norm_gain[None], side, weights, ((0, 1, 2), (3, 4), (5, 6)),
        (decay_first_matrix, learning_rate_first_matrix),
        (
            decay_second_matrix, learning_rate_second_matrix, decay_offset_channel[None], learning_rate_offset[None],
            convolution_filter_taps, per_head_norm_gain[None], convolution_channel_gain[None],
        ),
        head_size, "sp", "tp",
    )


def solution(mesh):
    return jax.shard_map(
        body,
        mesh=mesh,
        in_specs=(
            P("sp", None),
            P(),
            P("sp", "tp"),
            P("sp", "tp"),
            P("sp", "tp"),
            P("sp", "tp"),
            P("sp", "tp"),
            P("tp"),
            P(),
            P(None, "tp"),
            P("tp"),
            P(),
            P(None, "tp"),
            P("sp", "tp"),
            P("sp", "tp"),
            P("tp"),
            P(None, "tp"),
            P("tp"),
            P("sp", "tp"),
            P("sp", "tp"),
        ),
        out_specs=P("sp", None),
        check_vma=False,
    )
```

```python
import functools
import math

import jax
import jax.numpy as jnp
from jax import lax
from jax.experimental import pallas as pl
from jax.experimental.pallas import tpu as pltpu
from jax.sharding import PartitionSpec as P


MESH = pl.DeviceIdType.MESH
HIGHEST = lax.Precision.HIGHEST
RMS_EPSILON = 1e-06
GROUP_EPSILON = 0.00064
LAYER_EPSILON = 1e-05
UNIT_EPSILON = 1e-06
EXP_HALF = math.exp(-0.5)


def split(x):
    top = x.astype(jnp.bfloat16)
    return top, (x - top.astype(jnp.float32)).astype(jnp.bfloat16)


def dot3(left, right, dims=((1,), (0,))):
    (lh, ll), (rh, rl) = split(left), split(right)

    def one(p, q):
        return lax.dot_general(p, q, (dims, ((), ())), preferred_element_type=jnp.float32)

    return one(lh, rh) + (one(lh, rl) + one(ll, rh))


def dot3t(left, right):
    return dot3(left, right, ((1,), (1,)))


def exact(left, right):
    return jnp.dot(left, right, precision=HIGHEST, preferred_element_type=jnp.float32)


def column(values, index):
    lanes = lax.broadcasted_iota(jnp.int32, values.shape, 1)
    return jnp.sum(jnp.where(lanes == index, values, 0.0), axis=1, keepdims=True)


def delta_kernel(
    head_size, chunk, block,
    query_ref, key_ref, value_ref, decay_ref, rate_ref, factor_ref, share_ref,
    local_ref, carried_ref, pair_ref,
):
    rows, width = query_ref.shape
    per = width // head_size
    pair = 0 if factor_ref.shape[1] == per else pl.program_id(0)
    lane = lax.broadcasted_iota(jnp.int32, (1, width), 1)
    lane_head = lane // head_size
    row_w = lax.broadcasted_iota(jnp.int32, (width, width), 0)
    col_w = lax.broadcasted_iota(jnp.int32, (width, width), 1)
    same_head = (row_w // head_size) == (col_w // head_size)
    ones_head = jnp.where(same_head, 1.0, 0.0)
    row_b = lax.broadcasted_iota(jnp.int32, (block, block), 0)
    col_b = lax.broadcasted_iota(jnp.int32, (block, block), 1)
    same_chunk = (row_b // chunk) == (col_b // chunk)
    strict = same_chunk & (row_b > col_b)
    incl = same_chunk & (row_b >= col_b)
    sums = jnp.concatenate([jnp.where(incl, 1.0, 0.0), jnp.where(same_chunk, 1.0, 0.0)], axis=0)
    eye_b = jnp.where(row_b == col_b, 1.0, 0.0)

    factor, share = factor_ref[...], jnp.log(share_ref[...])
    factor_w = jnp.zeros((rows, width), jnp.float32)
    share_w = jnp.zeros((rows, width), jnp.float32)
    for h in range(per):
        factor_w = jnp.where(lane_head == h, column(factor, pair * per + h), factor_w)
        share_w = jnp.where(lane_head == h, column(share, pair * per + h), share_w)
    logdec = share_w - (EXP_HALF * jax.nn.sigmoid(decay_ref[...])) * factor_w
    learn = jax.nn.sigmoid(rate_ref[...])
    key = key_ref[...]
    unit = key * lax.rsqrt(exact(key * key, ones_head) + UNIT_EPSILON)

    blocks = []
    for start in range(0, rows, block):
        cut = slice(start, start + block)
        q, k, v, ld = query_ref[cut], key[cut], value_ref[cut], logdec[cut]
        er, wr = -unit[cut], unit[cut] * learn[cut]
        both = exact(sums, ld)
        gain, total = both[:block], both[block:]
        mid = 0.5 * total
        up, down, bup = jnp.exp(gain - mid), jnp.exp(mid - gain), jnp.exp(gain - ld - mid)
        ehat, qhat, what, khat = er * bup, q * up, wr * down, k * down
        right = jnp.concatenate([what, khat], axis=0)
        eh_full, q_full = er * jnp.exp(gain - ld), q * jnp.exp(gain)
        to_end = jnp.exp(total - gain)
        pulled = solved = local = query = None
        heads = []
        for h in range(per):
            left = jnp.where(lane_head == h, jnp.concatenate([ehat, qhat], axis=0), 0.0)
            grid = dot3t(left, right)
            ew = jnp.where(strict, grid[:block, :block], 0.0)
            ek = jnp.where(strict, grid[:block, block:], 0.0)
            rw = jnp.where(incl, grid[block:, :block], 0.0)
            rk = jnp.where(incl, grid[block:, block:], 0.0)
            size = 2
            off = (row_b // size == col_b // size) & (row_b > col_b)
            inv = eye_b + jnp.where(off, ew, 0.0)
            while size < chunk:
                off = (row_b // (2 * size) == col_b // (2 * size)) & (row_b // size > col_b // size)
                inv = inv + dot3(dot3(inv, jnp.where(off, ew, 0.0)), inv)
                size *= 2
            seen = dot3(jnp.concatenate([ek, rk], axis=0), v)
            both = dot3(inv, jnp.concatenate([seen[:block], eh_full], axis=1))
            read = dot3(rw, both)
            heads.append((both[:, :width], both[:, width:], read[:, :width] + seen[block:], read[:, width:]))
        merged = list(heads[0])
        for h in range(1, per):
            merged = [jnp.where(lane_head == h, new, old) for new, old in zip(heads[h], merged)]
        pulled, solved, local, query = merged
        blocks.append((pulled, solved, local, q_full + query, v, wr * to_end, k * to_end, jnp.exp(total)))

    state = jnp.concatenate([jnp.where(row_w == col_w, 1.0, 0.0), jnp.zeros((width, width), jnp.float32)], axis=0)
    across = ((0,), (0,))
    for number, (pulled, solved, local, query, v, wend, kend, gain) in enumerate(blocks):
        for first in range(0, block, chunk):
            cut = slice(first, first + chunk)
            place = slice(number * block + first, number * block + first + chunk)
            got = dot3t(query[cut], state)
            carried_ref[place] = got[:, :width]
            local_ref[place] = local[cut] + got[:, width:]
            step = jnp.where(same_head, dot3(solved[cut], wend[cut], across), 0.0)
            added = dot3(
                jnp.concatenate([pulled[cut], v[cut]], axis=0),
                jnp.concatenate([wend[cut], kend[cut]], axis=0),
                across,
            )
            added = jnp.where(same_head, added, 0.0)
            moved = state * gain[first : first + 1] + dot3(state, step)
            state = jnp.concatenate([moved[:width], moved[width:] + added], axis=0)
    pair_ref[0] = state


def finish_kernel(head_size, local_ref, carried_ref, state_ref, gain_ref, out_ref):
    width = local_ref.shape[1]
    row_w = lax.broadcasted_iota(jnp.int32, (width, width), 0)
    col_w = lax.broadcasted_iota(jnp.int32, (width, width), 1)
    same_head = (row_w // head_size) == (col_w // head_size)
    average = jnp.where(same_head, 1.0 / head_size, 0.0)
    y = local_ref[...] + dot3t(carried_ref[...], state_ref[0])
    centred = y - exact(y, average)
    variance = exact(centred * centred, average)
    out_ref[...] = (centred * lax.rsqrt(variance + GROUP_EPSILON) * gain_ref[...]).astype(jnp.bfloat16)


def from_behind(value, axis, steps):
    count = lax.axis_size(axis)
    initial, last = (max(0, -steps), min(count, count - steps))
    return lax.ppermute(value, axis, [(source, source + steps) for source in range(initial, last)])


def head_blocks(pairs, head_size):
    width = pairs.shape[-1]
    return jnp.stack(
        [pairs[:, a : a + head_size, a : a + head_size] for a in range(0, width, head_size)], axis=1
    )


def delta_rule(query, key, value, decay_pre, rate_pre, factor, share, gain):
    rows, channels = query.shape
    heads = factor.shape[1]
    head_size = channels // heads
    per = math.gcd(heads, max(1, 128 // head_size))
    width, pairs = per * head_size, heads // per
    block = math.gcd(rows, 128)
    chunk = math.gcd(block, 16)
    wide = pl.BlockSpec((rows, width), lambda i: (0, i))
    whole = pl.BlockSpec((rows, heads), lambda i: (0, 0))
    local, carried, pair = pl.pallas_call(
        functools.partial(delta_kernel, head_size, chunk, block),
        grid=(pairs,),
        in_specs=[wide] * 5 + [whole] * 2,
        out_specs=[wide, wide, pl.BlockSpec((1, 2 * width, width), lambda i: (i, 0, 0))],
        out_shape=[
            jax.ShapeDtypeStruct((rows, channels), jnp.float32),
            jax.ShapeDtypeStruct((rows, channels), jnp.float32),
            jax.ShapeDtypeStruct((pairs, 2 * width, width), jnp.float32),
        ],
        cost_estimate=pl.CostEstimate(
            flops=pairs * rows * width * width * 60, bytes_accessed=rows * channels * 32, transcendentals=rows * channels * 10
        ),
        name="delta_chunks",
    )(query, key, value, decay_pre, rate_pre, factor, share)

    phi, psi = head_blocks(pair[:, :width], head_size), head_blocks(pair[:, width:], head_size)
    both = jnp.concatenate([phi, psi], axis=-2).reshape(heads, 2 * head_size, head_size)
    count, place = lax.axis_size("sp"), lax.axis_index("sp")
    steps = 1
    while steps < count - 1:
        earlier = from_behind(both, "sp", steps)
        new = exact_mul("hcd,hde->hce", earlier, both[:, :head_size])
        new = new + jnp.concatenate([jnp.zeros_like(both[:, :head_size]), both[:, head_size:]], axis=1)
        both = jnp.where(place >= steps, new, both)
        steps *= 2
    state = from_behind(both[:, head_size:], "sp", 1).reshape(pairs, per, head_size, head_size)
    same = jnp.eye(per, dtype=jnp.float32)
    state = (state[:, :, :, None, :] * same[None, :, None, :, None]).reshape(pairs, width, width)
    return pl.pallas_call(
        functools.partial(finish_kernel, head_size),
        grid=(pairs,),
        in_specs=[wide, wide, pl.BlockSpec((1, width, width), lambda i: (i, 0, 0)), pl.BlockSpec((1, width), lambda i: (0, i))],
        out_specs=wide,
        out_shape=jax.ShapeDtypeStruct((rows, channels), jnp.bfloat16),
        name="delta_finish",
    )(local, carried, state, gain[None])


def exact_mul(form, left, right):
    return jnp.einsum(form, left, right, precision=HIGHEST)


def gather_kernel(axis, radices, number, *refs):
    ins, outs = refs[:number], refs[number : 2 * number]
    own_sem, far_send, far_recv, near_send, near_recv = refs[2 * number :]
    outer, middle, inner = radices
    me = lax.axis_index(axis)
    x, y, z = me % inner, (me // inner) % middle, me // (inner * middle)

    def index(z_at, y_at, x_at):
        return (z_at * middle + y_at) * inner + x_at

    far = [index((z + step) % outer, y, x) for step in range(1, outer)]
    near = {}
    if inner == 2:
        near["x"] = index(z, y, 1 - x)
    if middle == 2:
        near["y"] = index(z, 1 - y, x)
    barrier = pltpu.get_barrier_semaphore()
    peers = far + list(near.values())
    for peer in peers:
        pl.semaphore_signal(barrier, inc=1, device_id={axis: peer}, device_id_type=MESH)
    pl.semaphore_wait(barrier, len(peers))

    def far_copy(w, step, to, z_from):
        return pltpu.make_async_remote_copy(
            src_ref=ins[w],
            dst_ref=outs[w].at[z_from, y, x],
            send_sem=far_send.at[w, step],
            recv_sem=far_recv.at[w, step],
            device_id={axis: to},
            device_id_type=MESH,
        )

    own = [pltpu.make_async_copy(ins[w], outs[w].at[z, y, x], own_sem.at[w]) for w in range(number)]
    for w in range(number):
        own[w].start()
        for step in range(outer - 1):
            far_copy(w, step, far[step], z).start()

    def region(w, order, stage, from_y, from_x):
        if stage == 0:
            return outs[w].at[:, from_y, from_x]
        return outs[w].at[:, from_y] if order[0] == "x" else outs[w].at[:, :, from_x]

    def near_copy(w, order, stage, from_y, from_x):
        part = region(w, order, stage, from_y, from_x)
        return pltpu.make_async_remote_copy(
            src_ref=part,
            dst_ref=part,
            send_sem=near_send.at[w, stage],
            recv_sem=near_recv.at[w, stage],
            device_id={axis: near[order[stage]]},
            device_id_type=MESH,
        )

    def theirs(w, order, stage):
        from_y, from_x = (y, 1 - x) if order[stage] == "x" else (1 - y, x)
        return near_copy(w, order, stage, from_y, from_x)

    names = list(near)
    orders = [names if w % 2 == 0 else names[::-1] for w in range(number)]

    def advance(w, stage):
        if stage == 0:
            own[w].wait()
            for step in range(outer - 1):
                far_copy(w, step, far[step], (z + outer - step - 1) % outer).wait_recv()
        else:
            theirs(w, orders[w], stage - 1).wait_recv()
        if stage < len(names):
            near_copy(w, orders[w], stage, y, x).start()

    last = len(names)
    for tick in range(number + last):
        for stage in range(last, -1, -1):
            w = tick - stage
            if 0 <= w < number:
                advance(w, stage)
    for w in range(number):
        for step in range(outer - 1):
            far_copy(w, step, far[step], z).wait_send()
        for stage in range(last):
            near_copy(w, orders[w], stage, y, x).wait_send()


def gather_rows(arrays, axis, number_id=0):
    count, number = lax.axis_size(axis), len(arrays)
    inner = math.gcd(count, 2)
    middle = math.gcd(count // inner, 2)
    radices = (count // inner // middle, middle, inner)
    outs = pl.pallas_call(
        functools.partial(gather_kernel, axis, radices, number),
        in_specs=[pl.BlockSpec(memory_space=pltpu.VMEM)] * number,
        out_specs=[pl.BlockSpec(memory_space=pl.ANY)] * number,
        out_shape=[jax.ShapeDtypeStruct(radices + item.shape, item.dtype) for item in arrays],
        scratch_shapes=[
            pltpu.SemaphoreType.DMA((number,)),
            pltpu.SemaphoreType.DMA((number, max(1, radices[0] - 1))),
            pltpu.SemaphoreType.DMA((number, max(1, radices[0] - 1))),
            pltpu.SemaphoreType.DMA((number, 2)),
            pltpu.SemaphoreType.DMA((number, 2)),
        ],
        compiler_params=pltpu.CompilerParams(collective_id=number_id, has_side_effects=True),
        cost_estimate=pl.CostEstimate(
            flops=10**9, bytes_accessed=sum(item.size for item in arrays) * 2 * count, transcendentals=0
        ),
        name="gather_rows",
    )(*arrays)
    return [out.reshape((-1,) + item.shape[1:]) for out, item in zip(outs, arrays)]


def plain_body(
    tokens,
    input_norm_gain,
    query_matrix,
    key_matrix,
    value_matrix,
    convolution_value_matrix,
    convolution_gate_matrix,
    decay_offset_channel,
    decay_first_matrix,
    decay_second_matrix,
    learning_rate_offset,
    learning_rate_first_matrix,
    learning_rate_second_matrix,
    forgetting_rate_factor,
    state_retention_share,
    per_head_norm_gain,
    convolution_filter_taps,
    convolution_channel_gain,
    attention_output_matrix,
    convolution_output_matrix,
):
    tok_rows = tokens.shape[0]
    widened = tokens.astype(jnp.float32)
    normed = (
        widened
        * lax.rsqrt(jnp.mean(widened * widened, axis=-1, keepdims=True) + RMS_EPSILON)
        * input_norm_gain
    ).astype(jnp.bfloat16)
    pieces = (
        *gather_rows((query_matrix, key_matrix, value_matrix), "sp"),
        lax.all_gather(convolution_value_matrix, "sp", axis=0, tiled=True),
        lax.all_gather(convolution_gate_matrix, "sp", axis=0, tiled=True),
    )
    query_proj, key_proj, value_proj, conv_value, conv_gate = tuple(
        (jnp.dot(normed, piece, preferred_element_type=jnp.float32) for piece in pieces)
    )
    decay_mid = jnp.tanh(
        jnp.dot(normed, decay_first_matrix, preferred_element_type=jnp.float32)
    ).astype(jnp.bfloat16)
    rate_mid = jnp.dot(
        normed, learning_rate_first_matrix, preferred_element_type=jnp.float32
    ).astype(jnp.bfloat16)
    decay_pre = decay_offset_channel + jnp.dot(
        decay_mid, decay_second_matrix, preferred_element_type=jnp.float32
    )
    rate_pre = learning_rate_offset + jnp.dot(
        rate_mid, learning_rate_second_matrix, preferred_element_type=jnp.float32
    )
    state_mixed = delta_rule(
        query_proj, key_proj, value_proj, decay_pre, rate_pre,
        forgetting_rate_factor, state_retention_share, per_head_norm_gain,
    )
    gated = (conv_value * jax.nn.sigmoid(conv_gate)).astype(jnp.bfloat16)
    span = convolution_filter_taps.shape[0]
    rim = from_behind(gated[tok_rows - (span - 1) :], "sp", 1)
    padded = jnp.concatenate([rim, gated], axis=0)
    filtered = jnp.zeros(gated.shape, jnp.float32)
    for offset in range(span):
        filtered = filtered + convolution_filter_taps[offset] * padded[offset : offset + tok_rows]
    total_sum, total_square = lax.psum(
        (jnp.sum(filtered, axis=-1), jnp.sum(filtered * filtered, axis=-1)), "tp"
    )
    conv_channels = filtered.shape[1] * lax.axis_size("tp")
    row_mean = total_sum / conv_channels
    deviation = filtered - row_mean[:, None]
    variance = total_square / conv_channels - row_mean * row_mean
    conv_mixed = jax.nn.silu(
        deviation * lax.rsqrt(variance + LAYER_EPSILON)[:, None] * convolution_channel_gain
    ).astype(jnp.bfloat16)
    contract_dims = (((1,), (1,)), ((), ()))
    pieces = lax.all_gather(
        (attention_output_matrix, convolution_output_matrix), "sp", axis=0, tiled=True
    )
    partial_out = lax.dot_general(
        state_mixed, pieces[0], contract_dims, preferred_element_type=jnp.float32
    ) + lax.dot_general(conv_mixed, pieces[1], contract_dims, preferred_element_type=jnp.float32)
    partial_out = partial_out.astype(jnp.bfloat16)
    if lax.axis_size("tp") != 2:
        return lax.psum(partial_out, "tp")
    other = lax.ppermute(partial_out, "tp", [(0, 1), (1, 0)])
    return (partial_out.astype(jnp.float32) + other.astype(jnp.float32)).astype(jnp.bfloat16)


def radices_of(axis):
    count = lax.axis_size(axis)
    inner = math.gcd(count, 2)
    middle = math.gcd(count // inner, 2)
    return count // inner // middle, middle, inner


def place_of(axis, radices):
    outer, middle, inner = radices
    me = lax.axis_index(axis)
    return me // (inner * middle), (me // inner) % middle, me % inner


def greet(devices, meanwhile=None):
    barrier = pltpu.get_barrier_semaphore()
    for device in devices:
        pl.semaphore_signal(barrier, inc=1, device_id=device, device_id_type=MESH)
    if meanwhile is not None:
        meanwhile()
    pl.semaphore_wait(barrier, len(devices))


def spread_kernel(axis, pair_axis, radices, widths, placed, firsts, early, head_size, chunk, block, *refs):
    number = len(widths)
    raw_ref, gain_ref, side_ref, ins = refs[0], refs[1], refs[2], refs[3 : 3 + number]
    refs = refs[3 + number :]
    extra, maps, refs = refs[: len(firsts)], refs[len(firsts) : len(firsts) + 7], refs[len(firsts) + 7 :]
    decay_ref, rate_ref, decay_offset_ref, rate_offset_ref, taps_ref, head_gain_ref, conv_gain_ref = maps
    kinds = 1 + max(out for out, _ in placed)
    out_ref, local_ref, carried_ref, pair_ref, filtered_ref, stats_ref, last_out = refs[:7]
    finish_refs, refs = refs[7:27], refs[27:]
    (first_out, second_out, padded, rim_out, rim_in, rim_send, rim_recv, tokens_out, side_out, tokens_ref, proj, mats, adds, hist, queries,
     first_sem, own_sem, far_send, far_recv, near_send, near_recv, side_send, side_recv,
     tok_send, tok_recv, sib_send, sib_recv) = refs
    outs = [first_out, second_out, last_out]
    outer, middle, inner = radices
    z, y, x = place_of(axis, radices)
    core = lax.axis_index(pair_axis)
    half = tokens_ref.shape[0] // 2
    mine, other = pl.ds(pl.multiple_of(core * half, half), half), pl.ds(pl.multiple_of((1 - core) * half, half), half)

    def index(z_at, y_at, x_at):
        return (z_at * middle + y_at) * inner + x_at

    far = [(z + step) % outer for step in range(1, outer)]
    near = {"x": index(z, y, 1 - x), "y": index(z, 1 - y, x)}
    planes = middle * inner
    plane = y * inner + x
    peers, send_pairs, send_stats, wait_pairs, make_states, state_rows, wait_stats, reduce_all = finish_phases(
        axis, pair_axis, radices, head_size,
        pair_ref, stats_ref, local_ref, carried_ref, head_gain_ref, filtered_ref, conv_gain_ref, last_out, out_ref,
        *finish_refs,
    )

    def normalize():
        widened = raw_ref[...].astype(jnp.float32)
        scale = lax.rsqrt(jnp.mean(widened * widened, axis=-1, keepdims=True) + RMS_EPSILON)
        tokens_ref[...] = (widened * scale * gain_ref[...]).astype(jnp.bfloat16)

    greet(peers, normalize)

    def part(w, at):
        return ins[w].at[:, pl.ds(pl.multiple_of(at * widths[w], widths[w]), widths[w])]

    def slot(w, *where, cut=slice(None)):
        out, offset = placed[w]
        return outs[out].at[(*where, cut, pl.ds(offset, widths[w]))]

    def far_copy(w, step, to, z_from):
        return pltpu.make_async_remote_copy(
            src_ref=part(w, to), dst_ref=slot(w, z_from, y, x),
            send_sem=far_send.at[w, step], recv_sem=far_recv.at[w, step],
            device_id={axis: index(to, y, x)}, device_id_type=MESH,
        )

    def side_copy(step, to, z_from):
        return pltpu.make_async_remote_copy(
            src_ref=side_ref, dst_ref=side_out.at[z_from],
            send_sem=side_send.at[step], recv_sem=side_recv.at[step],
            device_id={axis: index(to, y, x)}, device_id_type=MESH,
        )

    names = list(near)
    depth = ins[0].shape[0]
    orders = [names, names[::-1]]

    def near_copy(w, part_at, stage, y_at, x_at):
        order = orders[part_at]
        cut = pl.ds(part_at * (depth // 2), depth // 2)
        if stage == 0:
            region = slot(w, slice(None), y_at, x_at, cut=cut)
        elif order[0] == "x":
            region = slot(w, slice(None), y_at, slice(None), cut=cut)
        else:
            region = slot(w, slice(None), slice(None), x_at, cut=cut)
        return pltpu.make_async_remote_copy(
            src_ref=region, dst_ref=region,
            send_sem=near_send.at[w, part_at, stage], recv_sem=near_recv.at[w, part_at, stage],
            device_id={axis: near[order[stage]]}, device_id_type=MESH,
        )

    def theirs(w, part_at, stage):
        y_at, x_at = (y, 1 - x) if orders[part_at][stage] == "x" else (1 - y, x)
        return near_copy(w, part_at, stage, y_at, x_at)

    def inside(at):
        return (at >= 0) & (at < outer)

    ways = (1, -1)

    def token_copy(way, step, block, source):
        return pltpu.make_async_remote_copy(
            src_ref=source, dst_ref=tokens_out.at[block, mine],
            send_sem=tok_send.at[way, step], recv_sem=tok_recv.at[way, step],
            device_id={axis: index((z + ways[way] + outer) % outer, y, x)}, device_id_type=MESH,
        )

    def sibling_copy(way, step, block, rows):
        return pltpu.make_async_remote_copy(
            src_ref=tokens_out.at[block, rows], dst_ref=tokens_out.at[block, rows],
            send_sem=sib_send.at[way, step], recv_sem=sib_recv.at[way, step],
            device_id={pair_axis: 1 - core}, device_id_type=MESH,
        )

    def arrived(way, step):
        return z - ways[way] * (step + 1)

    def sends(way, step):
        return inside(z + ways[way]) & inside(z - ways[way] * step)

    own = [pltpu.make_async_copy(part(w, z), slot(w, z, y, x), own_sem.at[w]) for w in range(number)]
    own.append(pltpu.make_async_copy(tokens_ref, tokens_out.at[z], own_sem.at[number]))
    own.append(pltpu.make_async_copy(side_ref, side_out.at[z], own_sem.at[number + 1]))
    for step in range(outer - 1):
        side_copy(step, far[step], z).start()
    def send_far(some):
        for w in some:
            own[w].start()
            for step in range(outer - 1):
                far_copy(w, step, far[step], z).start()

    send_far(early)
    for way in range(2):
        @pl.when(sends(way, 0))
        def _():
            token_copy(way, 0, z, tokens_ref.at[mine]).start()
    rest = [[w for w in range(number) if placed[w][0] == out] for out in range(1, kinds)]
    send_far(rest[0])
    own[number].start()
    own[number + 1].start()
    kept = []
    for item, (out, offset) in enumerate(firsts):
        for at in range(outer * middle * inner):
            where = (at // (middle * inner), (at // inner) % middle, at % inner)
            kept.append(pltpu.make_async_copy(
                extra[item].at[at * depth : (at + 1) * depth],
                outs[out].at[(*where, slice(None), pl.ds(offset, extra[item].shape[1]))],
                first_sem.at[item, at],
            ))
            kept[-1].start()

    def advance(w, stage):
        if stage == 0:
            own[w].wait()
            for step in range(outer - 1):
                far_copy(w, step, far[step], (z + outer - step - 1) % outer).wait_recv()
        for part_at in range(2):
            if stage:
                theirs(w, part_at, stage - 1).wait_recv()
            if stage < len(names):
                near_copy(w, part_at, stage, y, x).start()

    def token_step(step):
        for way in range(2):
            block = arrived(way, step)
            @pl.when(inside(block))
            def _():
                token_copy(way, step, block, tokens_out.at[block, mine]).wait_recv()
                @pl.when(sends(way, step + 1) & (step + 1 < outer - 1))
                def _():
                    token_copy(way, step + 1, block, tokens_out.at[block, mine]).start()
                sibling_copy(way, step, block, mine).start()

    last = len(names)

    def sibling_step(step):
        for way in range(2):
            block = arrived(way, step)
            @pl.when(inside(block))
            def _():
                sibling_copy(way, step, block, other).wait_recv()

    def run(some):
        for tick in range(len(some) + last):
            for stage in range(last + 1):
                if 0 <= tick - stage < len(some):
                    advance(some[tick - stage], stage)

    run(early)
    own[number].wait()
    own[number + 1].wait()
    for item in kept:
        item.wait()
    for step in range(outer - 1):
        side_copy(step, far[step], (z + outer - step - 1) % outer).wait_recv()
    token_step(0)
    send_far(rest[1])
    one_block, chain, read = delta_phases(
        z, head_size, chunk, block, proj, side_out, decay_ref, rate_ref, decay_offset_ref, rate_offset_ref,
        local_ref, carried_ref, pair_ref, mats, adds, hist, queries,
    )
    pieces = tokens_ref.shape[0] // block
    edge = jnp.minimum(z, outer - 1 - z)
    toward = jnp.where(z < outer // 2, -1, 1)
    piece_depth = middle * inner * depth

    def project(group):
        total = None
        for part_at in range(outer):
            matrix = first_out[part_at].reshape(piece_depth, first_out.shape[-1])
            term = jnp.dot(
                tokens_out[group, :, part_at * piece_depth : (part_at + 1) * piece_depth], matrix,
                preferred_element_type=jnp.float32,
            )
            total = term if total is None else total + term
        proj[...] = total

    conv_width = second_out.shape[-1] // 2
    rows, rim_rows = tokens_ref.shape[0], rim_out.shape[1]

    def group_of(k):
        twosided = k <= 2 * edge
        distance = jnp.where(twosided, (k + 1) // 2, k - edge)
        return z + jnp.where(twosided & (k % 2 == 1), toward, -toward) * distance

    def gate(k, carry):
        group, total = group_of(k), None
        for part_at in range(outer):
            matrix = second_out[part_at].reshape(piece_depth, 2 * conv_width)
            term = jnp.dot(
                tokens_out[group, :, part_at * piece_depth : (part_at + 1) * piece_depth], matrix,
                preferred_element_type=jnp.float32,
            )
            total = term if total is None else total + term
        gated = (total[:, :conv_width] * jax.nn.sigmoid(total[:, conv_width:])).astype(jnp.bfloat16)
        padded[group, rim_rows:] = gated.astype(jnp.float32)
        rim_out[group] = gated[rows - rim_rows :]
        return carry

    def one_round(k, carry):
        group = group_of(k)

        @pl.when(k == outer - 1)
        def _():
            for w in rest[1]:
                advance(w, 0)
            for w in rest[0]:
                advance(w, last)
            lax.fori_loop(0, outer - 1, gate, 0)
            for w in rest[1]:
                advance(w, 1)
            token_step(outer - 2)

        @pl.when(k > 0)
        def _():
            sibling_step(k - 1)

        project(group)
        for piece in range(pieces):
            one_block(group, piece)
            if piece == 0:
                @pl.when(k == 1)
                def _():
                    for w in rest[0]:
                        advance(w, 1)

                @pl.when((k > 0) & (k < outer - 2))
                def _():
                    token_step(k)

        @pl.when(k == 0)
        def _():
            for w in rest[0]:
                advance(w, 0)

        return carry

    lax.fori_loop(0, outer, one_round, 0)
    gate(outer - 1, 0)
    span = taps_ref.shape[0]
    rim_copy = pltpu.make_async_remote_copy(
        src_ref=rim_out, dst_ref=rim_in, send_sem=rim_send.at[0], recv_sem=rim_recv.at[0],
        device_id={axis: z * planes + (plane + 1) % planes}, device_id_type=MESH,
    )
    rim_copy.start()
    chain()
    send_pairs()
    read()
    rim_copy.wait_recv()
    for group in range(outer):
        before = jnp.zeros(rim_in.shape[1:], jnp.bfloat16) if group == 0 else rim_in[group - 1]
        padded[group, :rim_rows] = jnp.where(plane == 0, before, rim_in[group]).astype(jnp.float32)
    taps = taps_ref[:, pl.ds(pl.multiple_of(z * conv_width, conv_width), conv_width)]
    part_rows = math.gcd(rows, 64)
    row_8 = lax.broadcasted_iota(jnp.int32, (8, conv_width), 0)
    sum_rows = [jnp.where(row_8 == at, 1.0, 0.0).astype(jnp.bfloat16) for at in range(2)]
    skip = rim_rows - (span - 1)

    def row_sums(values, marks):
        total = None
        for _ in range(3):
            top = values.astype(jnp.bfloat16)
            term = lax.dot_general(marks, top, (((1,), (1,)), ((), ())), preferred_element_type=jnp.float32)
            total = term if total is None else total + term
            values = values - top.astype(jnp.float32)
        return total

    def convolve(number, carry):
        group, start = number // (rows // part_rows), (number % (rows // part_rows)) * part_rows
        window = padded[group, pl.ds(pl.multiple_of(start, part_rows), part_rows + rim_rows)]
        total = jnp.zeros((part_rows, conv_width), jnp.float32)
        for turn in range(8):
            moved = window if turn == 0 else window[turn : turn + part_rows + rim_rows - 8]
            for tap in range(span):
                if (tap + skip) % 8 == turn:
                    first = tap + skip - turn
                    total = total + taps[tap : tap + 1] * moved[first : first + part_rows]
        filtered_ref[pl.ds(pl.multiple_of(number * part_rows, part_rows), part_rows)] = total
        return carry

    lax.fori_loop(0, outer * (rows // part_rows), convolve, 0)
    for group in range(outer):
        values = filtered_ref[group * rows : (group + 1) * rows]
        stats_ref[group] = row_sums(values, sum_rows[0]) + row_sums(values * values, sum_rows[1])
    for w in rest[1]:
        advance(w, last)
    send_stats()
    wait_pairs()
    make_states()
    state_rows()
    wait_stats()
    reduce_all()
    rim_copy.wait_send()
    for step in range(outer - 1):
        side_copy(step, far[step], z).wait_send()
    for step in range(outer - 1):
        for way in range(2):
            block = arrived(way, step)
            @pl.when(inside(block))
            def _():
                sibling_copy(way, step, block, mine).wait_send()
            @pl.when(sends(way, step))
            def _():
                token_copy(way, step, z - ways[way] * step, tokens_ref.at[mine]).wait_send()
    for w in range(number):
        for step in range(outer - 1):
            far_copy(w, step, far[step], z).wait_send()
        for stage in range(last):
            for part_at in range(2):
                near_copy(w, part_at, stage, y, x).wait_send()


def spread(tokens, gain, side, weights, groups, firsts, maps, head_size, axis, pair_axis):
    radices = radices_of(axis)
    outer, number = radices[0], len(weights)
    widths = [item.shape[1] // outer for item in weights]
    placed, totals = [None] * number, []
    for out, members in enumerate(groups):
        offset = 0
        for w in members:
            placed[w] = (out, offset)
            offset += widths[w]
        totals.append(offset)
    extras, width = [], widths[0]
    for item in firsts:
        extras.append((0, totals[0]))
        totals[0] += item.shape[1]
    depth, rows = weights[0].shape[0], tokens.shape[0]
    block = math.gcd(rows, 128)
    chunk = math.gcd(block, 32)
    total = outer * rows
    conv_width, rim_rows = totals[1] // 2, -(-(maps[4].shape[0] - 1) // 16) * 16
    vmem, dma = pl.BlockSpec(memory_space=pltpu.VMEM), pltpu.SemaphoreType.DMA
    planes, lines = radices[1] * radices[2], outer * lax.axis_size(pair_axis) - 1
    half, slots = tokens.shape[1] // 2, (2, outer - 1)
    return pl.pallas_call(
        functools.partial(
            spread_kernel, axis, pair_axis, radices, widths, placed, extras, groups[0], head_size, chunk, block
        ),
        in_specs=[vmem] * (3 + number + len(firsts) + len(maps)),
        out_specs=vmem,
        out_shape=jax.ShapeDtypeStruct(tokens.shape, jnp.bfloat16),
        scratch_shapes=[
            pltpu.VMEM((total, width), jnp.float32),
            pltpu.VMEM((total, width), jnp.float32),
            pltpu.VMEM((outer, width, width), jnp.float32),
            pltpu.VMEM((total, conv_width), jnp.float32),
            pltpu.VMEM((outer, 8, rows), jnp.float32),
            pltpu.VMEM(radices + (depth, totals[2]), weights[0].dtype),
            pltpu.VMEM((planes, outer, width, width), jnp.float32),
            pltpu.VMEM((lines, outer, 8, rows), jnp.float32),
            pltpu.VMEM((outer, width, width), jnp.float32),
            pltpu.VMEM((outer, rows, width + conv_width), jnp.bfloat16),
            pltpu.VMEM((outer, rows, half), jnp.float32),
            pltpu.VMEM((outer, rows, half), jnp.bfloat16),
            pltpu.VMEM((outer, rows, half), jnp.bfloat16),
            pltpu.VMEM(slots + (rows, half), jnp.bfloat16),
            pltpu.VMEM(slots + (rows, half), jnp.bfloat16),
            dma((1,)), dma((planes - 1,)), dma((planes - 1,)), dma((lines,)), dma((lines,)),
            dma((outer,)), dma((outer,)), dma(slots), dma(slots), dma((1,)), dma((1,)),
            pltpu.VMEM(radices + (depth, totals[0]), weights[0].dtype),
            pltpu.VMEM(radices + (depth, totals[1]), weights[0].dtype),
            pltpu.VMEM((outer, rim_rows + rows, conv_width), jnp.float32),
            pltpu.VMEM((outer, rim_rows, conv_width), weights[0].dtype),
            pltpu.VMEM((outer, rim_rows, conv_width), weights[0].dtype),
            pltpu.SemaphoreType.DMA((1,)),
            pltpu.SemaphoreType.DMA((1,)),
            pltpu.VMEM((outer,) + tokens.shape, tokens.dtype),
            pltpu.VMEM((outer,) + side.shape, side.dtype),
            pltpu.VMEM(tokens.shape, tokens.dtype),
            pltpu.VMEM((rows, totals[0]), jnp.float32),
        ]
        + [pltpu.VMEM((total // chunk, width, width), jnp.float32)] * 3
        + [
            pltpu.VMEM((total, width), jnp.float32),
            pltpu.SemaphoreType.DMA((len(firsts), math.prod(radices))),
            pltpu.SemaphoreType.DMA((number + 3,)),
            pltpu.SemaphoreType.DMA((number, outer - 1)),
            pltpu.SemaphoreType.DMA((number, outer - 1)),
            pltpu.SemaphoreType.DMA((number, 2, 2)),
            pltpu.SemaphoreType.DMA((number, 2, 2)),
            pltpu.SemaphoreType.DMA((outer - 1,)),
            pltpu.SemaphoreType.DMA((outer - 1,)),
            pltpu.SemaphoreType.DMA((2, outer - 1)),
            pltpu.SemaphoreType.DMA((2, outer - 1)),
            pltpu.SemaphoreType.DMA((2, outer - 1)),
            pltpu.SemaphoreType.DMA((2, outer - 1)),
        ],
        compiler_params=pltpu.CompilerParams(collective_id=0, has_side_effects=True, vmem_limit_bytes=60 * 2**20),
        cost_estimate=pl.CostEstimate(flops=10**10, bytes_accessed=8 * tokens.size * outer, transcendentals=0),
        name="whole_layer",
    )(tokens, gain, side, *weights, *firsts, *maps)


def spread_sum(values, matrix):
    top, rest = split(values)
    return jnp.dot(top, matrix, preferred_element_type=jnp.float32) + jnp.dot(
        rest, matrix, preferred_element_type=jnp.float32
    )


def finish_phases(
    axis, pair_axis, radices, head_size,
    pair_ref, stats_ref, local_ref, carried_ref, gain_ref, filtered_ref, conv_gain_ref, matrix_ref,
    out_ref,
    held, stats, smat, mixed_all, keep, twin_out, twin_in, chain_out, chain_in,
    own_sem, pair_send, pair_recv, stat_send, stat_recv,
    twin_send, twin_recv, chain_send, chain_recv, last_send, last_recv,
):
    outer, middle, inner = radices
    planes = middle * inner
    z, y, x = place_of(axis, radices)
    place = y * inner + x
    core = lax.axis_index(pair_axis)
    width, conv_width = pair_ref.shape[-1], filtered_ref.shape[-1]
    rows, half = keep.shape[1:]
    ways = (1, -1)
    plane_peers = [(place + step) % planes for step in range(1, planes)]
    cores = lax.axis_size(pair_axis)
    lines = [(dz, dc) for dz in range(outer) for dc in range(cores) if dz or dc]

    def line_device(dz, dc):
        return {axis: ((z + dz) % outer) * planes + place, pair_axis: (core + dc) % cores}

    def inside(at):
        return (at >= 0) & (at < outer)

    peers = [{axis: z * planes + peer} for peer in plane_peers] + [line_device(*line) for line in lines]

    def pair_copy(step, p_from):
        return pltpu.make_async_remote_copy(
            src_ref=pair_ref, dst_ref=held.at[p_from],
            send_sem=pair_send.at[step], recv_sem=pair_recv.at[step],
            device_id={axis: z * planes + plane_peers[step]}, device_id_type=MESH,
        )

    def stat_copy(number):
        return pltpu.make_async_remote_copy(
            src_ref=stats_ref, dst_ref=stats.at[number],
            send_sem=stat_send.at[number], recv_sem=stat_recv.at[number],
            device_id=line_device(*lines[number]), device_id_type=MESH,
        )

    def twin_copy(block):
        return pltpu.make_async_remote_copy(
            src_ref=twin_out.at[block], dst_ref=twin_in.at[block],
            send_sem=twin_send.at[block], recv_sem=twin_recv.at[block],
            device_id={pair_axis: 1 - core}, device_id_type=MESH,
        )

    def chain_copy(way, steps):
        return pltpu.make_async_remote_copy(
            src_ref=chain_out.at[way, steps - 1], dst_ref=chain_in.at[way, steps - 1],
            send_sem=chain_send.at[way, steps - 1], recv_sem=chain_recv.at[way, steps - 1],
            device_id={axis: ((z + 1 - 2 * way + outer) % outer) * planes + place}, device_id_type=MESH,
        )

    own = pltpu.make_async_copy(pair_ref, held.at[place], own_sem.at[0])

    def send_pairs():
        for step in range(planes - 1):
            pair_copy(step, place).start()
        own.start()

    def send_stats():
        for number in range(len(lines)):
            stat_copy(number).start()

    channels = conv_width * outer * cores
    conv_gain = conv_gain_ref[:, pl.ds(pl.multiple_of(z * conv_width, conv_width), conv_width)]
    lane_2 = lax.broadcasted_iota(jnp.int32, (8, 256), 1) // 128
    pick = jnp.where(lax.broadcasted_iota(jnp.int32, (8, 256), 0) == lane_2, 1.0, 0.0)
    dims = (((1,), (1,)), ((), ()))

    def rows_of(block):
        return pl.ds(pl.multiple_of(block * rows, rows), rows)

    def side_rows(side):
        return pl.ds(pl.multiple_of(side * half, half), half)

    def side_matrix(side):
        these = matrix_ref[pl.ds(side * (outer // 2), outer // 2)]
        return these.reshape(half, matrix_ref.shape[-1])

    def conv_part(block):
        totals = stats_ref[block]
        for number in range(len(lines)):
            totals = totals + stats[number, block]
        spread_totals = lax.dot_general(
            totals, pick, (((0,), (0,)), ((), ())), precision=HIGHEST, preferred_element_type=jnp.float32
        )
        mean, square = spread_totals[:, :128] / channels, spread_totals[:, 128:] / channels
        scale = lax.rsqrt(square - mean * mean + LAYER_EPSILON)
        mean = jnp.concatenate([mean] * (conv_width // 128), axis=1)
        scale = jnp.concatenate([scale] * (conv_width // 128), axis=1)
        normal = (filtered_ref[rows_of(block), :] - mean) * scale * conv_gain
        mixed_all[block, :, width:] = jax.nn.silu(normal).astype(jnp.bfloat16)

    row = lax.broadcasted_iota(jnp.int32, (width, width), 0)
    lane = lax.broadcasted_iota(jnp.int32, (width, width), 1)
    average = jnp.where((row // head_size) == (lane // head_size), 1.0 / head_size, 0.0).astype(jnp.bfloat16)
    first_head, moves = row < head_size, lane < head_size

    def step_matrix(item):
        part = jnp.where(moves, item, 0.0)
        return jnp.where(first_head, part, pltpu.roll(part, head_size, 1))

    def state_matrix(item):
        part = jnp.where(moves, 0.0, item)
        return jnp.where(first_head, pltpu.roll(part, head_size, 1), part)

    def compose(earlier, later):
        return dot3(step_matrix(later), earlier) + jnp.where(moves, 0.0, later)

    nothing = jnp.where(moves & (row % head_size == lane), 1.0, 0.0)

    def wait_pairs():
        own.wait()
        for step in range(planes - 1):
            pair_copy(step, (place + planes - step - 1) % planes).wait_recv()

    def make_states():
        before, whole = [], []
        for block in range(outer):
            total, kept = held[0, block], nothing
            for p in range(1, planes):
                kept = jnp.where(place == p, total, kept)
                total = compose(total, held[p, block])
            before.append(kept)
            whole.append(total)
        state = jnp.zeros((width, width), jnp.float32)
        for block in range(outer):
            smat[block] = state_matrix(compose(state, before[block]))
            if block + 1 < outer:
                state = compose(state, whole[block])

    gain = gain_ref[:, pl.ds(pl.multiple_of(z * width, width), width)]

    def state_part(block, carry):
        cut = rows_of(block)
        full = local_ref[cut, :] + dot3(carried_ref[cut, :], smat[block])
        centred = full - spread_sum(full, average)
        variance = spread_sum(centred * centred, average)
        mixed_all[block, :, :width] = (centred * lax.rsqrt(variance + GROUP_EPSILON) * gain).astype(jnp.bfloat16)
        return carry

    def at_end():
        return (z == 0) | (z == outer - 1)

    def order(number):
        return jnp.where(z < outer // 2, outer - 1 - number, number)

    def product(block, side):
        return lax.dot_general(
            mixed_all[block], side_matrix(side), dims, preferred_element_type=jnp.float32
        )

    def one_product(number, carry):
        block = order(number)
        conv_part(block)
        twin_out[block] = product(block, 1 - core).astype(jnp.bfloat16)
        twin_copy(block).start()
        keep[block] = product(block, core)

        @pl.when(at_end() & (number > 0))
        def _():
            earlier = order(number - 1)
            way = jnp.where(z == 0, 0, 1)
            steps = jnp.where(z == 0, earlier, z - earlier)
            twin_copy(earlier).wait_recv()
            chain_out[way, steps - 1] = (keep[earlier] + twin_in[earlier].astype(jnp.float32)).astype(jnp.bfloat16)
            chain_copy(way, steps).start()
        return carry

    def wait_stats():
        for number in range(len(lines)):
            stat_copy(number).wait_recv()

    def reduce_all():
        lax.fori_loop(0, outer, one_product, 0)
        for steps in range(outer - 2, 0, -1):
            for way in range(2):
                block = z + ways[way] * steps

                @pl.when(inside(block) & (z > 0) & (z < outer - 1))
                def _():
                    twin_copy(block).wait_recv()
                    keep[block] += twin_in[block].astype(jnp.float32)
                    chain_copy(way, steps + 1).wait_recv()
                    chain_out[way, steps - 1] = (keep[block] + chain_in[way, steps].astype(jnp.float32)).astype(jnp.bfloat16)
                    chain_copy(way, steps).start()

        twin_copy(z).wait_recv()
        keep[z] += twin_in[z].astype(jnp.float32)
        for way in range(2):
            @pl.when(inside(z - ways[way]))
            def _():
                chain_copy(way, 1).wait_recv()
                keep[z] += chain_in[way, 0].astype(jnp.float32)

        out_ref[:, side_rows(core)] = keep[z].astype(jnp.bfloat16)

        def last_copy(side):
            where = out_ref.at[:, side_rows(side)]
            return pltpu.make_async_remote_copy(
                src_ref=where, dst_ref=where, send_sem=last_send.at[0], recv_sem=last_recv.at[0],
                device_id={pair_axis: 1 - core}, device_id_type=MESH,
            )

        last_copy(core).start()
        for step in range(planes - 1):
            pair_copy(step, place).wait_send()
        for number in range(len(lines)):
            stat_copy(number).wait_send()
        for block in range(outer):
            twin_copy(block).wait_send()
        for steps in range(outer - 1, 0, -1):
            for way in range(2):
                @pl.when(inside(z + ways[way] * steps))
                def _():
                    chain_copy(way, steps).wait_send()
        last_copy(1 - core).wait_recv()
        last_copy(core).wait_send()

    return peers, send_pairs, send_stats, wait_pairs, make_states, lambda: lax.fori_loop(0, outer, state_part, 0), wait_stats, reduce_all


def dotp(left, right, passes, dims=((1,), (0,))):
    def one(p, q):
        return lax.dot_general(p, q, (dims, ((), ())), preferred_element_type=jnp.float32)

    if passes == 1:
        return one(left.astype(jnp.bfloat16), right.astype(jnp.bfloat16))
    (lh, ll), (rh, rl) = split(left), split(right)
    return one(lh, rh) + (one(lh, rl) + one(ll, rh))


GRID_PASSES, SOLVE_PASSES, SEEN_PASSES, STEP_PASSES, CHAIN_PASSES, READ_PASSES = 3, 3, 3, 3, 3, 3


def delta_phases(
    z, head_size, chunk, block,
    proj_ref, side_ref, decay_ref, rate_ref, decay_offset_ref, rate_offset_ref,
    local_ref, carried_ref, pair_ref,
    mats, adds, hist, queries,
):
    groups, _, rows = side_ref.shape
    width = local_ref.shape[1]
    heads = side_ref.shape[1] // 2
    per, pieces = width // head_size, rows // block
    chunks, steps = block // chunk, rows // chunk
    wide = per * block

    def iota(shape, dim):
        return lax.broadcasted_iota(jnp.int32, shape, dim)

    lane_head = iota((1, width), 1) // head_size
    lane_head2 = (iota((1, 2 * width), 1) % width) // head_size
    row_w, col_w = iota((width, width), 0), iota((width, width), 1)
    same_head = (row_w // head_size) == (col_w // head_size)
    ones_head = jnp.where(same_head, 1.0, 0.0).astype(jnp.bfloat16)
    row_b, col_b = iota((block, block), 0), iota((block, block), 1)
    same_chunk = (row_b // chunk) == (col_b // chunk)
    strict = same_chunk & (row_b > col_b)
    incl = same_chunk & (row_b >= col_b)
    sums = jnp.concatenate([jnp.where(incl, 1.0, 0.0), jnp.where(same_chunk, 1.0, 0.0)], axis=0).astype(jnp.bfloat16)
    row_c, col_c = iota((chunk, wide), 0), iota((chunk, wide), 1) % chunk
    eye_c = jnp.where(row_c == col_c, 1.0, 0.0)
    diagonal = (iota((wide, wide), 0) // chunk) == (iota((wide, wide), 1) // chunk)
    spread_rows = (iota((block, wide), 0) // chunk) == ((iota((block, wide), 1) % block) // chunk)
    place = iota((2 * heads, 2 * width), 0)
    chosen = z * per + lane_head2 + jnp.where(iota((1, 2 * width), 1) < width, 0, heads)
    expand = jnp.where(place == chosen, 1.0, 0.0)
    ours = pl.ds(pl.multiple_of(z * width, width), width)
    decay_matrix, rate_matrix = decay_ref[:, ours], rate_ref[:, ours]
    decay_offset, rate_offset = decay_offset_ref[:, ours], rate_offset_ref[:, ours]
    side_row = iota((2 * heads, block), 0)

    def by_head(values, mark):
        return jnp.concatenate([jnp.where(mark == h, values, 0.0) for h in range(per)], axis=0)

    def widen(compact):
        return jnp.where(diagonal, jnp.concatenate([compact] * (wide // chunk), axis=0), 0.0)

    def one_block(group, piece):
        start = pl.multiple_of(group * rows + piece * block, block)
        cut = pl.ds(start, block)
        here = slice(piece * block, (piece + 1) * block)
        q, key, v = proj_ref[here, 0:width], proj_ref[here, width : 2 * width], proj_ref[here, 2 * width : 3 * width]
        inner_width = decay_ref.shape[0]
        mid_at = 3 * width
        decay_mid = jnp.tanh(proj_ref[here, mid_at : mid_at + inner_width]).astype(jnp.bfloat16)
        rate_mid = proj_ref[here, mid_at + inner_width : mid_at + 2 * inner_width].astype(jnp.bfloat16)
        decay_pre = decay_offset + jnp.dot(decay_mid, decay_matrix, preferred_element_type=jnp.float32)
        rate_pre = rate_offset + jnp.dot(rate_mid, rate_matrix, preferred_element_type=jnp.float32)
        thin = side_ref[group, :, piece * block : (piece + 1) * block]
        thin = jnp.where(side_row < heads, thin, jnp.log(thin))
        both = lax.dot_general(
            thin, expand, (((0,), (0,)), ((), ())), precision=HIGHEST, preferred_element_type=jnp.float32
        )
        ld = both[:, width:] - (EXP_HALF * jax.nn.sigmoid(decay_pre)) * both[:, :width]
        learn = jax.nn.sigmoid(rate_pre)
        unit = key * lax.rsqrt(spread_sum(key * key, ones_head) + UNIT_EPSILON)
        er, wr = -unit, unit * learn
        top, rest = split(ld)
        third = (ld - top.astype(jnp.float32) - rest.astype(jnp.float32)).astype(jnp.bfloat16)
        both = jnp.dot(sums, top, preferred_element_type=jnp.float32) + (
            jnp.dot(sums, rest, preferred_element_type=jnp.float32)
            + jnp.dot(sums, third, preferred_element_type=jnp.float32)
        )
        gain, total = both[:block], both[block:]
        mid = 0.5 * total
        up, down, bup = jnp.exp(gain - mid), jnp.exp(mid - gain), jnp.exp(gain - ld - mid)
        left = jnp.concatenate([er * bup, q * up], axis=0)
        what, khat = wr * down, key * down
        right = jnp.concatenate(
            [jnp.where(lane_head == h, item, 0.0) for h in range(per) for item in (what, khat)], axis=0
        )
        grid = dotp(left, right, GRID_PASSES, ((1,), (1,)))

        def piece_of(upper, kind, mask):
            cut_rows = slice(0, block) if upper else slice(block, 2 * block)
            return jnp.concatenate(
                [jnp.where(mask, grid[cut_rows, (2 * h + kind) * block : (2 * h + kind + 1) * block], 0.0) for h in range(per)],
                axis=1,
            )

        ew, ek = piece_of(True, 0, strict), piece_of(True, 1, strict)
        rw, rk = piece_of(False, 0, incl), piece_of(False, 1, incl)
        compact = ew[:chunk]
        for c in range(1, chunks):
            compact = compact + ew[c * chunk : (c + 1) * chunk]
        size = 2
        inv = eye_c + jnp.where((row_c // size == col_c // size) & (row_c > col_c), compact, 0.0)
        while size < chunk:
            off = (row_c // (2 * size) == col_c // (2 * size)) & (row_c // size > col_c // size)
            part = dotp(inv, widen(jnp.where(off, compact, 0.0)), SOLVE_PASSES)
            inv = inv + dotp(part, widen(inv), SOLVE_PASSES)
            size *= 2
        inverse = jnp.where(spread_rows, jnp.concatenate([inv] * chunks, axis=0), 0.0)
        seen = dotp(jnp.concatenate([ek, rk], axis=0), by_head(v, lane_head), SEEN_PASSES)
        eh_full = er * jnp.exp(gain - ld)
        both = jnp.concatenate([seen[:block], eh_full], axis=1)
        both = dotp(inverse, by_head(both, lane_head2), SEEN_PASSES)
        read = dotp(rw, by_head(both, lane_head2), SEEN_PASSES)
        local_ref[cut] = read[:, :width] + seen[block:]
        queries[cut] = q * jnp.exp(gain) + read[:, width:]
        to_end, ends = jnp.exp(total - gain), jnp.exp(total)
        wend, kend = wr * to_end, key * to_end
        zero = jnp.zeros((chunk, width), jnp.float32)
        for c in range(chunks):
            now = slice(c * chunk, (c + 1) * chunk)
            lhs = jnp.concatenate([wend[now], kend[now]], axis=0)
            rhs = jnp.concatenate(
                [
                    jnp.concatenate([both[now, width:], both[now, :width]], axis=1),
                    jnp.concatenate([zero, v[now]], axis=1),
                ],
                axis=0,
            )
            made = dotp(lhs, rhs, STEP_PASSES, ((0,), (0,)))
            number = group * steps + piece * chunks + c
            step = jnp.where(same_head, made[:, :width], 0.0)
            mats[number] = step + jnp.where(row_w == col_w, ends[c * chunk : c * chunk + 1], 0.0)
            added = made[:, width:]
            added = jnp.where(row_w < head_size, pltpu.roll(added, head_size, 1), added)
            adds[number] = jnp.where(col_w < head_size, 0.0, added)

    begin = jnp.where(row_w % head_size == col_w, 1.0, 0.0)

    def one_step(step, carry):
        for group in range(groups):
            number = group * steps + step
            state = pair_ref[group]
            hist[number] = state
            pair_ref[group] = dotp(mats[number], state, CHAIN_PASSES) + adds[number]
        return carry

    def chain():
        for group in range(groups):
            pair_ref[group] = begin
        lax.fori_loop(0, steps, one_step, 0)

    def one_read(group, carry):
        for step in range(steps):
            place_rows = pl.ds(pl.multiple_of(group * rows + step * chunk, chunk), chunk)
            got = dotp(by_head(queries[place_rows], lane_head), hist[group * steps + step], READ_PASSES)
            upper, lower = got[:chunk], got[chunk:]
            carried_ref[place_rows] = jnp.where(lane_head == 0, upper, pltpu.roll(lower, head_size, 1))
            local_ref[place_rows] += jnp.where(lane_head == 0, pltpu.roll(upper, head_size, 1), lower)
        return carry

    return one_block, chain, lambda: lax.fori_loop(0, groups, one_read, 0)


def body(*args):
    outer, middle, inner = radices_of("sp")
    heads, channels = args[13].shape[1], args[2].shape[1]
    width = channels // outer
    fits = (
        lax.axis_size("tp") == 2 and outer > 3 and middle == 2 and inner == 2
        and heads % outer == 0 and width == 128 and args[5].shape[1] % (128 * outer) == 0
    )
    return fast_body(*args) if fits else plain_body(*args)


def fast_body(
    tokens,
    input_norm_gain,
    query_matrix,
    key_matrix,
    value_matrix,
    convolution_value_matrix,
    convolution_gate_matrix,
    decay_offset_channel,
    decay_first_matrix,
    decay_second_matrix,
    learning_rate_offset,
    learning_rate_first_matrix,
    learning_rate_second_matrix,
    forgetting_rate_factor,
    state_retention_share,
    per_head_norm_gain,
    convolution_filter_taps,
    convolution_channel_gain,
    attention_output_matrix,
    convolution_output_matrix,
):
    heads, channels = forgetting_rate_factor.shape[1], query_matrix.shape[1]
    head_size = channels // heads
    side = jnp.concatenate([forgetting_rate_factor.T, state_retention_share.T], axis=0)
    weights = (
        query_matrix, key_matrix, value_matrix, convolution_value_matrix, convolution_gate_matrix,
        attention_output_matrix, convolution_output_matrix,
    )
    return spread(
        tokens, input_norm_gain[None], side, weights, ((0, 1, 2), (3, 4), (5, 6)),
        (decay_first_matrix, learning_rate_first_matrix),
        (
            decay_second_matrix, learning_rate_second_matrix, decay_offset_channel[None], learning_rate_offset[None],
            convolution_filter_taps, per_head_norm_gain[None], convolution_channel_gain[None],
        ),
        head_size, "sp", "tp",
    )


def solution(mesh):
    return jax.shard_map(
        body,
        mesh=mesh,
        in_specs=(
            P("sp", None),
            P(),
            P("sp", "tp"),
            P("sp", "tp"),
            P("sp", "tp"),
            P("sp", "tp"),
            P("sp", "tp"),
            P("tp"),
            P(),
            P(None, "tp"),
            P("tp"),
            P(),
            P(None, "tp"),
            P("sp", "tp"),
            P("sp", "tp"),
            P("tp"),
            P(None, "tp"),
            P("tp"),
            P("sp", "tp"),
            P("sp", "tp"),
        ),
        out_specs=P("sp", None),
        check_vma=False,
    )
```
